128 devices in a mesh: kv: 16 (over z, y), tp: 8 (over x, core).
Axes of the slice: x: 4, y: 4, z: 4, core: 2. Of those that a mesh axis runs over, the one named last changes fastest.
Arguments:
- activations: bfloat16 [128, 4096], P(None, ('kv', 'tp')), may hold values from -60 to 60
- mixer_gain: bfloat16 [4096], P(('kv', 'tp')), may hold values from 0.099609375 to 1.8984375
- channel_gain: bfloat16 [4096], P(('kv', 'tp')), may hold values from 0.099609375 to 1.8984375
- query_weight: bfloat16 [4096, 4096], P('kv', 'tp'), may hold values from -0.09375 to 0.09375
- key_weight: bfloat16 [4096, 4096], P('kv', 'tp'), may hold values from -0.09375 to 0.09375
- value_weight: bfloat16 [4096, 8192], P('kv', 'tp'), may hold values from -0.09375 to 0.09375
- gate_weight: bfloat16 [4096, 8192], P('kv', 'tp'), may hold values from -0.09375 to 0.09375
- output_weight: bfloat16 [8192, 4096], P('tp', 'kv'), may hold values from -0.1875 to 0.1875
- up_weight: bfloat16 [4096, 16384], P('kv', 'tp'), may hold values from -0.09375 to 0.09375
- down_weight: bfloat16 [16384, 4096], P('tp', 'kv'), may hold values from -0.046875 to 0.046875
- state_in: float32 [128, 16, 256, 512], P('kv', 'tp'), may hold values from -0.5 to 0.5
Outputs:
- activations_out: bfloat16 [128, 4096], P(None, ('kv', 'tp'))
- state_out: float32 [128, 16, 256, 512], P('kv', 'tp')
The draws below stay inside these ranges and needn't reach their ends.
All inputs are finite; a program needn't handle non-finite values.
Results may differ from the reference program's by a relative error of at most 0.022.
Values may be sent and summed in bfloat16 or wider, within the bound.
No kernel may reach another device: no remote copies, remote signals or barrier semaphores. Data moves between devices by JAX's collectives and lax.ppermute only.
A program may use at most 64 MiB of HBM per device.

```python
import jax
import jax.numpy as jnp
from jax import lax

D = 4096
HEADS = 16
DK = 256
DV = 512
FF = 16384
BATCH = 128
QK = 4096
RV = 8192
N_TP = 8


def draw_activations(key, part):
    base_key, row_key = jax.random.split(key, 2)
    columns = jnp.exp(jnp.linspace(0.0, jnp.log(3.0), D, dtype=jnp.float32))
    base = jnp.clip(jax.random.normal(base_key, (BATCH, D), jnp.float32), -5.0, 5.0)
    scales = jnp.exp(jax.random.uniform(row_key, (BATCH, 1), jnp.float32, jnp.log(0.3), jnp.log(3.0)))
    return jnp.clip(base * scales * columns, -60.0, 60.0).astype(jnp.bfloat16)


def level_of(key, extent, shards, least, high):
    factor_of, own = 1.0, jax.random.fold_in(key, 6)
    for axis_at, shards_of in shards:
        heights = jnp.exp(jax.random.uniform(jax.random.fold_in(own, axis_at), (shards_of,), jnp.float32, least / len(shards), high / len(shards)))
        factor_of = factor_of * jnp.repeat(heights, extent[axis_at] // shards_of).reshape([-1 if axis == axis_at else 1 for axis in range(len(extent))])
    return factor_of


def normal_values(own_key, dims, spread, most, pieces=(), kind=jnp.bfloat16):
    values = spread * jax.random.normal(own_key, dims, jnp.float32)
    if pieces:
        values = values * level_of(own_key, dims, pieces, -0.22, 0.18)
    return jnp.clip(values, -most, most).astype(kind)


def setup_inputs(seed: int = 0) -> dict:
    key_list = jax.random.split(jax.random.key(seed), 12)
    activations = draw_activations(jax.random.fold_in(key_list[11], 71), 0)
    mixer_gain = jnp.clip(1.0 + 0.18 * jax.random.normal(key_list[1], (D,), jnp.float32), 0.099609375, 1.8984375).astype(jnp.bfloat16)
    channel_gain = jnp.clip(1.0 + 0.18 * jax.random.normal(key_list[2], (D,), jnp.float32), 0.099609375, 1.8984375).astype(jnp.bfloat16)
    query_weight = normal_values(key_list[3], (D, QK), D ** -0.5, 0.09375, ((0, 16), (1, 8)))
    key_weight = normal_values(key_list[4], (D, QK), D ** -0.5, 0.09375, ((0, 16), (1, 8)))
    value_weight = normal_values(key_list[5], (D, RV), D ** -0.5, 0.09375, ((0, 16), (1, 8)))
    gate_weight = normal_values(key_list[6], (D, RV), D ** -0.5, 0.09375, ((0, 16), (1, 8)))
    output_weight = normal_values(key_list[7], (RV, D), (RV // 8) ** -0.5, 0.1875, ((0, 8), (1, 16)))
    up_weight = normal_values(key_list[8], (D, FF), D ** -0.5, 0.09375, ((0, 16), (1, 8)))
    down_weight = normal_values(key_list[9], (FF, D), FF ** -0.5, 0.046875, ((0, 8), (1, 16)))
    state_in = normal_values(key_list[10], (BATCH, HEADS, DK, DV), 0.06, 0.5, ((0, 16), (1, 8)), jnp.float32)
    return dict(activations=activations, mixer_gain=mixer_gain, channel_gain=channel_gain, query_weight=query_weight, key_weight=key_weight, value_weight=value_weight, gate_weight=gate_weight, output_weight=output_weight, up_weight=up_weight, down_weight=down_weight, state_in=state_in)


EPS = 1e-06

def head_decays(count):
    index = jnp.arange(count, dtype=jnp.float32)
    return 1.0 - 2.0 ** (-1.0 - 6.0 * index / (count - 1))

def summed_blocks(left, right, parts):
    width = left.shape[1] // parts
    total = jnp.zeros((left.shape[0], right.shape[1]), jnp.float32)
    for index in range(parts):
        term = jnp.dot(left[:, index * width:(index + 1) * width], right[index * width:(index + 1) * width], preferred_element_type=jnp.float32)
        total = total + lax.optimization_barrier(term.astype(jnp.bfloat16)).astype(jnp.float32)
    return total

def reference(activations, mixer_gain, channel_gain, query_weight, key_weight, value_weight, gate_weight, output_weight, up_weight, down_weight, state_in):
    stream = activations.astype(jnp.float32)
    scale_rows = lax.rsqrt(lax.optimization_barrier(jnp.sum(stream * stream, axis=1, keepdims=True)) / D + EPS)
    normed = (stream * mixer_gain.astype(jnp.float32)).astype(jnp.bfloat16)
    query = scale_rows * jnp.dot(normed, query_weight, preferred_element_type=jnp.float32)
    key = scale_rows * jnp.dot(normed, key_weight, preferred_element_type=jnp.float32) * DK ** (-0.5)
    value = scale_rows * jnp.dot(normed, value_weight, preferred_element_type=jnp.float32)
    gate = scale_rows * jnp.dot(normed, gate_weight, preferred_element_type=jnp.float32)
    rates = head_decays(HEADS)

    def advance(inputs):
        query_row, key_row, value_row, old_state = inputs
        query_heads = query_row.reshape(HEADS, DK)
        key_heads = key_row.reshape(HEADS, DK)
        value_heads = value_row.reshape(HEADS, DV)
        new_state = rates[:, None, None] * old_state + key_heads[:, :, None] * value_heads[:, None, :]
        output = jnp.einsum('hd,hde->he', query_heads, new_state, precision=lax.Precision.HIGHEST)
        return (new_state, output)
    state_out, retained = lax.map(advance, (query, key, value, state_in))
    retained = retained * lax.rsqrt(lax.optimization_barrier(jnp.mean(retained * retained, axis=2, keepdims=True)) + EPS)
    mixed = (jax.nn.silu(gate) * retained.reshape(retained.shape[0], HEADS * DV)).astype(jnp.bfloat16)
    attention = summed_blocks(mixed, output_weight, N_TP)
    middle = (stream + attention).astype(jnp.bfloat16)
    middle = lax.optimization_barrier(middle).astype(jnp.float32)
    channel_scale = lax.rsqrt(lax.optimization_barrier(jnp.sum(middle * middle, axis=1, keepdims=True)) / D + EPS)
    channel_normed = (middle * channel_gain.astype(jnp.float32)).astype(jnp.bfloat16)
    lifted = channel_scale * jnp.dot(channel_normed, up_weight, preferred_element_type=jnp.float32)
    hidden = jnp.square(jax.nn.relu(lifted)).astype(jnp.bfloat16)
    lowered = summed_blocks(hidden, down_weight, N_TP)
    return ((middle + lowered).astype(jnp.bfloat16), state_out)
```

```python
import jax
import jax.numpy as jnp
from jax import lax
from jax.sharding import PartitionSpec as P

D = 4096
HEADS = 16
DK = 256
DV = 512
EPS = 1e-06
F32 = jnp.float32
BF16 = jnp.bfloat16


def head_decays(count):
    index = jnp.arange(count, dtype=F32)
    return 1.0 - 2.0 ** (-1.0 - 6.0 * index / (count - 1))


def gather_all(value, axis):
    size = lax.axis_size(axis)
    return lax.all_to_all(
        jnp.broadcast_to(value[None], (size, *value.shape)), axis, 0, 0, tiled=True
    )


def spread_sum(value, axis):
    parts = lax.all_to_all(value, axis, 0, 0, tiled=True)
    return jnp.sum(parts.astype(F32), axis=0)


def swap_cores(value):
    return lax.ppermute(value, "tp", [(i, i ^ 1) for i in range(8)])


def shift_chips(value, step):
    return lax.ppermute(value, "tp", [(i, (i + 2 * step) % 8) for i in range(8)])


def retain(query_sum, key_sum, value_sum, gate_sum, scale_rows, old_state, rates):
    count, heads = (old_state.shape[0], old_state.shape[1])
    query = (scale_rows * query_sum).reshape(count, heads, DK)
    key = (scale_rows * key_sum * DK ** (-0.5)).reshape(count, heads, DK)
    value = (scale_rows * value_sum).reshape(count, heads, DV)
    gate = scale_rows * gate_sum
    new_state = rates[None, :, None, None] * old_state + key[:, :, :, None] * value[:, :, None, :]
    output = jnp.einsum("shd,shde->she", query, new_state, precision=lax.Precision.HIGHEST)
    output = output * lax.rsqrt(jnp.mean(output * output, axis=2, keepdims=True) + EPS)
    mixed = (jax.nn.silu(gate) * output.reshape(count, heads * DV)).astype(BF16)
    return (new_state, mixed)


def per_device(
    activations,
    mixer_gain,
    channel_gain,
    query_weight,
    key_weight,
    value_weight,
    gate_weight,
    output_weight,
    up_weight,
    down_weight,
    state_in,
):
    tp = lax.axis_index("tp")
    core = tp % 2
    chip = tp // 2
    heads_dev = state_in.shape[1]
    rates = lax.dynamic_slice_in_dim(head_decays(HEADS), tp * heads_dev, heads_dev, 0)

    rows = jnp.concatenate(
        [
            activations.T,
            jnp.pad(mixer_gain[None], ((0, 0), (0, 96))),
            jnp.pad(channel_gain[None], ((0, 6), (0, 96))),
        ],
        axis=0,
    )
    packed = gather_all(rows, "tp")
    stream = packed[:, :32].reshape(256, 128).T.astype(F32)
    mixer = packed[:, 32, :32].reshape(1, 256).astype(F32)
    channel = packed[:, 33, :32].reshape(1, 256).astype(F32)

    squares = jnp.sum(stream * stream, axis=1, keepdims=True)
    normed = (stream * mixer).astype(BF16)
    terms = [
        jnp.dot(normed, w, preferred_element_type=F32).astype(BF16)
        for w in (query_weight, key_weight, value_weight, gate_weight)
    ]
    terms.append(jnp.pad(squares.astype(BF16), ((0, 0), (0, 127))))
    sums = spread_sum(jnp.concatenate(terms, axis=1).reshape(16, 8, -1), "kv")
    scale_rows = lax.rsqrt(sums[:, 3072:3073] / D + EPS)
    new_state, mixed = retain(
        sums[:, :512], sums[:, 512:1024], sums[:, 1024:2048], sums[:, 2048:3072],
        scale_rows, state_in, rates,
    )

    mixed_all = gather_all(mixed, "kv").reshape(128, 1024)
    out_terms = jnp.dot(mixed_all, output_weight, preferred_element_type=F32).astype(BF16)
    halves = (out_terms[:, :128], out_terms[:, 128:])
    mine = jnp.where(core == 0, halves[0], halves[1])
    theirs = jnp.where(core == 0, halves[1], halves[0])
    pair = (mine.astype(F32) + swap_cores(theirs).astype(F32)).astype(BF16)
    attention = pair.astype(F32)
    for step in (1, 3, 2):
        attention = attention + shift_chips(pair, step).astype(F32)
    stream_half = jnp.where(core == 0, stream[:, :128], stream[:, 128:])
    middle_half = (stream_half + attention).astype(BF16)
    other_half = swap_cores(middle_half)
    middle_bf = jnp.concatenate(
        [
            jnp.where(core == 0, middle_half, other_half),
            jnp.where(core == 0, other_half, middle_half),
        ],
        axis=1,
    )
    middle = middle_bf.astype(F32)
    middle_squares = jnp.sum(middle * middle, axis=1, keepdims=True)
    channel_normed = (middle * channel).astype(BF16)
    up_terms = jnp.concatenate(
        [
            jnp.dot(channel_normed, up_weight, preferred_element_type=F32).astype(BF16),
            jnp.pad(middle_squares.astype(BF16), ((0, 0), (0, 127))),
        ],
        axis=1,
    )
    up_sum = spread_sum(up_terms.reshape(16, 8, -1), "kv")
    lifted = lax.rsqrt(up_sum[:, 2048:2049] / D + EPS) * up_sum[:, :2048]
    hidden = jnp.square(jax.nn.relu(lifted)).astype(BF16)

    hidden_all = gather_all(hidden, "kv").reshape(128, 2048)
    down_terms = jnp.dot(hidden_all, down_weight, preferred_element_type=F32).astype(BF16)
    down_t = down_terms.T.reshape(4, 2, 32, 128)
    mine = jnp.where(core == 0, down_t[:, 0], down_t[:, 1])
    theirs = jnp.where(core == 0, down_t[:, 1], down_t[:, 0])
    pair = (mine.astype(F32) + swap_cores(theirs).astype(F32)).astype(BF16)
    lowered = lax.dynamic_index_in_dim(pair, chip, 0, keepdims=False).astype(F32)
    for step in (1, 3, 2):
        piece = lax.dynamic_index_in_dim(pair, (chip + step) % 4, 0, keepdims=False)
        lowered = lowered + shift_chips(piece, step).astype(F32)
    own = lax.dynamic_slice_in_dim(middle_bf.T, tp * 32, 32, 0).astype(F32)
    return ((own + lowered).astype(BF16).T, new_state)


def solution(mesh):
    return jax.shard_map(
        per_device,
        mesh=mesh,
        in_specs=(
            P(None, ("kv", "tp")),
            P(("kv", "tp")),
            P(("kv", "tp")),
            P("kv", "tp"),
            P("kv", "tp"),
            P("kv", "tp"),
            P("kv", "tp"),
            P("tp", "kv"),
            P("kv", "tp"),
            P("tp", "kv"),
            P("kv", "tp", None, None),
        ),
        out_specs=(P(None, ("kv", "tp")), P("kv", "tp", None, None)),
        check_vma=False,
    )
```

```python
import jax
import jax.numpy as jnp
from jax import lax
from jax.experimental import pallas as pl
from jax.experimental.pallas import tpu as pltpu
from jax.sharding import PartitionSpec as P

D = 4096
HEADS = 16
DK = 256
DV = 512
EPS = 1e-06
F32 = jnp.float32
BF16 = jnp.bfloat16
VMEM = pl.BlockSpec(memory_space=pltpu.VMEM)
SMEM = pl.BlockSpec(memory_space=pltpu.SMEM)
HBM = pl.BlockSpec(memory_space=pltpu.HBM)


def in_hbm(value):
    return pltpu.with_memory_space_constraint(value, pltpu.HBM)


def gather_all(value, axis):
    size = lax.axis_size(axis)
    return lax.all_to_all(
        jnp.broadcast_to(value[None], (size, *value.shape)), axis, 0, 0, tiled=True
    )


def swap_cores(value):
    return lax.ppermute(value, "tp", [(i, i ^ 1) for i in range(8)])


def swap_chips(value, mask):
    return lax.ppermute(value, "tp", [(i, i ^ (2 * mask)) for i in range(8)])


def squares_lanes(total, width):
    lane = lax.broadcasted_iota(jnp.int32, (total.shape[0], width), 1)
    high = total.astype(BF16).astype(F32)
    return jnp.where(lane == 0, high, jnp.where(lane == 1, total - high, 0.0)).astype(BF16)


def project_body(packed, wq, wk, wv, wg, terms, stream_out, gains_out, bq, bk, bv, bg, sems):
    pairs = ((wq, bq), (wk, bk), (wv, bv), (wg, bg))
    copies = [pltpu.make_async_copy(w, buf, sems.at[i]) for i, (w, buf) in enumerate(pairs)]
    for copy in copies:
        copy.start()
    stream = packed[:, :32, :].astype(F32).reshape(256, 128).T
    stream_out[...] = stream.astype(BF16)
    gains = jnp.sum(packed[:, 32:40, :].astype(F32), axis=0)
    gains_out[...] = gains
    mixer = jnp.concatenate([gains[0:1], gains[1:2]], axis=1)
    normed = (stream * mixer).astype(BF16)
    terms[:, 3072:] = squares_lanes(jnp.sum(stream * stream, axis=1, keepdims=True), 128)
    at = 0
    for copy, (_, buf) in zip(copies, pairs):
        n = buf.shape[1]
        copy.wait()
        terms[:, at : at + n] = jnp.dot(normed, buf[...], preferred_element_type=F32).astype(BF16)
        at += n


def retain_body(rates, parts, state_hbm, mixed_out, key_out, value_out, kept, state, sems):
    copies = [pltpu.make_async_copy(state_hbm.at[b], state.at[b], sems.at[b]) for b in range(8)]
    for copy in copies:
        copy.start()
    sums = jnp.sum(parts[...].astype(F32), axis=0)
    scale = lax.rsqrt((sums[:, 3072:3073] + sums[:, 3073:3074]) / D + EPS)
    query = scale * sums[:, :512]
    key = scale * sums[:, 512:1024] * DK ** (-0.5)
    value = scale * sums[:, 1024:2048]
    gate = scale * sums[:, 2048:3072]
    query_t = query.T
    key_out[...] = key.T
    value_out[...] = value
    for b in range(8):
        copies[b].wait()
        for h in range(2):
            total = jnp.zeros((8, 512), F32)
            for r in range(0, 256, 64):
                qc = query_t[h * 256 + r : h * 256 + r + 64, b : b + 1]
                total = total + jnp.sum((qc * state[b, h, r : r + 64, :]).reshape(8, 8, 512), axis=0)
            kept[b : b + 1, h * 512 : (h + 1) * 512] = jnp.sum(total, axis=0, keepdims=True)
    for h in range(2):
        cols = slice(h * 512, (h + 1) * 512)
        heads = slice(h * 256, (h + 1) * 256)
        match = jnp.sum(query[:, heads] * key[:, heads], axis=1, keepdims=True)
        out = rates[h] * kept[:, cols] + match * value[:, cols]
        out = out * lax.rsqrt(jnp.mean(out * out, axis=1, keepdims=True) + EPS)
        g = gate[:, cols]
        mixed = (g * jax.nn.sigmoid(g) * out).astype(BF16)
        for j in range(16):
            mixed_out[j, :, cols] = mixed


def advance_body(rates, key_t, value, state_hbm, new_hbm, state, new, in_sems, out_sems):
    reads = [pltpu.make_async_copy(state_hbm.at[b], state.at[b], in_sems.at[b]) for b in range(8)]
    writes = [pltpu.make_async_copy(new.at[b], new_hbm.at[b], out_sems.at[b]) for b in range(8)]
    for copy in reads:
        copy.start()
    for b in range(8):
        reads[b].wait()
        for h in range(2):
            row = value[b : b + 1, h * 512 : (h + 1) * 512]
            for r in range(0, 256, 64):
                kc = key_t[h * 256 + r : h * 256 + r + 64, b : b + 1]
                new[b, h, r : r + 64, :] = rates[h] * state[b, h, r : r + 64, :] + kc * row
        writes[b].start()
    for copy in writes:
        copy.wait()


def per_device(
    activations,
    mixer_gain,
    channel_gain,
    query_weight,
    key_weight,
    value_weight,
    gate_weight,
    output_weight,
    up_weight,
    down_weight,
    state_in,
):
    tp = lax.axis_index("tp")
    core = tp % 2
    chip = tp // 2
    heads_dev = state_in.shape[1]
    index = (tp * heads_dev + jnp.arange(heads_dev, dtype=jnp.int32)).astype(F32)
    rates = 1.0 - 2.0 ** (-1.0 - 6.0 * index / (HEADS - 1))

    spread = jnp.arange(128) // 32 == tp % 4
    tiled = [jnp.where(spread, jnp.tile(g, 4), 0) for g in (mixer_gain, channel_gain)]
    row = jnp.arange(8)[:, None]
    first = tp // 4
    gain_rows = jnp.where(row == first, tiled[0], jnp.where(row == first + 2, tiled[1], 0))
    rows = jnp.concatenate([activations.T, gain_rows.astype(BF16)], axis=0)
    rows, rates = lax.optimization_barrier((rows, rates))
    packed = gather_all(rows, "tp")

    weights = (query_weight, key_weight, value_weight, gate_weight)
    terms, stream, gains = pl.pallas_call(
        project_body,
        out_shape=(
            jax.ShapeDtypeStruct((128, 3200), BF16),
            jax.ShapeDtypeStruct((128, 256), BF16),
            jax.ShapeDtypeStruct((8, 128), F32),
        ),
        in_specs=[VMEM, HBM, HBM, HBM, HBM],
        out_specs=(VMEM, VMEM, VMEM),
        scratch_shapes=[pltpu.VMEM(w.shape, BF16) for w in weights]
        + [pltpu.SemaphoreType.DMA((4,))],
        compiler_params=pltpu.CompilerParams(vmem_limit_bytes=16 << 20),
        name="project",
    )(packed, *map(in_hbm, weights))
    channel = jnp.concatenate([gains[2:3], gains[3:4]], axis=1)
    stream = stream.astype(F32)
    parts = lax.all_to_all(terms.reshape(16, 8, 3200), "kv", 0, 0, tiled=True)

    state = in_hbm(state_in)
    mixed, key_t, value = pl.pallas_call(
        retain_body,
        out_shape=(
            jax.ShapeDtypeStruct((16, 8, 1024), BF16),
            jax.ShapeDtypeStruct((512, 8), F32),
            jax.ShapeDtypeStruct((8, 1024), F32),
        ),
        in_specs=[SMEM, VMEM, HBM],
        out_specs=(VMEM, VMEM, VMEM),
        scratch_shapes=[
            pltpu.VMEM((8, 1024), F32),
            pltpu.VMEM(state_in.shape, F32),
            pltpu.SemaphoreType.DMA((8,)),
        ],
        compiler_params=pltpu.CompilerParams(vmem_limit_bytes=16 << 20),
        name="retain",
    )(rates, parts, state)
    new_state = pl.pallas_call(
        advance_body,
        out_shape=jax.ShapeDtypeStruct(state_in.shape, F32),
        in_specs=[SMEM, VMEM, VMEM, HBM],
        out_specs=HBM,
        scratch_shapes=[
            pltpu.VMEM(state_in.shape, F32),
            pltpu.VMEM(state_in.shape, F32),
            pltpu.SemaphoreType.DMA((8,)),
            pltpu.SemaphoreType.DMA((8,)),
        ],
        compiler_params=pltpu.CompilerParams(vmem_limit_bytes=24 << 20),
        cost_estimate=pl.CostEstimate(flops=40_000_000, transcendentals=0, bytes_accessed=16 << 20),
        name="advance",
    )(rates, key_t, value, state)

    mixed_all = lax.all_to_all(mixed, "kv", 0, 0, tiled=True)
    mixed_all, new_state = lax.optimization_barrier((mixed_all, new_state))
    mixed_all = mixed_all.reshape(128, 1024)
    out_terms = jnp.dot(mixed_all, output_weight, preferred_element_type=F32).astype(BF16)
    halves = (out_terms[:, :128], out_terms[:, 128:])
    mine = jnp.where(core == 0, halves[0], halves[1])
    theirs = jnp.where(core == 0, halves[1], halves[0])
    pair = (mine.astype(F32) + swap_cores(theirs).astype(F32)).astype(BF16)
    quad = (pair.astype(F32) + swap_chips(pair, 1).astype(F32)).astype(BF16)
    attention = quad.astype(F32) + swap_chips(quad, 3).astype(F32)
    stream_half = jnp.where(core == 0, stream[:, :128], stream[:, 128:])
    middle_half = (stream_half + attention).astype(BF16)
    other_half = swap_cores(middle_half)
    middle_bf = jnp.concatenate(
        [
            jnp.where(core == 0, middle_half, other_half),
            jnp.where(core == 0, other_half, middle_half),
        ],
        axis=1,
    )
    middle = middle_bf.astype(F32)
    middle_squares = jnp.sum(middle * middle, axis=1, keepdims=True)
    channel_normed = (middle * channel).astype(BF16)
    up_terms = jnp.concatenate(
        [
            jnp.dot(channel_normed, up_weight, preferred_element_type=F32).astype(BF16),
            jnp.pad(middle_squares.astype(BF16), ((0, 0), (0, 127))),
        ],
        axis=1,
    )
    up_parts = lax.all_to_all(up_terms.reshape(16, 8, -1), "kv", 0, 0, tiled=True)
    up_sum = jnp.sum(up_parts.astype(F32), axis=0)
    lifted = lax.rsqrt(up_sum[:, 2048:2049] / D + EPS) * up_sum[:, :2048]
    hidden = jnp.square(jax.nn.relu(lifted)).astype(BF16)

    hidden_all = gather_all(hidden, "kv").reshape(128, 2048)
    down_terms = jnp.dot(hidden_all, down_weight, preferred_element_type=F32).astype(BF16)
    down_t = down_terms.T.reshape(4, 2, 32, 128)
    mine = jnp.where(core == 0, down_t[:, 0], down_t[:, 1])
    theirs = jnp.where(core == 0, down_t[:, 1], down_t[:, 0])
    pair = (mine.astype(F32) + swap_cores(theirs).astype(F32)).astype(BF16)
    keep = jnp.stack([lax.dynamic_index_in_dim(pair, chip ^ m, 0, keepdims=False) for m in (0, 3)])
    give = jnp.stack([lax.dynamic_index_in_dim(pair, chip ^ m, 0, keepdims=False) for m in (1, 2)])
    keep = keep.astype(F32) + swap_chips(give, 1).astype(F32)
    lowered = keep[0] + swap_chips(keep[1].astype(BF16), 3).astype(F32)
    own = lax.dynamic_slice_in_dim(middle_bf.T, tp * 32, 32, 0).astype(F32)
    return ((own + lowered).astype(BF16).T, new_state)


def solution(mesh):
    return jax.shard_map(
        per_device,
        mesh=mesh,
        in_specs=(
            P(None, ("kv", "tp")),
            P(("kv", "tp")),
            P(("kv", "tp")),
            P("kv", "tp"),
            P("kv", "tp"),
            P("kv", "tp"),
            P("kv", "tp"),
            P("tp", "kv"),
            P("kv", "tp"),
            P("tp", "kv"),
            P("kv", "tp", None, None),
        ),
        out_specs=(P(None, ("kv", "tp")), P("kv", "tp", None, None)),
        check_vma=False,
    )
```

```python
import jax
import jax.numpy as jnp
from jax import lax
from jax.experimental import pallas as pl
from jax.experimental.pallas import tpu as pltpu
from jax.sharding import PartitionSpec as P

D = 4096
HEADS = 16
DK = 256
DV = 512
EPS = 1e-06
F32 = jnp.float32
BF16 = jnp.bfloat16
VMEM = pl.BlockSpec(memory_space=pltpu.VMEM)
SMEM = pl.BlockSpec(memory_space=pltpu.SMEM)
HBM = pl.BlockSpec(memory_space=pltpu.HBM)


def in_hbm(value):
    return pltpu.with_memory_space_constraint(value, pltpu.HBM)


def kernel(body, outs, in_specs, name, scratch=(), limit_mib=16, out_specs=None, flops=0):
    return pl.pallas_call(
        body,
        out_shape=outs,
        in_specs=in_specs,
        out_specs=jax.tree.map(lambda _: VMEM, outs) if out_specs is None else out_specs,
        scratch_shapes=list(scratch),
        compiler_params=pltpu.CompilerParams(vmem_limit_bytes=limit_mib << 20),
        cost_estimate=pl.CostEstimate(flops=flops, transcendentals=0, bytes_accessed=0)
        if flops
        else None,
        name=name,
    )


def shape(dims, dtype):
    return jax.ShapeDtypeStruct(dims, dtype)


def swap_cores(value):
    return lax.ppermute(value, "tp", [(i, i ^ 1) for i in range(8)])


def swap_chips(value, mask):
    return lax.ppermute(value, "tp", [(i, i ^ (2 * mask)) for i in range(8)])


def squares_lanes(total, width):
    lane = lax.broadcasted_iota(jnp.int32, (total.shape[0], width), 1)
    high = total.astype(BF16).astype(F32)
    return jnp.where(lane == 0, high, jnp.where(lane == 1, total - high, 0.0)).astype(BF16)


def pack_body(where, act_hbm, mixer_hbm, channel_hbm, out, act_t, mixer, channel, sems):
    pairs = ((act_hbm, act_t), (mixer_hbm, mixer), (channel_hbm, channel))
    copies = [pltpu.make_async_copy(a, b, sems.at[i]) for i, (a, b) in enumerate(pairs)]
    for copy in copies:
        copy.start()
    for copy in copies:
        copy.wait()
    first, slot = where[0] // 4, where[0] % 4
    lane = lax.broadcasted_iota(jnp.int32, (8, 128), 1) // 32
    row = lax.broadcasted_iota(jnp.int32, (8, 128), 0)
    tiled = [jnp.concatenate([g[...].astype(F32)] * 4, axis=1) for g in (mixer, channel)]
    gains = jnp.where(row == first, tiled[0], jnp.where(row == first + 2, tiled[1], 0.0))
    gains = jnp.where(lane == slot, gains, 0.0).astype(BF16)
    rows = act_t[...]
    for j in range(8):
        out[j, :32, :] = rows
        out[j, 32:, :] = gains


def project_body(packed, wq, wk, wv, wg, terms, stream_out, gains_out, bq, bk, bv, bg, sems):
    pairs = ((wq, bq), (wk, bk), (wv, bv), (wg, bg))
    copies = [pltpu.make_async_copy(w, buf, sems.at[i]) for i, (w, buf) in enumerate(pairs)]
    for copy in copies:
        copy.start()
    stream = packed[:, :32, :].astype(F32).reshape(256, 128).T
    stream_out[...] = stream.astype(BF16)
    gains = jnp.sum(packed[:, 32:40, :].astype(F32), axis=0)
    gains_out[...] = gains
    mixer = jnp.concatenate([gains[0:1], gains[1:2]], axis=1)
    normed = (stream * mixer).astype(BF16)
    terms[:, 3072:] = squares_lanes(jnp.sum(stream * stream, axis=1, keepdims=True), 128)
    at = 0
    for copy, (_, buf) in zip(copies, pairs):
        n = buf.shape[1]
        copy.wait()
        terms[:, at : at + n] = jnp.dot(normed, buf[...], preferred_element_type=F32).astype(BF16)
        at += n


def retain_body(rates, parts, state_hbm, mixed_out, key_out, value_out, kept, state, sems):
    copies = [pltpu.make_async_copy(state_hbm.at[b], state.at[b], sems.at[b]) for b in range(8)]
    for copy in copies:
        copy.start()
    sums = jnp.sum(parts[...].astype(F32), axis=0)
    scale = lax.rsqrt((sums[:, 3072:3073] + sums[:, 3073:3074]) / D + EPS)
    query = scale * sums[:, :512]
    key = scale * sums[:, 512:1024] * DK ** (-0.5)
    value = scale * sums[:, 1024:2048]
    gate = scale * sums[:, 2048:3072]
    query_t = query.T
    key_out[...] = key.T
    value_out[...] = value
    silu = gate * jax.nn.sigmoid(gate)
    for b in range(8):
        copies[b].wait()
        for h in range(2):
            total = jnp.zeros((8, 512), F32)
            for r in range(0, 256, 64):
                qc = query_t[h * 256 + r : h * 256 + r + 64, b : b + 1]
                total = total + jnp.sum((qc * state[b, h, r : r + 64, :]).reshape(8, 8, 512), axis=0)
            kept[b : b + 1, h * 512 : (h + 1) * 512] = jnp.sum(total, axis=0, keepdims=True)
    for h in range(2):
        cols = slice(h * 512, (h + 1) * 512)
        heads = slice(h * 256, (h + 1) * 256)
        match = jnp.sum(query[:, heads] * key[:, heads], axis=1, keepdims=True)
        out = rates[h] * kept[:, cols] + match * value[:, cols]
        out = out * lax.rsqrt(jnp.mean(out * out, axis=1, keepdims=True) + EPS)
        mixed = (silu[:, cols] * out).astype(BF16)
        for j in range(16):
            mixed_out[j, :, cols] = mixed


def lift_body(parts, out):
    sums = jnp.sum(parts[...].astype(F32), axis=0)
    scale = lax.rsqrt((sums[:, 2048:2049] + sums[:, 2049:2050]) / D + EPS)
    lifted = jnp.maximum(scale * sums[:, :2048], 0.0)
    hidden = (lifted * lifted).astype(BF16)
    for j in range(16):
        out[j] = hidden


def finish_body(where, parts, middle_t, out):
    lowered = jnp.sum(parts[...].astype(F32), axis=0)
    own = middle_t[pl.ds(pl.multiple_of(where[0] * 32, 32), 32), :]
    out[...] = (own.astype(F32) + lowered).astype(BF16)


def advance_body(rates, key_t, value, state_hbm, new_hbm, state, new, in_sems, out_sems):
    reads = [pltpu.make_async_copy(state_hbm.at[b], state.at[b], in_sems.at[b]) for b in range(8)]
    writes = [pltpu.make_async_copy(new.at[b], new_hbm.at[b], out_sems.at[b]) for b in range(8)]
    for copy in reads:
        copy.start()
    for b in range(8):
        reads[b].wait()
        for h in range(2):
            row = value[b : b + 1, h * 512 : (h + 1) * 512]
            for r in range(0, 256, 64):
                kc = key_t[h * 256 + r : h * 256 + r + 64, b : b + 1]
                new[b, h, r : r + 64, :] = rates[h] * state[b, h, r : r + 64, :] + kc * row
        writes[b].start()
    for copy in writes:
        copy.wait()


def per_device(
    activations,
    mixer_gain,
    channel_gain,
    query_weight,
    key_weight,
    value_weight,
    gate_weight,
    output_weight,
    up_weight,
    down_weight,
    state_in,
):
    tp = lax.axis_index("tp")
    core = tp % 2
    heads_dev = state_in.shape[1]
    index = (tp * heads_dev + jnp.arange(heads_dev, dtype=jnp.int32)).astype(F32)
    rates = 1.0 - 2.0 ** (-1.0 - 6.0 * index / (HEADS - 1))

    where = tp.astype(jnp.int32)[None]
    where, rates = lax.optimization_barrier((where, rates))
    sources = (activations.T, mixer_gain[None], channel_gain[None])
    rows = kernel(
        pack_body,
        shape((8, 40, 128), BF16),
        [SMEM, HBM, HBM, HBM],
        "pack",
        [pltpu.VMEM(v.shape, BF16) for v in sources] + [pltpu.SemaphoreType.DMA((3,))],
    )(where, *map(in_hbm, sources))
    packed = lax.all_to_all(rows, "tp", 0, 0, tiled=True)
    weights = (query_weight, key_weight, value_weight, gate_weight)
    terms, stream, gains = kernel(
        project_body,
        (shape((128, 3200), BF16), shape((128, 256), BF16), shape((8, 128), F32)),
        [VMEM, HBM, HBM, HBM, HBM],
        "project",
        [pltpu.VMEM(w.shape, BF16) for w in weights] + [pltpu.SemaphoreType.DMA((4,))],
    )(packed, *map(in_hbm, weights))
    channel = jnp.concatenate([gains[2:3], gains[3:4]], axis=1)
    stream = stream.astype(F32)
    parts = lax.all_to_all(terms.reshape(16, 8, 3200), "kv", 0, 0, tiled=True)
    state = in_hbm(state_in)
    mixed, key_t, value = kernel(
        retain_body,
        (shape((16, 8, 1024), BF16), shape((512, 8), F32), shape((8, 1024), F32)),
        [SMEM, VMEM, HBM],
        "retain",
        [
            pltpu.VMEM((8, 1024), F32),
            pltpu.VMEM(state_in.shape, F32),
            pltpu.SemaphoreType.DMA((8,)),
        ],
    )(rates, parts, state)
    new_state = pl.pallas_call(
        advance_body,
        out_shape=jax.ShapeDtypeStruct(state_in.shape, F32),
        in_specs=[SMEM, VMEM, VMEM, HBM],
        out_specs=HBM,
        scratch_shapes=[
            pltpu.VMEM(state_in.shape, F32),
            pltpu.VMEM(state_in.shape, F32),
            pltpu.SemaphoreType.DMA((8,)),
            pltpu.SemaphoreType.DMA((8,)),
        ],
        compiler_params=pltpu.CompilerParams(vmem_limit_bytes=24 << 20),
        cost_estimate=pl.CostEstimate(flops=40_000_000, transcendentals=0, bytes_accessed=16 << 20),
        name="advance",
    )(rates, key_t, value, state)

    mixed_all = lax.all_to_all(mixed, "kv", 0, 0, tiled=True)
    mixed_all, new_state = lax.optimization_barrier((mixed_all, new_state))
    mixed_all = mixed_all.reshape(128, 1024)
    out_terms = jnp.dot(mixed_all, output_weight, preferred_element_type=F32).astype(BF16)
    halves = (out_terms[:, :128], out_terms[:, 128:])
    mine = jnp.where(core == 0, halves[0], halves[1])
    theirs = jnp.where(core == 0, halves[1], halves[0])
    pair = (mine.astype(F32) + swap_cores(theirs).astype(F32)).astype(BF16)
    quad = (pair.astype(F32) + swap_chips(pair, 1).astype(F32)).astype(BF16)
    attention = quad.astype(F32) + swap_chips(quad, 3).astype(F32)
    stream_half = jnp.where(core == 0, stream[:, :128], stream[:, 128:])
    middle_half = (stream_half + attention).astype(BF16)
    other_half = swap_cores(middle_half)
    middle_bf = jnp.concatenate(
        [
            jnp.where(core == 0, middle_half, other_half),
            jnp.where(core == 0, other_half, middle_half),
        ],
        axis=1,
    )
    middle = middle_bf.astype(F32)
    middle_squares = jnp.sum(middle * middle, axis=1, keepdims=True)
    channel_normed = (middle * channel).astype(BF16)
    up_terms = jnp.concatenate(
        [
            jnp.dot(channel_normed, up_weight, preferred_element_type=F32).astype(BF16),
            squares_lanes(middle_squares, 128),
        ],
        axis=1,
    )
    up_terms, middle_t = lax.optimization_barrier((up_terms, middle_bf.T))
    up_parts = lax.all_to_all(up_terms.reshape(16, 8, -1), "kv", 0, 0, tiled=True)
    hidden = kernel(lift_body, shape((16, 8, 2048), BF16), [VMEM], "lift")(up_parts)
    hidden_all = lax.all_to_all(hidden, "kv", 0, 0, tiled=True).reshape(128, 2048)
    down_terms = jnp.dot(hidden_all, down_weight, preferred_element_type=F32).astype(BF16)
    down_parts = lax.all_to_all(down_terms.T.reshape(8, 32, 128), "tp", 0, 0, tiled=True)
    out_t = kernel(finish_body, shape((32, 128), BF16), [SMEM, VMEM, VMEM], "finish")(
        where, down_parts, middle_t
    )
    return (out_t.T, new_state)


def solution(mesh):
    return jax.shard_map(
        per_device,
        mesh=mesh,
        in_specs=(
            P(None, ("kv", "tp")),
            P(("kv", "tp")),
            P(("kv", "tp")),
            P("kv", "tp"),
            P("kv", "tp"),
            P("kv", "tp"),
            P("kv", "tp"),
            P("tp", "kv"),
            P("kv", "tp"),
            P("tp", "kv"),
            P("kv", "tp", None, None),
        ),
        out_specs=(P(None, ("kv", "tp")), P("kv", "tp", None, None)),
        check_vma=False,
    )
```

```python
from functools import partial

import jax
import jax.numpy as jnp
from jax import lax
from jax.experimental import pallas as pl
from jax.experimental.pallas import tpu as pltpu
from jax.sharding import PartitionSpec as P

D = 4096
HEADS = 16
DK = 256
DV = 512
EPS = 1e-06
F32 = jnp.float32
BF16 = jnp.bfloat16
VMEM = pl.BlockSpec(memory_space=pltpu.VMEM)
SMEM = pl.BlockSpec(memory_space=pltpu.SMEM)
HBM = pl.BlockSpec(memory_space=pltpu.HBM)


def in_vmem(value):
    return pltpu.with_memory_space_constraint(value, pltpu.VMEM)


def in_hbm(value):
    return pltpu.with_memory_space_constraint(value, pltpu.HBM)


def kernel(body, outs, in_specs, name, scratch=(), limit_mib=16, out_specs=None, flops=0):
    return pl.pallas_call(
        body,
        out_shape=outs,
        in_specs=in_specs,
        out_specs=jax.tree.map(lambda _: VMEM, outs) if out_specs is None else out_specs,
        scratch_shapes=list(scratch),
        compiler_params=pltpu.CompilerParams(vmem_limit_bytes=limit_mib << 20),
        cost_estimate=pl.CostEstimate(flops=flops, transcendentals=0, bytes_accessed=0)
        if flops
        else None,
        name=name,
    )


def shape(dims, dtype):
    return jax.ShapeDtypeStruct(dims, dtype)


def load_body(source, out, sem):
    copy = pltpu.make_async_copy(source, out, sem)
    copy.start()
    copy.wait()


def load(array, name):
    return kernel(
        load_body,
        pltpu.VMEM(array.shape, array.dtype),
        [HBM],
        name,
        [pltpu.SemaphoreType.DMA],
        limit_mib=1,
        flops=8_000_000,
    )(in_hbm(array))


def shift_pairs(step, first):
    pairs = []
    for kv in range(16):
        z, y = kv // 4, kv % 4
        for tp in range(8):
            if (tp % 2 == 0) == first:
                to = (z + step) % 4 * 4 + y
            else:
                to = z * 4 + (y + step) % 4
            pairs.append((kv * 8 + tp, to * 8 + tp))
    return pairs


def exchange(pieces, first):
    return [
        lax.ppermute(piece, ("kv", "tp"), shift_pairs(step, first))
        for step, piece in zip((1, 3, 2), pieces)
    ]


def place(where):
    core, kv = where[0] % 2, where[1]
    z, y = kv // 4, kv % 4
    return core, jnp.where(core == 0, z, y), jnp.where(core == 0, y, z)


def send_order(where, rows, out):
    core, first, _ = place(where)
    for k, step in enumerate((0, 1, 3, 2)):
        to = (first + step) % 4
        for i in range(4):
            out[k * 4 + i] = rows[jnp.where(core == 0, to * 4 + i, i * 4 + to)]


def fold_body(width, where, own, a, b, c, kept, *outs):
    _, _, second = place(where)
    for k, step in enumerate((0, 1, 3, 2)):
        i = (second + step) % 4
        total = own[i].astype(F32) + a[i].astype(F32) + b[i].astype(F32) + c[i].astype(F32)
        squares = total[:, width : width + 1] + total[:, width + 1 : width + 2]
        if k == 0:
            kept[:, :width] = total[:, :width]
            kept[:, width:] = jnp.broadcast_to(squares, (8, 128))
        else:
            outs[k - 1][:, :width] = total[:, :width].astype(BF16)
            outs[k - 1][:, width:] = squares_lanes(squares, 128)


def fold(where, own, received, width, name):
    return kernel(
        partial(fold_body, width),
        (shape((8, width + 128), F32),) + (shape((8, width + 128), BF16),) * 3,
        [SMEM] + [VMEM] * 4,
        name,
        limit_mib=8,
    )(where, own, *received)


def total_of(width, kept, a, b, c):
    squares = kept[:, width : width + 1]
    for part in (a, b, c):
        squares = squares + part[:, width : width + 1].astype(F32)
        squares = squares + part[:, width + 1 : width + 2].astype(F32)
    total = kept[:, :width] + a[:, :width].astype(F32)
    total = total + b[:, :width].astype(F32) + c[:, :width].astype(F32)
    return total, lax.rsqrt(squares / D + EPS)


def swap_cores(value):
    return lax.ppermute(value, "tp", [(i, i ^ 1) for i in range(8)])


def swap_chips(value, mask):
    return lax.ppermute(value, "tp", [(i, i ^ (2 * mask)) for i in range(8)])


def squares_lanes(total, width):
    lane = lax.broadcasted_iota(jnp.int32, (total.shape[0], width), 1)
    high = total.astype(BF16).astype(F32)
    return jnp.where(lane == 0, high, jnp.where(lane == 1, total - high, 0.0)).astype(BF16)


def pack_body(where, act_hbm, mixer_hbm, channel_hbm, out, act_t, mixer, channel, sems):
    pairs = ((act_hbm, act_t), (mixer_hbm, mixer), (channel_hbm, channel))
    copies = [pltpu.make_async_copy(a, b, sems.at[i]) for i, (a, b) in enumerate(pairs)]
    for copy in copies:
        copy.start()
    for copy in copies:
        copy.wait()
    first, slot = where[0] // 4, where[0] % 4
    lane = lax.broadcasted_iota(jnp.int32, (8, 128), 1) // 32
    row = lax.broadcasted_iota(jnp.int32, (8, 128), 0)
    tiled = [jnp.concatenate([g[...].astype(F32)] * 4, axis=1) for g in (mixer, channel)]
    gains = jnp.where(row == first, tiled[0], jnp.where(row == first + 2, tiled[1], 0.0))
    gains = jnp.where(lane == slot, gains, 0.0).astype(BF16)
    rows = act_t[...]
    for j in range(8):
        out[j, :32, :] = rows
        out[j, 32:, :] = gains


def project_body(where, packed, *refs):
    weights, outs = refs[:4], refs[4:8]
    stream_out, gains_out = refs[8:10]
    buffers, rows, ordered, sems = refs[10:14], refs[14], refs[15], refs[16]
    copies = [pltpu.make_async_copy(weights[i], buffers[i], sems.at[i]) for i in range(4)]
    for copy in copies:
        copy.start()
    stream = packed[:, :32, :].astype(F32).reshape(256, 128).T
    stream_out[...] = stream.astype(BF16)
    gains = jnp.sum(packed[:, 32:40, :].astype(F32), axis=0)
    gains_out[...] = gains
    mixer = jnp.concatenate([gains[0:1], gains[1:2]], axis=1)
    rows[...] = stream.reshape(16, 8, 256)
    send_order(where, rows, ordered)
    stream = ordered[...].reshape(128, 256)
    normed = (stream * mixer).astype(BF16)
    squares = squares_lanes(jnp.sum(stream * stream, axis=1, keepdims=True), 128)
    squares = squares.reshape(16, 8, 128)
    for k in range(4):
        outs[k][:, :, 3072:] = squares[k * 4 : k * 4 + 4]
    at = 0
    for copy, buf in zip(copies, buffers):
        n = buf.shape[1]
        copy.wait()
        out = jnp.dot(normed, buf[...], preferred_element_type=F32).astype(BF16)
        out = out.reshape(16, 8, n)
        for k in range(4):
            outs[k][:, :, at : at + n] = out[k * 4 : k * 4 + 4]
        at += n


def retain_body(rates, own, a, b, c, state, mixed_out, key_out, value_out, kept):
    sums, scale = total_of(3072, own, a, b, c)
    query = scale * sums[:, :512]
    key = scale * sums[:, 512:1024] * DK ** (-0.5)
    value = scale * sums[:, 1024:2048]
    gate = scale * sums[:, 2048:3072]
    query_t = query.T
    key_out[...] = key.T
    value_out[...] = value
    silu = gate * jax.nn.sigmoid(gate)
    for b in range(8):
        for h in range(2):
            total = jnp.zeros((8, 512), F32)
            for r in range(0, 256, 64):
                qc = query_t[h * 256 + r : h * 256 + r + 64, b : b + 1]
                total = total + jnp.sum((qc * state[b, h, r : r + 64, :]).reshape(8, 8, 512), axis=0)
            kept[b : b + 1, h * 512 : (h + 1) * 512] = jnp.sum(total, axis=0, keepdims=True)
    for h in range(2):
        cols = slice(h * 512, (h + 1) * 512)
        heads = slice(h * 256, (h + 1) * 256)
        match = jnp.sum(query[:, heads] * key[:, heads], axis=1, keepdims=True)
        out = rates[h] * kept[:, cols] + match * value[:, cols]
        out = out * lax.rsqrt(jnp.mean(out * out, axis=1, keepdims=True) + EPS)
        mixed = (silu[:, cols] * out).astype(BF16)
        for j in range(16):
            mixed_out[j, :, cols] = mixed


def up_body(where, mine, other, gains, weight, *refs):
    outs, middle_t, rows, ordered = refs[:4], refs[4], refs[5], refs[6]
    even = where[0] % 2 == 0
    mine, other = mine[...].astype(F32), other[...].astype(F32)
    middle = jnp.concatenate(
        [jnp.where(even, mine, other), jnp.where(even, other, mine)], axis=1
    )
    middle_t[...] = middle.T.astype(BF16)
    rows[...] = middle.reshape(16, 8, 256)
    send_order(where, rows, ordered)
    middle = ordered[...].reshape(128, 256)
    channel = jnp.concatenate([gains[2:3, :], gains[3:4, :]], axis=1)
    normed = (middle * channel).astype(BF16)
    squares = squares_lanes(jnp.sum(middle * middle, axis=1, keepdims=True), 128)
    squares = squares.reshape(16, 8, 128)
    out = jnp.dot(normed, weight[...], preferred_element_type=F32).astype(BF16)
    out = out.reshape(16, 8, 2048)
    for k in range(4):
        outs[k][:, :, :2048] = out[k * 4 : k * 4 + 4]
        outs[k][:, :, 2048:] = squares[k * 4 : k * 4 + 4]


def lift_body(own, a, b, c, out):
    sums, scale = total_of(2048, own, a, b, c)
    lifted = jnp.maximum(scale * sums, 0.0)
    hidden = (lifted * lifted).astype(BF16)
    for j in range(16):
        out[j] = hidden


def finish_body(where, parts, middle_t, out):
    lowered = jnp.sum(parts[...].astype(F32), axis=0)
    own = middle_t[pl.ds(pl.multiple_of(where[0] * 32, 32), 32), :]
    out[...] = (own.astype(F32) + lowered).astype(BF16)


def advance_body(rates, key_t, value, state_hbm, new_hbm, state, new, in_sems, out_sems):
    reads = [pltpu.make_async_copy(state_hbm.at[b], state.at[b], in_sems.at[b]) for b in range(8)]
    writes = [pltpu.make_async_copy(new.at[b], new_hbm.at[b], out_sems.at[b]) for b in range(8)]
    for copy in reads:
        copy.start()
    for b in range(8):
        reads[b].wait()
        for h in range(2):
            row = value[b : b + 1, h * 512 : (h + 1) * 512]
            for r in range(0, 256, 64):
                kc = key_t[h * 256 + r : h * 256 + r + 64, b : b + 1]
                new[b, h, r : r + 64, :] = rates[h] * state[b, h, r : r + 64, :] + kc * row
        writes[b].start()
    for copy in writes:
        copy.wait()


def per_device(
    activations,
    mixer_gain,
    channel_gain,
    query_weight,
    key_weight,
    value_weight,
    gate_weight,
    output_weight,
    up_weight,
    down_weight,
    state_in,
):
    tp = lax.axis_index("tp")
    kv = lax.axis_index("kv")
    heads_dev = state_in.shape[1]
    index = (tp * heads_dev + jnp.arange(heads_dev, dtype=jnp.int32)).astype(F32)
    rates = 1.0 - 2.0 ** (-1.0 - 6.0 * index / (HEADS - 1))

    where = jnp.stack([tp, kv]).astype(jnp.int32)
    even = tp % 2 == 0
    where, rates, even = lax.optimization_barrier((where, rates, even))
    sources = (activations.T, mixer_gain[None], channel_gain[None])
    rows = kernel(
        pack_body,
        shape((8, 40, 128), BF16),
        [SMEM, HBM, HBM, HBM],
        "pack",
        [pltpu.VMEM(v.shape, BF16) for v in sources] + [pltpu.SemaphoreType.DMA((3,))],
    )(where, *map(in_hbm, sources))
    packed = lax.all_to_all(rows, "tp", 0, 0, tiled=True)
    weights = (query_weight, key_weight, value_weight, gate_weight)
    *terms, stream, gains = kernel(
        project_body,
        (shape((4, 8, 3200), BF16),) * 4 + (shape((128, 256), BF16), shape((8, 128), F32)),
        [SMEM, VMEM, HBM, HBM, HBM, HBM],
        "project",
        [pltpu.VMEM(w.shape, BF16) for w in weights]
        + [pltpu.VMEM((16, 8, 256), F32)] * 2
        + [pltpu.SemaphoreType.DMA((4,))],
    )(where, packed, *map(in_hbm, weights))
    state = load(state_in, "load_state")
    own, state = lax.optimization_barrier((terms[0], state))
    own, *parts = fold(where, own, exchange(terms[1:], True), 3072, "fold_heads")
    mixed, key_t, value = kernel(
        retain_body,
        (shape((16, 8, 1024), BF16), shape((512, 8), F32), shape((8, 1024), F32)),
        [SMEM] + [VMEM] * 5,
        "retain",
        [pltpu.VMEM((8, 1024), F32)],
        limit_mib=8,
    )(rates, own, *exchange(parts, False), in_vmem(state))
    new_state = pl.pallas_call(
        advance_body,
        out_shape=jax.ShapeDtypeStruct(state_in.shape, F32),
        in_specs=[SMEM, VMEM, VMEM, HBM],
        out_specs=HBM,
        scratch_shapes=[
            pltpu.VMEM(state_in.shape, F32),
            pltpu.VMEM(state_in.shape, F32),
            pltpu.SemaphoreType.DMA((8,)),
            pltpu.SemaphoreType.DMA((8,)),
        ],
        compiler_params=pltpu.CompilerParams(vmem_limit_bytes=24 << 20),
        cost_estimate=pl.CostEstimate(flops=40_000_000, transcendentals=0, bytes_accessed=16 << 20),
        name="advance",
    )(rates, key_t, value, in_hbm(state_in))

    mixed_all = lax.all_to_all(mixed, "kv", 0, 0, tiled=True)
    mixed_all, new_state = lax.optimization_barrier((mixed_all, new_state))
    mixed_all = mixed_all.reshape(128, 1024)
    out_terms = jnp.dot(mixed_all, output_weight, preferred_element_type=F32).astype(BF16)
    halves = (out_terms[:, :128], out_terms[:, 128:])
    mine = jnp.where(even, halves[0], halves[1])
    theirs = jnp.where(even, halves[1], halves[0])
    pair = (mine.astype(F32) + swap_cores(theirs).astype(F32)).astype(BF16)
    quad = (pair.astype(F32) + swap_chips(pair, 1).astype(F32)).astype(BF16)
    attention = quad.astype(F32) + swap_chips(quad, 3).astype(F32)
    stream_half = jnp.where(even, stream[:, :128], stream[:, 128:]).astype(F32)
    middle_half = (stream_half + attention).astype(BF16)
    *up_terms, middle_t = kernel(
        up_body,
        (shape((4, 8, 2176), BF16),) * 4 + (shape((256, 128), BF16),),
        [SMEM] + [VMEM] * 4,
        "up",
        [pltpu.VMEM((16, 8, 256), F32)] * 2,
    )(where, middle_half, swap_cores(middle_half), gains, in_vmem(load(up_weight, "load_up")))
    own, *parts = fold(where, up_terms[0], exchange(up_terms[1:], True), 2048, "fold_hidden")
    hidden = kernel(lift_body, shape((16, 8, 2048), BF16), [VMEM] * 4, "lift")(
        own, *exchange(parts, False)
    )
    hidden_all = lax.all_to_all(hidden, "kv", 0, 0, tiled=True).reshape(128, 2048)
    down_terms = jnp.dot(hidden_all, down_weight, preferred_element_type=F32).astype(BF16)
    down_parts = lax.all_to_all(down_terms.T.reshape(8, 32, 128), "tp", 0, 0, tiled=True)
    out_t = kernel(finish_body, shape((32, 128), BF16), [SMEM, VMEM, VMEM], "finish")(
        where, down_parts, middle_t
    )
    return (out_t.T, new_state)


def solution(mesh):
    return jax.shard_map(
        per_device,
        mesh=mesh,
        in_specs=(
            P(None, ("kv", "tp")),
            P(("kv", "tp")),
            P(("kv", "tp")),
            P("kv", "tp"),
            P("kv", "tp"),
            P("kv", "tp"),
            P("kv", "tp"),
            P("tp", "kv"),
            P("kv", "tp"),
            P("tp", "kv"),
            P("kv", "tp", None, None),
        ),
        out_specs=(P(None, ("kv", "tp")), P("kv", "tp", None, None)),
        check_vma=False,
    )
```

```python
from functools import partial

import jax
import jax.numpy as jnp
from jax import lax
from jax.experimental import pallas as pl
from jax.experimental.pallas import tpu as pltpu
from jax.sharding import PartitionSpec as P

D = 4096
HEADS = 16
DK = 256
DV = 512
EPS = 1e-06
DECAYS = [float(1.0 - 2.0 ** (-1.0 - 6.0 * h / (HEADS - 1))) for h in range(HEADS)]
F32 = jnp.float32
BF16 = jnp.bfloat16
VMEM = pl.BlockSpec(memory_space=pltpu.VMEM)
SMEM = pl.BlockSpec(memory_space=pltpu.SMEM)
HBM = pl.BlockSpec(memory_space=pltpu.HBM)


def in_vmem(value):
    return pltpu.with_memory_space_constraint(value, pltpu.VMEM)


def in_hbm(value):
    return pltpu.with_memory_space_constraint(value, pltpu.HBM)


def kernel(body, outs, in_specs, name, scratch=(), limit_mib=16, out_specs=None, flops=0):
    return pl.pallas_call(
        body,
        out_shape=outs,
        in_specs=in_specs,
        out_specs=jax.tree.map(lambda _: VMEM, outs) if out_specs is None else out_specs,
        scratch_shapes=list(scratch),
        compiler_params=pltpu.CompilerParams(vmem_limit_bytes=limit_mib << 20),
        cost_estimate=pl.CostEstimate(flops=flops, transcendentals=0, bytes_accessed=0)
        if flops
        else None,
        name=name,
    )


def shape(dims, dtype):
    return jax.ShapeDtypeStruct(dims, dtype)


def load_body(*refs):
    count = len(refs) // 2
    sems = refs[-1]
    copies = [
        pltpu.make_async_copy(refs[i], refs[count + i], sems.at[i]) for i in range(count)
    ]
    for copy in copies:
        copy.start()
    for copy in copies:
        copy.wait()


def load(arrays, name):
    return kernel(
        load_body,
        tuple(pltpu.VMEM(a.shape, a.dtype) for a in arrays),
        [HBM] * len(arrays),
        name,
        [pltpu.SemaphoreType.DMA((len(arrays),))],
        limit_mib=1,
        flops=8_000_000,
    )(*map(in_hbm, arrays))


def shift_pairs(step, first):
    pairs = []
    for kv in range(16):
        z, y = kv // 4, kv % 4
        for tp in range(8):
            if (tp % 2 == 0) == first:
                to = (z + step) % 4 * 4 + y
            else:
                to = z * 4 + (y + step) % 4
            pairs.append((kv * 8 + tp, to * 8 + tp))
    return pairs


def exchange(pieces, first):
    return [
        lax.ppermute(piece, ("kv", "tp"), shift_pairs(step, first))
        for step, piece in zip((1, 3, 2), pieces)
    ]


def place(where, kv_at):
    core, kv = where[0] % 2, kv_at[0]
    z, y = kv // 4, kv % 4
    return core, jnp.where(core == 0, z, y), jnp.where(core == 0, y, z)


def send_order(where, kv_at, rows, out):
    core, first, _ = place(where, kv_at)
    for k, step in enumerate((0, 1, 3, 2)):
        to = (first + step) % 4
        for i in range(4):
            out[k * 4 + i] = rows[jnp.where(core == 0, to * 4 + i, i * 4 + to)]


def fold_body(width, where, kv_at, own, a, b, c, kept, *outs):
    _, _, second = place(where, kv_at)
    for k, step in enumerate((0, 1, 3, 2)):
        i = (second + step) % 4
        total = own[i].astype(F32) + a[i].astype(F32) + b[i].astype(F32) + c[i].astype(F32)
        squares = total[:, width : width + 1] + total[:, width + 1 : width + 2]
        if k == 0:
            kept[:, :width] = total[:, :width]
            kept[:, width:] = jnp.broadcast_to(squares, (8, 128))
        else:
            outs[k - 1][:, :width] = total[:, :width].astype(BF16)
            outs[k - 1][:, width:] = squares_lanes(squares, 128)


def total_of(width, kept, a, b, c):
    squares = kept[:, width : width + 1]
    for part in (a, b, c):
        squares = squares + part[:, width : width + 1].astype(F32)
        squares = squares + part[:, width + 1 : width + 2].astype(F32)
    total = kept[:, :width] + a[:, :width].astype(F32)
    total = total + b[:, :width].astype(F32) + c[:, :width].astype(F32)
    return total, lax.rsqrt(squares / D + EPS)


def swap_cores(value):
    return lax.ppermute(value, "tp", [(i, i ^ 1) for i in range(8)])


def swap_chips(value, mask):
    return lax.ppermute(value, "tp", [(i, i ^ (2 * mask)) for i in range(8)])


def squares_lanes(total, width):
    lane = lax.broadcasted_iota(jnp.int32, (total.shape[0], width), 1)
    high = total.astype(BF16).astype(F32)
    return jnp.where(lane == 0, high, jnp.where(lane == 1, total - high, 0.0)).astype(BF16)


def pack_body(where, act_hbm, mixer_hbm, channel_hbm, out, act_t, mixer, channel, sems):
    pairs = ((act_hbm, act_t), (mixer_hbm, mixer), (channel_hbm, channel))
    copies = [pltpu.make_async_copy(a, b, sems.at[i]) for i, (a, b) in enumerate(pairs)]
    for copy in copies:
        copy.start()
    for copy in copies:
        copy.wait()
    first, slot = where[0] // 4, where[0] % 4
    lane = lax.broadcasted_iota(jnp.int32, (8, 128), 1) // 32
    row = lax.broadcasted_iota(jnp.int32, (8, 128), 0)
    tiled = [jnp.concatenate([g[...].astype(F32)] * 4, axis=1) for g in (mixer, channel)]
    gains = jnp.where(row == first, tiled[0], jnp.where(row == first + 2, tiled[1], 0.0))
    gains = jnp.where(lane == slot, gains, 0.0).astype(BF16)
    rows = act_t[...]
    for j in range(8):
        out[j, :32, :] = rows
        out[j, 32:, :] = gains


def rate_of(where, h):
    rate = jnp.float32(DECAYS[h])
    for t in range(1, 8):
        rate = jnp.where(where[0] == t, jnp.float32(DECAYS[2 * t + h]), rate)
    return rate


def project_body(where, kv_at, packed, *refs):
    weights, outs = refs[:4], refs[4:8]
    stream_out, gains_out = refs[8:10]
    buffers, rows, ordered, sems = refs[10:14], refs[14], refs[15], refs[16]
    copies = [pltpu.make_async_copy(weights[i], buffers[i], sems.at[i]) for i in range(4)]
    for copy in copies:
        copy.start()
    stream = packed[:, :32, :].astype(F32).reshape(256, 128).T
    stream_out[...] = stream.astype(BF16)
    gains = jnp.sum(packed[:, 32:40, :].astype(F32), axis=0)
    gains_out[...] = gains
    mixer = jnp.concatenate([gains[0:1], gains[1:2]], axis=1)
    rows[...] = stream.reshape(16, 8, 256)
    send_order(where, kv_at, rows, ordered)
    stream = ordered[...].reshape(128, 256)
    normed = (stream * mixer).astype(BF16)
    squares = squares_lanes(jnp.sum(stream * stream, axis=1, keepdims=True), 128)
    squares = squares.reshape(16, 8, 128)
    for k in range(4):
        outs[k][:, :, 3072:] = squares[k * 4 : k * 4 + 4]
    at = 0
    for copy, buf in zip(copies, buffers):
        n = buf.shape[1]
        copy.wait()
        out = jnp.dot(normed, buf[...], preferred_element_type=F32).astype(BF16)
        out = out.reshape(16, 8, n)
        for k in range(4):
            outs[k][:, :, at : at + n] = out[k * 4 : k * 4 + 4]
        at += n


def retain_body(where, own, a, b, c, state, mixed_out, key_out, value_out, kept):
    sums, scale = total_of(3072, own, a, b, c)
    query = scale * sums[:, :512]
    key = scale * sums[:, 512:1024] * DK ** (-0.5)
    value = scale * sums[:, 1024:2048]
    gate = scale * sums[:, 2048:3072]
    query_t = query.T
    key_out[...] = key.T
    value_out[...] = value
    silu = gate * jax.nn.sigmoid(gate)
    for b in range(8):
        for h in range(2):
            total = jnp.zeros((8, 512), F32)
            for r in range(0, 256, 64):
                qc = query_t[h * 256 + r : h * 256 + r + 64, b : b + 1]
                total = total + jnp.sum((qc * state[b, h, r : r + 64, :]).reshape(8, 8, 512), axis=0)
            kept[b : b + 1, h * 512 : (h + 1) * 512] = jnp.sum(total, axis=0, keepdims=True)
    for h in range(2):
        cols = slice(h * 512, (h + 1) * 512)
        heads = slice(h * 256, (h + 1) * 256)
        match = jnp.sum(query[:, heads] * key[:, heads], axis=1, keepdims=True)
        out = rate_of(where, h) * kept[:, cols] + match * value[:, cols]
        out = out * lax.rsqrt(jnp.mean(out * out, axis=1, keepdims=True) + EPS)
        mixed = (silu[:, cols] * out).astype(BF16)
        for j in range(16):
            mixed_out[j, :, cols] = mixed


def out_body(where, mixed, weight, mine_out, theirs_out):
    out = jnp.dot(mixed[...].reshape(128, 1024), weight[...], preferred_element_type=F32)
    out = out.astype(BF16)
    even = where[0] % 2 == 0
    mine_out[...] = jnp.where(even, out[:, :128], out[:, 128:])
    theirs_out[...] = jnp.where(even, out[:, 128:], out[:, :128])


def add_body(a, b, out):
    out[...] = (a[...].astype(F32) + b[...].astype(F32)).astype(BF16)


def middle_body(where, stream, a, b, out):
    attention = a[...].astype(F32) + b[...].astype(F32)
    own = jnp.where(where[0] % 2 == 0, stream[:, :128], stream[:, 128:])
    out[...] = (own.astype(F32) + attention).astype(BF16)


def up_body(where, mine, other, gains, weight, out, middle_t):
    even = where[0] % 2 == 0
    mine, other = mine[...].astype(F32), other[...].astype(F32)
    middle = jnp.concatenate(
        [jnp.where(even, mine, other), jnp.where(even, other, mine)], axis=1
    )
    middle_t[...] = middle.T.astype(BF16)
    channel = jnp.concatenate([gains[2:3, :], gains[3:4, :]], axis=1)
    normed = (middle * channel).astype(BF16)
    out[:, 2048:] = squares_lanes(jnp.sum(middle * middle, axis=1, keepdims=True), 128)
    out[:, :2048] = jnp.dot(normed, weight[...], preferred_element_type=F32).astype(BF16)


def lift_body(parts, out):
    sums = jnp.sum(parts[...].astype(F32), axis=0)
    scale = lax.rsqrt((sums[:, 2048:2049] + sums[:, 2049:2050]) / D + EPS)
    lifted = jnp.maximum(scale * sums[:, :2048], 0.0)
    hidden = (lifted * lifted).astype(BF16)
    for j in range(16):
        out[j] = hidden


def finish_body(where, parts, middle_t, out):
    lowered = jnp.sum(parts[...].astype(F32), axis=0)
    own = middle_t[pl.ds(pl.multiple_of(where[0] * 32, 32), 32), :]
    out[...] = (own.astype(F32) + lowered).astype(BF16)


def advance_body(half, where, key_t, value, state, *refs):
    new_hbm, new, sems = refs[-3:]
    writes = []
    for i in range(4):
        b = half * 4 + i
        for h in range(2):
            rate = rate_of(where, h)
            row = value[b : b + 1, h * 512 : (h + 1) * 512]
            for r in range(0, 256, 64):
                kc = key_t[h * 256 + r : h * 256 + r + 64, b : b + 1]
                new[i, h, r : r + 64, :] = rate * state[b, h, r : r + 64, :] + kc * row
        copy = pltpu.make_async_copy(new.at[i], new_hbm.at[b], sems.at[i])
        copy.start()
        writes.append(copy)
    for copy in writes:
        copy.wait()


def advance(half, where, key_t, value, state, new_state=None):
    before = [] if new_state is None else [new_state]
    return pl.pallas_call(
        partial(advance_body, half),
        out_shape=shape(state.shape, F32),
        in_specs=[SMEM, VMEM, VMEM, VMEM] + [HBM] * len(before),
        out_specs=HBM,
        scratch_shapes=[pltpu.VMEM((4,) + state.shape[1:], F32), pltpu.SemaphoreType.DMA((4,))],
        input_output_aliases={4: 0} if before else {},
        compiler_params=pltpu.CompilerParams(vmem_limit_bytes=8 << 20),
        cost_estimate=pl.CostEstimate(flops=20_000_000, transcendentals=0, bytes_accessed=8 << 20),
        name="advance_" + str(half),
    )(where, key_t, value, in_vmem(state), *before)


def per_device(
    activations,
    mixer_gain,
    channel_gain,
    query_weight,
    key_weight,
    value_weight,
    gate_weight,
    output_weight,
    up_weight,
    down_weight,
    state_in,
):
    where = lax.axis_index("tp").astype(jnp.int32)[None]
    kv_at = lax.axis_index("kv").astype(jnp.int32)[None]
    where, kv_at = lax.optimization_barrier((where, kv_at))
    sources = (activations.T, mixer_gain[None], channel_gain[None])
    rows = kernel(
        pack_body,
        shape((8, 40, 128), BF16),
        [SMEM, HBM, HBM, HBM],
        "pack",
        [pltpu.VMEM(v.shape, BF16) for v in sources] + [pltpu.SemaphoreType.DMA((3,))],
    )(where, *map(in_hbm, sources))
    packed = lax.all_to_all(rows, "tp", 0, 0, tiled=True)
    weights = (query_weight, key_weight, value_weight, gate_weight)
    *terms, stream, gains = kernel(
        project_body,
        (shape((4, 8, 3200), BF16),) * 4 + (shape((128, 256), BF16), shape((8, 128), F32)),
        [SMEM, SMEM, VMEM, HBM, HBM, HBM, HBM],
        "project",
        [pltpu.VMEM(w.shape, BF16) for w in weights]
        + [pltpu.VMEM((16, 8, 256), F32)] * 2
        + [pltpu.SemaphoreType.DMA((4,))],
    )(where, kv_at, packed, *map(in_hbm, weights))
    state, out_w = load((state_in, output_weight), "load_early")
    own, state, out_w = lax.optimization_barrier((terms[0], state, out_w))
    own, *parts = kernel(
        partial(fold_body, 3072),
        (shape((8, 3200), F32),) + (shape((8, 3200), BF16),) * 3,
        [SMEM, SMEM] + [VMEM] * 4,
        "fold",
        limit_mib=8,
    )(where, kv_at, own, *exchange(terms[1:], True))
    mixed, key_t, value = kernel(
        retain_body,
        (shape((16, 8, 1024), BF16), shape((512, 8), F32), shape((8, 1024), F32)),
        [SMEM] + [VMEM] * 5,
        "retain",
        [pltpu.VMEM((8, 1024), F32)],
        limit_mib=8,
    )(where, own, *exchange(parts, False), in_vmem(state))
    mixed_all = lax.all_to_all(mixed, "kv", 0, 0, tiled=True)

    half = shape((128, 128), BF16)
    mine, theirs = kernel(out_body, (half, half), [SMEM, VMEM, VMEM], "out", limit_mib=4)(
        where, mixed_all, in_vmem(out_w)
    )
    pair = kernel(add_body, half, [VMEM] * 2, "add_pair", limit_mib=1)(mine, swap_cores(theirs))
    received = swap_chips(pair, 1)
    new_state = advance(0, where, key_t, value, state)
    received, new_state = lax.optimization_barrier((received, new_state))
    quad = kernel(add_body, half, [VMEM] * 2, "add_quad", limit_mib=1)(pair, received)
    received = swap_chips(quad, 3)
    new_state = advance(1, where, key_t, value, state, new_state)
    received, new_state = lax.optimization_barrier((received, new_state))
    middle_half = kernel(middle_body, half, [SMEM] + [VMEM] * 3, "middle", limit_mib=1)(
        where, stream, quad, received
    )
    up_w = load((up_weight,), "load_up")[0]
    up_terms, middle_t = kernel(
        up_body,
        (shape((128, 2176), BF16), shape((256, 128), BF16)),
        [SMEM] + [VMEM] * 4,
        "up",
        limit_mib=4,
    )(where, middle_half, swap_cores(middle_half), gains, in_vmem(up_w))
    up_parts = lax.all_to_all(up_terms.reshape(16, 8, 2176), "kv", 0, 0, tiled=True)
    hidden = kernel(lift_body, shape((16, 8, 2048), BF16), [VMEM], "lift", limit_mib=4)(up_parts)
    hidden_all = lax.all_to_all(hidden, "kv", 0, 0, tiled=True).reshape(128, 2048)
    down_terms = jnp.dot(hidden_all, down_weight, preferred_element_type=F32).astype(BF16)
    down_parts = lax.all_to_all(down_terms.T.reshape(8, 32, 128), "tp", 0, 0, tiled=True)
    out_t = kernel(finish_body, shape((32, 128), BF16), [SMEM, VMEM, VMEM], "finish")(
        where, down_parts, middle_t
    )
    return (out_t.T, new_state)


def solution(mesh):
    return jax.shard_map(
        per_device,
        mesh=mesh,
        in_specs=(
            P(None, ("kv", "tp")),
            P(("kv", "tp")),
            P(("kv", "tp")),
            P("kv", "tp"),
            P("kv", "tp"),
            P("kv", "tp"),
            P("kv", "tp"),
            P("tp", "kv"),
            P("kv", "tp"),
            P("tp", "kv"),
            P("kv", "tp", None, None),
        ),
        out_specs=(P(None, ("kv", "tp")), P("kv", "tp", None, None)),
        check_vma=False,
    )
```

```python
from functools import partial

import jax
import jax.numpy as jnp
from jax import lax
from jax.experimental import pallas as pl
from jax.experimental.pallas import tpu as pltpu
from jax.sharding import PartitionSpec as P

D = 4096
HEADS = 16
DK = 256
DV = 512
EPS = 1e-06
DECAYS = [float(1.0 - 2.0 ** (-1.0 - 6.0 * h / (HEADS - 1))) for h in range(HEADS)]
F32 = jnp.float32
BF16 = jnp.bfloat16
VMEM = pl.BlockSpec(memory_space=pltpu.VMEM)
SMEM = pl.BlockSpec(memory_space=pltpu.SMEM)
HBM = pl.BlockSpec(memory_space=pltpu.HBM)


def in_vmem(value):
    return pltpu.with_memory_space_constraint(value, pltpu.VMEM)


def in_hbm(value):
    return pltpu.with_memory_space_constraint(value, pltpu.HBM)


def kernel(body, outs, in_specs, name, scratch=(), limit_mib=16, out_specs=None, flops=0):
    return pl.pallas_call(
        body,
        out_shape=outs,
        in_specs=in_specs,
        out_specs=jax.tree.map(lambda _: VMEM, outs) if out_specs is None else out_specs,
        scratch_shapes=list(scratch),
        compiler_params=pltpu.CompilerParams(vmem_limit_bytes=limit_mib << 20),
        cost_estimate=pl.CostEstimate(flops=flops, transcendentals=0, bytes_accessed=0)
        if flops
        else None,
        name=name,
    )


def shape(dims, dtype):
    return jax.ShapeDtypeStruct(dims, dtype)


def load_body(*refs):
    count = len(refs) // 2
    sems = refs[-1]
    copies = [
        pltpu.make_async_copy(refs[i], refs[count + i], sems.at[i]) for i in range(count)
    ]
    for copy in copies:
        copy.start()
    for copy in copies:
        copy.wait()


def load(arrays, name):
    return kernel(
        load_body,
        tuple(pltpu.VMEM(a.shape, a.dtype) for a in arrays),
        [HBM] * len(arrays),
        name,
        [pltpu.SemaphoreType.DMA((len(arrays),))],
        limit_mib=1,
        flops=8_000_000,
    )(*map(in_hbm, arrays))


def shift_pairs(step, first):
    pairs = []
    for kv in range(16):
        z, y = kv // 4, kv % 4
        for tp in range(8):
            if (tp % 2 == 0) == first:
                to = (z + step) % 4 * 4 + y
            else:
                to = z * 4 + (y + step) % 4
            pairs.append((kv * 8 + tp, to * 8 + tp))
    return pairs


def exchange(pieces, first):
    return [
        lax.ppermute(piece, ("kv", "tp"), shift_pairs(step, first))
        for step, piece in zip((1, 3, 2), pieces)
    ]


def place(where, kv_at):
    core, kv = where[0] % 2, kv_at[0]
    z, y = kv // 4, kv % 4
    return core, jnp.where(core == 0, z, y), jnp.where(core == 0, y, z)


def send_order(where, kv_at, rows, out):
    core, first, _ = place(where, kv_at)
    for k, step in enumerate((0, 1, 3, 2)):
        to = (first + step) % 4
        for i in range(4):
            out[k * 4 + i] = rows[jnp.where(core == 0, to * 4 + i, i * 4 + to)]


def fold_body(width, where, kv_at, own, a, b, c, kept, *outs):
    _, _, second = place(where, kv_at)
    for k, step in enumerate((0, 1, 3, 2)):
        i = (second + step) % 4
        total = own[i].astype(F32) + a[i].astype(F32) + b[i].astype(F32) + c[i].astype(F32)
        squares = total[:, width : width + 1] + total[:, width + 1 : width + 2]
        if k == 0:
            kept[:, :width] = total[:, :width]
            kept[:, width:] = jnp.broadcast_to(squares, (8, 128))
        else:
            outs[k - 1][:, :width] = total[:, :width].astype(BF16)
            outs[k - 1][:, width:] = squares_lanes(squares, 128)


def total_of(width, kept, a, b, c):
    squares = kept[:, width : width + 1]
    for part in (a, b, c):
        squares = squares + part[:, width : width + 1].astype(F32)
        squares = squares + part[:, width + 1 : width + 2].astype(F32)
    total = kept[:, :width] + a[:, :width].astype(F32)
    total = total + b[:, :width].astype(F32) + c[:, :width].astype(F32)
    return total, lax.rsqrt(squares / D + EPS)


def to_core(value, core):
    return lax.ppermute(value, "tp", [(i ^ 1, i) for i in range(core, 8, 2)])


def swap_chips(value, mask):
    return lax.ppermute(value, "tp", [(i, i ^ (2 * mask)) for i in range(1, 8, 2)])


def load_body(*refs):
    count = len(refs) // 2
    sems = refs[-1]
    copies = [
        pltpu.make_async_copy(refs[i], refs[count + i], sems.at[i]) for i in range(count)
    ]
    for copy in copies:
        copy.start()
    for copy in copies:
        copy.wait()


def load(arrays, name):
    return kernel(
        load_body,
        tuple(pltpu.VMEM(a.shape, a.dtype) for a in arrays),
        [HBM] * len(arrays),
        name,
        [pltpu.SemaphoreType.DMA((len(arrays),))],
        limit_mib=1,
        flops=8_000_000,
    )(*map(in_hbm, arrays))


def shift_pairs(step, first):
    pairs = []
    for kv in range(16):
        z, y = kv // 4, kv % 4
        for tp in range(8):
            if (tp % 2 == 0) == first:
                to = (z + step) % 4 * 4 + y
            else:
                to = z * 4 + (y + step) % 4
            pairs.append((kv * 8 + tp, to * 8 + tp))
    return pairs


def exchange(pieces, first):
    return [
        lax.ppermute(piece, ("kv", "tp"), shift_pairs(step, first))
        for step, piece in zip((1, 3, 2), pieces)
    ]


def place(where, kv_at):
    core, kv = where[0] % 2, kv_at[0]
    z, y = kv // 4, kv % 4
    return core, jnp.where(core == 0, z, y), jnp.where(core == 0, y, z)


def send_order(where, kv_at, rows, out):
    core, first, _ = place(where, kv_at)
    for k, step in enumerate((0, 1, 3, 2)):
        to = (first + step) % 4
        for i in range(4):
            out[k * 4 + i] = rows[jnp.where(core == 0, to * 4 + i, i * 4 + to)]


def fold_body(width, where, kv_at, own, a, b, c, kept, *outs):
    _, _, second = place(where, kv_at)
    for k, step in enumerate((0, 1, 3, 2)):
        i = (second + step) % 4
        total = own[i].astype(F32) + a[i].astype(F32) + b[i].astype(F32) + c[i].astype(F32)
        squares = total[:, width : width + 1] + total[:, width + 1 : width + 2]
        if k == 0:
            kept[:, :width] = total[:, :width]
            kept[:, width:] = jnp.broadcast_to(squares, (8, 128))
        else:
            outs[k - 1][:, :width] = total[:, :width].astype(BF16)
            outs[k - 1][:, width:] = squares_lanes(squares, 128)


def total_of(width, kept, a, b, c):
    squares = kept[:, width : width + 1]
    for part in (a, b, c):
        squares = squares + part[:, width : width + 1].astype(F32)
        squares = squares + part[:, width + 1 : width + 2].astype(F32)
    total = kept[:, :width] + a[:, :width].astype(F32)
    total = total + b[:, :width].astype(F32) + c[:, :width].astype(F32)
    return total, lax.rsqrt(squares / D + EPS)


def swap_cores(value):
    return lax.ppermute(value, "tp", [(i, i ^ 1) for i in range(8)])


def swap_chips(value, mask):
    return lax.ppermute(value, "tp", [(i, i ^ (2 * mask)) for i in range(8)])


def squares_lanes(total, width):
    lane = lax.broadcasted_iota(jnp.int32, (total.shape[0], width), 1)
    high = total.astype(BF16).astype(F32)
    return jnp.where(lane == 0, high, jnp.where(lane == 1, total - high, 0.0)).astype(BF16)


def pack_body(where, act_hbm, mixer_hbm, channel_hbm, wq, wk, wv, wg, out, *refs):
    weights, (act_t, mixer, channel, sems) = refs[:4], refs[4:]
    pairs = ((act_hbm, act_t), (mixer_hbm, mixer), (channel_hbm, channel))
    pairs += tuple(zip((wq, wk, wv, wg), weights))
    copies = [pltpu.make_async_copy(a, b, sems.at[i]) for i, (a, b) in enumerate(pairs)]
    for copy in copies:
        copy.start()
    for copy in copies[:3]:
        copy.wait()
    first, slot = where[0] // 4, where[0] % 4
    lane = lax.broadcasted_iota(jnp.int32, (8, 128), 1) // 32
    row = lax.broadcasted_iota(jnp.int32, (8, 128), 0)
    tiled = [jnp.concatenate([g[...].astype(F32)] * 4, axis=1) for g in (mixer, channel)]
    gains = jnp.where(row == first, tiled[0], jnp.where(row == first + 2, tiled[1], 0.0))
    gains = jnp.where(lane == slot, gains, 0.0).astype(BF16)
    rows = act_t[...]
    for j in range(8):
        out[j, :32, :] = rows
        out[j, 32:, :] = gains
    for copy in copies[3:]:
        copy.wait()


def rate_of(where, h):
    rate = jnp.float32(DECAYS[h])
    for t in range(1, 8):
        rate = jnp.where(where[0] == t, jnp.float32(DECAYS[2 * t + h]), rate)
    return rate


def project_body(where, kv_at, packed, *refs):
    weights, outs = refs[:4], refs[4:8]
    stream_out, gains_out, rows, ordered = refs[8:]
    stream = packed[:, :32, :].astype(F32).reshape(256, 128).T
    stream_out[...] = stream.astype(BF16)
    gains = jnp.sum(packed[:, 32:40, :].astype(F32), axis=0)
    gains_out[...] = gains
    mixer = jnp.concatenate([gains[0:1], gains[1:2]], axis=1)
    rows[...] = stream.reshape(16, 8, 256)
    send_order(where, kv_at, rows, ordered)
    stream = ordered[...].reshape(128, 256)
    normed = (stream * mixer).astype(BF16)
    squares = squares_lanes(jnp.sum(stream * stream, axis=1, keepdims=True), 128)
    squares = squares.reshape(16, 8, 128)
    for k in range(4):
        outs[k][:, :, 3072:] = squares[k * 4 : k * 4 + 4]
    at = 0
    for weight in weights:
        n = weight.shape[1]
        out = jnp.dot(normed, weight[...], preferred_element_type=F32).astype(BF16)
        out = out.reshape(16, 8, n)
        for k in range(4):
            outs[k][:, :, at : at + n] = out[k * 4 : k * 4 + 4]
        at += n


def retain_body(where, own, a, b, c, state, mixed_out, key_out, value_out, kept):
    sums, scale = total_of(3072, own, a, b, c)
    query = scale * sums[:, :512]
    key = scale * sums[:, 512:1024] * DK ** (-0.5)
    value = scale * sums[:, 1024:2048]
    gate = scale * sums[:, 2048:3072]
    query_t = query.T
    key_out[...] = key.T
    value_out[...] = value
    silu = gate * jax.nn.sigmoid(gate)
    for b in range(8):
        for h in range(2):
            total = jnp.zeros((8, 512), F32)
            for r in range(0, 256, 64):
                qc = query_t[h * 256 + r : h * 256 + r + 64, b : b + 1]
                total = total + jnp.sum((qc * state[b, h, r : r + 64, :]).reshape(8, 8, 512), axis=0)
            kept[b : b + 1, h * 512 : (h + 1) * 512] = jnp.sum(total, axis=0, keepdims=True)
    for h in range(2):
        cols = slice(h * 512, (h + 1) * 512)
        heads = slice(h * 256, (h + 1) * 256)
        match = jnp.sum(query[:, heads] * key[:, heads], axis=1, keepdims=True)
        out = rate_of(where, h) * kept[:, cols] + match * value[:, cols]
        out = out * lax.rsqrt(jnp.mean(out * out, axis=1, keepdims=True) + EPS)
        mixed = (silu[:, cols] * out).astype(BF16)
        for j in range(16):
            mixed_out[j, :, cols] = mixed


def out_body(mixed, weight, out):
    terms = jnp.dot(mixed[...].reshape(128, 1024), weight[...], preferred_element_type=F32)
    out[...] = terms.astype(BF16)


def add_body(*refs):
    out = refs[-1]
    out[...] = sum(ref[...].astype(F32) for ref in refs[:-1]).astype(BF16)


def up_body(where, mine, other, gains, weight, out, middle_t):
    odd = where[0] % 2 == 1
    middle = jnp.where(odd, mine[...].astype(F32), other[...].astype(F32))
    middle_t[...] = middle.T.astype(BF16)
    channel = jnp.concatenate([gains[2:3, :], gains[3:4, :]], axis=1)
    normed = (middle * channel).astype(BF16)
    out[:, 2048:] = squares_lanes(jnp.sum(middle * middle, axis=1, keepdims=True), 128)
    out[:, :2048] = jnp.dot(normed, weight[...], preferred_element_type=F32).astype(BF16)


def lift_body(parts, out):
    sums = jnp.sum(parts[...].astype(F32), axis=0)
    scale = lax.rsqrt((sums[:, 2048:2049] + sums[:, 2049:2050]) / D + EPS)
    lifted = jnp.maximum(scale * sums[:, :2048], 0.0)
    hidden = (lifted * lifted).astype(BF16)
    for j in range(16):
        out[j] = hidden


def finish_body(where, parts, middle_t, out):
    lowered = jnp.sum(parts[...].astype(F32), axis=0)
    own = middle_t[pl.ds(pl.multiple_of(where[0] * 32, 32), 32), :]
    out[...] = (own.astype(F32) + lowered).astype(BF16)


def advance_body(half, where, key_t, value, state, *refs):
    new_hbm, new, sems = refs[-3:]
    writes = []
    for i in range(4):
        b = half * 4 + i
        for h in range(2):
            rate = rate_of(where, h)
            row = value[b : b + 1, h * 512 : (h + 1) * 512]
            for r in range(0, 256, 64):
                kc = key_t[h * 256 + r : h * 256 + r + 64, b : b + 1]
                new[i, h, r : r + 64, :] = rate * state[b, h, r : r + 64, :] + kc * row
        copy = pltpu.make_async_copy(new.at[i], new_hbm.at[b], sems.at[i])
        copy.start()
        writes.append(copy)
    for copy in writes:
        copy.wait()


def advance(half, where, key_t, value, state, new_state=None):
    before = [] if new_state is None else [new_state]
    return pl.pallas_call(
        partial(advance_body, half),
        out_shape=shape(state.shape, F32),
        in_specs=[SMEM, VMEM, VMEM, VMEM] + [HBM] * len(before),
        out_specs=HBM,
        scratch_shapes=[pltpu.VMEM((4,) + state.shape[1:], F32), pltpu.SemaphoreType.DMA((4,))],
        input_output_aliases={4: 0} if before else {},
        compiler_params=pltpu.CompilerParams(vmem_limit_bytes=8 << 20),
        cost_estimate=pl.CostEstimate(flops=20_000_000, transcendentals=0, bytes_accessed=8 << 20),
        name="advance_" + str(half),
    )(where, key_t, value, in_vmem(state), *before)


def per_device(
    activations,
    mixer_gain,
    channel_gain,
    query_weight,
    key_weight,
    value_weight,
    gate_weight,
    output_weight,
    up_weight,
    down_weight,
    state_in,
):
    where = lax.axis_index("tp").astype(jnp.int32)[None]
    kv_at = lax.axis_index("kv").astype(jnp.int32)[None]
    where, kv_at = lax.optimization_barrier((where, kv_at))
    sources = (activations.T, mixer_gain[None], channel_gain[None])
    weights = (query_weight, key_weight, value_weight, gate_weight)
    rows, *weights = kernel(
        pack_body,
        (shape((8, 40, 128), BF16),) + tuple(pltpu.VMEM(w.shape, BF16) for w in weights),
        [SMEM] + [HBM] * 7,
        "pack",
        [pltpu.VMEM(v.shape, BF16) for v in sources] + [pltpu.SemaphoreType.DMA((7,))],
        limit_mib=1,
    )(where, *map(in_hbm, sources + weights))
    packed = lax.all_to_all(rows, "tp", 0, 0, tiled=True)
    *terms, stream, gains = kernel(
        project_body,
        (shape((4, 8, 3200), BF16),) * 4 + (shape((128, 256), BF16), shape((8, 128), F32)),
        [SMEM, SMEM] + [VMEM] * 5,
        "project",
        [pltpu.VMEM((16, 8, 256), F32)] * 2,
        limit_mib=8,
    )(where, kv_at, packed, *map(in_vmem, weights))
    state, out_w = load((state_in, output_weight), "load_early")
    own, state, out_w = lax.optimization_barrier((terms[0], state, out_w))
    own, *parts = kernel(
        partial(fold_body, 3072),
        (shape((8, 3200), F32),) + (shape((8, 3200), BF16),) * 3,
        [SMEM, SMEM] + [VMEM] * 4,
        "fold",
        limit_mib=8,
    )(where, kv_at, own, *exchange(terms[1:], True))
    mixed, key_t, value = kernel(
        retain_body,
        (shape((16, 8, 1024), BF16), shape((512, 8), F32), shape((8, 1024), F32)),
        [SMEM] + [VMEM] * 5,
        "retain",
        [pltpu.VMEM((8, 1024), F32)],
        limit_mib=8,
    )(where, own, *exchange(parts, False), in_vmem(state))
    mixed_all = lax.all_to_all(mixed, "kv", 0, 0, tiled=True)

    block = shape((128, 256), BF16)
    terms = kernel(out_body, block, [VMEM] * 2, "out", limit_mib=4)(mixed_all, in_vmem(out_w))
    pair = kernel(add_body, block, [VMEM] * 2, "add_pair", limit_mib=1)(terms, to_core(terms, 1))
    received = swap_chips(pair, 1)
    new_state = advance(0, where, key_t, value, state)
    received, new_state = lax.optimization_barrier((received, new_state))
    quad = kernel(add_body, block, [VMEM] * 2, "add_quad", limit_mib=1)(pair, received)
    received = swap_chips(quad, 3)
    new_state = advance(1, where, key_t, value, state, new_state)
    received, new_state = lax.optimization_barrier((received, new_state))
    middle = kernel(add_body, block, [VMEM] * 3, "middle", limit_mib=1)(stream, quad, received)
    up_w = load((up_weight,), "load_up")[0]
    up_terms, middle_t = kernel(
        up_body,
        (shape((128, 2176), BF16), shape((256, 128), BF16)),
        [SMEM] + [VMEM] * 4,
        "up",
        limit_mib=4,
    )(where, middle, to_core(middle, 0), gains, in_vmem(up_w))
    up_parts = lax.all_to_all(up_terms.reshape(16, 8, 2176), "kv", 0, 0, tiled=True)
    hidden = kernel(lift_body, shape((16, 8, 2048), BF16), [VMEM], "lift", limit_mib=4)(up_parts)
    hidden_all = lax.all_to_all(hidden, "kv", 0, 0, tiled=True).reshape(128, 2048)
    down_terms = jnp.dot(hidden_all, down_weight, preferred_element_type=F32).astype(BF16)
    down_parts = lax.all_to_all(down_terms.T.reshape(8, 32, 128), "tp", 0, 0, tiled=True)
    out_t = kernel(finish_body, shape((32, 128), BF16), [SMEM, VMEM, VMEM], "finish")(
        where, down_parts, middle_t
    )
    return (out_t.T, new_state)


def solution(mesh):
    return jax.shard_map(
        per_device,
        mesh=mesh,
        in_specs=(
            P(None, ("kv", "tp")),
            P(("kv", "tp")),
            P(("kv", "tp")),
            P("kv", "tp"),
            P("kv", "tp"),
            P("kv", "tp"),
            P("kv", "tp"),
            P("tp", "kv"),
            P("kv", "tp"),
            P("tp", "kv"),
            P("kv", "tp", None, None),
        ),
        out_specs=(P(None, ("kv", "tp")), P("kv", "tp", None, None)),
        check_vma=False,
    )
```

```python
from functools import partial

import jax
import jax.numpy as jnp
from jax import lax
from jax.experimental import pallas as pl
from jax.experimental.pallas import tpu as pltpu
from jax.sharding import PartitionSpec as P

D = 4096
HEADS = 16
DK = 256
DV = 512
EPS = 1e-06
DECAYS = [float(1.0 - 2.0 ** (-1.0 - 6.0 * h / (HEADS - 1))) for h in range(HEADS)]
F32 = jnp.float32
BF16 = jnp.bfloat16
VMEM = pl.BlockSpec(memory_space=pltpu.VMEM)
SMEM = pl.BlockSpec(memory_space=pltpu.SMEM)
HBM = pl.BlockSpec(memory_space=pltpu.HBM)


def in_vmem(value):
    return pltpu.with_memory_space_constraint(value, pltpu.VMEM)


def in_hbm(value):
    return pltpu.with_memory_space_constraint(value, pltpu.HBM)


def kernel(body, outs, in_specs, name, scratch=(), limit_mib=16, out_specs=None, flops=0):
    return pl.pallas_call(
        body,
        out_shape=outs,
        in_specs=in_specs,
        out_specs=jax.tree.map(lambda _: VMEM, outs) if out_specs is None else out_specs,
        scratch_shapes=list(scratch),
        compiler_params=pltpu.CompilerParams(vmem_limit_bytes=limit_mib << 20),
        cost_estimate=pl.CostEstimate(flops=flops, transcendentals=0, bytes_accessed=0)
        if flops
        else None,
        name=name,
    )


def shape(dims, dtype):
    return jax.ShapeDtypeStruct(dims, dtype)


def load_body(*refs):
    count = len(refs) // 2
    sems = refs[-1]
    copies = [
        pltpu.make_async_copy(refs[i], refs[count + i], sems.at[i]) for i in range(count)
    ]
    for copy in copies:
        copy.start()
    for copy in copies:
        copy.wait()


def load(arrays, name):
    return kernel(
        load_body,
        tuple(pltpu.VMEM(a.shape, a.dtype) for a in arrays),
        [HBM] * len(arrays),
        name,
        [pltpu.SemaphoreType.DMA((len(arrays),))],
        limit_mib=1,
        flops=8_000_000,
    )(*map(in_hbm, arrays))


def shift_pairs(step, first):
    pairs = []
    for kv in range(16):
        z, y = kv // 4, kv % 4
        for tp in range(8):
            if (tp % 2 == 0) == first:
                to = (z + step) % 4 * 4 + y
            else:
                to = z * 4 + (y + step) % 4
            pairs.append((kv * 8 + tp, to * 8 + tp))
    return pairs


def exchange(pieces, first):
    return [
        lax.ppermute(piece, ("kv", "tp"), shift_pairs(step, first))
        for step, piece in zip((2, 1, 3), pieces)
    ]


def place(where, kv_at):
    core, kv = where[0] % 2, kv_at[0]
    z, y = kv // 4, kv % 4
    return core, jnp.where(core == 0, z, y), jnp.where(core == 0, y, z)


def send_order(where, kv_at, rows, out):
    core, first, _ = place(where, kv_at)
    for k, step in enumerate((0, 2, 1, 3)):
        to = (first + step) % 4
        for i in range(4):
            out[k * 4 + i] = rows[jnp.where(core == 0, to * 4 + i, i * 4 + to)]


def fold_body(width, where, kv_at, own, a, b, c, kept, *outs):
    _, _, second = place(where, kv_at)
    for k, step in enumerate((0, 2, 1, 3)):
        i = (second + step) % 4
        total = own[i].astype(F32) + a[i].astype(F32) + b[i].astype(F32) + c[i].astype(F32)
        squares = total[:, width : width + 1] + total[:, width + 1 : width + 2]
        if k == 0:
            kept[:, :width] = total[:, :width]
            kept[:, width:] = jnp.broadcast_to(squares, (8, 128))
        else:
            outs[k - 1][:, :width] = total[:, :width].astype(BF16)
            outs[k - 1][:, width:] = squares_lanes(squares, 128)


def total_of(width, kept, a, b, c):
    squares = kept[:, width : width + 1]
    for part in (a, b, c):
        squares = squares + part[:, width : width + 1].astype(F32)
        squares = squares + part[:, width + 1 : width + 2].astype(F32)
    total = kept[:, :width] + a[:, :width].astype(F32)
    total = total + b[:, :width].astype(F32) + c[:, :width].astype(F32)
    return total, lax.rsqrt(squares / D + EPS)


def load_body(*refs):
    count = len(refs) // 2
    sems = refs[-1]
    copies = [
        pltpu.make_async_copy(refs[i], refs[count + i], sems.at[i]) for i in range(count)
    ]
    for copy in copies:
        copy.start()
    for copy in copies:
        copy.wait()


def load(arrays, name):
    return kernel(
        load_body,
        tuple(pltpu.VMEM(a.shape, a.dtype) for a in arrays),
        [HBM] * len(arrays),
        name,
        [pltpu.SemaphoreType.DMA((len(arrays),))],
        limit_mib=1,
        flops=8_000_000,
    )(*map(in_hbm, arrays))


def shift_pairs(step, first):
    pairs = []
    for kv in range(16):
        z, y = kv // 4, kv % 4
        for tp in range(8):
            if (tp % 2 == 0) == first:
                to = (z + step) % 4 * 4 + y
            else:
                to = z * 4 + (y + step) % 4
            pairs.append((kv * 8 + tp, to * 8 + tp))
    return pairs


def exchange(pieces, first):
    return [
        lax.ppermute(piece, ("kv", "tp"), shift_pairs(step, first))
        for step, piece in zip((2, 1, 3), pieces)
    ]


def place(where, kv_at):
    core, kv = where[0] % 2, kv_at[0]
    z, y = kv // 4, kv % 4
    return core, jnp.where(core == 0, z, y), jnp.where(core == 0, y, z)


def send_order(where, kv_at, rows, out):
    core, first, _ = place(where, kv_at)
    for k, step in enumerate((0, 2, 1, 3)):
        to = (first + step) % 4
        for i in range(4):
            out[k * 4 + i] = rows[jnp.where(core == 0, to * 4 + i, i * 4 + to)]


def fold_body(width, where, kv_at, own, a, b, c, kept, *outs):
    _, _, second = place(where, kv_at)
    for k, step in enumerate((0, 2, 1, 3)):
        i = (second + step) % 4
        total = own[i].astype(F32) + a[i].astype(F32) + b[i].astype(F32) + c[i].astype(F32)
        squares = total[:, width : width + 1] + total[:, width + 1 : width + 2]
        if k == 0:
            kept[:, :width] = total[:, :width]
            kept[:, width:] = jnp.broadcast_to(squares, (8, 128))
        else:
            outs[k - 1][:, :width] = total[:, :width].astype(BF16)
            outs[k - 1][:, width:] = squares_lanes(squares, 128)


def total_of(width, kept, a, b, c):
    squares = kept[:, width : width + 1]
    for part in (a, b, c):
        squares = squares + part[:, width : width + 1].astype(F32)
        squares = squares + part[:, width + 1 : width + 2].astype(F32)
    total = kept[:, :width] + a[:, :width].astype(F32)
    total = total + b[:, :width].astype(F32) + c[:, :width].astype(F32)
    return total, lax.rsqrt(squares / D + EPS)


def to_core(value, core):
    return lax.ppermute(value, "tp", [(i ^ 1, i) for i in range(core, 8, 2)])


def swap_chips(value, mask):
    return lax.ppermute(value, "tp", [(i, i ^ (2 * mask)) for i in range(1, 8, 2)])


def load_body(*refs):
    count = len(refs) // 2
    sems = refs[-1]
    copies = [
        pltpu.make_async_copy(refs[i], refs[count + i], sems.at[i]) for i in range(count)
    ]
    for copy in copies:
        copy.start()
    for copy in copies:
        copy.wait()


def load(arrays, name):
    return kernel(
        load_body,
        tuple(pltpu.VMEM(a.shape, a.dtype) for a in arrays),
        [HBM] * len(arrays),
        name,
        [pltpu.SemaphoreType.DMA((len(arrays),))],
        limit_mib=1,
        flops=8_000_000,
    )(*map(in_hbm, arrays))


def shift_pairs(step, first):
    pairs = []
    for kv in range(16):
        z, y = kv // 4, kv % 4
        for tp in range(8):
            if (tp % 2 == 0) == first:
                to = (z + step) % 4 * 4 + y
            else:
                to = z * 4 + (y + step) % 4
            pairs.append((kv * 8 + tp, to * 8 + tp))
    return pairs


def exchange(pieces, first):
    return [
        lax.ppermute(piece, ("kv", "tp"), shift_pairs(step, first))
        for step, piece in zip((2, 1, 3), pieces)
    ]


def place(where, kv_at):
    core, kv = where[0] % 2, kv_at[0]
    z, y = kv // 4, kv % 4
    return core, jnp.where(core == 0, z, y), jnp.where(core == 0, y, z)


def send_order(where, kv_at, rows, out):
    core, first, _ = place(where, kv_at)
    for k, step in enumerate((0, 2, 1, 3)):
        to = (first + step) % 4
        for i in range(4):
            out[k * 4 + i] = rows[jnp.where(core == 0, to * 4 + i, i * 4 + to)]


def fold_body(width, where, kv_at, own, a, b, c, kept, *outs):
    _, _, second = place(where, kv_at)
    for k, step in enumerate((0, 2, 1, 3)):
        i = (second + step) % 4
        total = own[i].astype(F32) + a[i].astype(F32) + b[i].astype(F32) + c[i].astype(F32)
        squares = total[:, width : width + 1] + total[:, width + 1 : width + 2]
        if k == 0:
            kept[:, :width] = total[:, :width]
            kept[:, width:] = jnp.broadcast_to(squares, (8, 128))
        else:
            outs[k - 1][:, :width] = total[:, :width].astype(BF16)
            outs[k - 1][:, width:] = squares_lanes(squares, 128)


def total_of(width, kept, a, b, c):
    squares = kept[:, width : width + 1]
    for part in (a, b, c):
        squares = squares + part[:, width : width + 1].astype(F32)
        squares = squares + part[:, width + 1 : width + 2].astype(F32)
    total = kept[:, :width] + a[:, :width].astype(F32)
    total = total + b[:, :width].astype(F32) + c[:, :width].astype(F32)
    return total, lax.rsqrt(squares / D + EPS)


def swap_cores(value):
    return lax.ppermute(value, "tp", [(i, i ^ 1) for i in range(8)])


def swap_chips(value, mask):
    return lax.ppermute(value, "tp", [(i, i ^ (2 * mask)) for i in range(8)])


def squares_lanes(total, width):
    lane = lax.broadcasted_iota(jnp.int32, (total.shape[0], width), 1)
    high = total.astype(BF16).astype(F32)
    return jnp.where(lane == 0, high, jnp.where(lane == 1, total - high, 0.0)).astype(BF16)


def pack_body(where, act_hbm, mixer_hbm, channel_hbm, wq, wk, wv, wg, out, *refs):
    weights, (act_t, mixer, channel, sems) = refs[:4], refs[4:]
    pairs = ((act_hbm, act_t), (mixer_hbm, mixer), (channel_hbm, channel))
    pairs += tuple(zip((wq, wk, wv, wg), weights))
    copies = [pltpu.make_async_copy(a, b, sems.at[i]) for i, (a, b) in enumerate(pairs)]
    for copy in copies:
        copy.start()
    for copy in copies[:3]:
        copy.wait()
    first, slot = where[0] // 4, where[0] % 4
    lane = lax.broadcasted_iota(jnp.int32, (8, 128), 1) // 32
    row = lax.broadcasted_iota(jnp.int32, (8, 128), 0)
    tiled = [jnp.concatenate([g[...].astype(F32)] * 4, axis=1) for g in (mixer, channel)]
    gains = jnp.where(row == first, tiled[0], jnp.where(row == first + 2, tiled[1], 0.0))
    gains = jnp.where(lane == slot, gains, 0.0).astype(BF16)
    rows = act_t[...]
    for j in range(8):
        out[j, :32, :] = rows
        out[j, 32:, :] = gains
    for copy in copies[3:]:
        copy.wait()


def rate_of(where, h):
    rate = jnp.float32(DECAYS[h])
    for t in range(1, 8):
        rate = jnp.where(where[0] == t, jnp.float32(DECAYS[2 * t + h]), rate)
    return rate


def project_body(where, kv_at, packed, *refs):
    weights, outs = refs[:4], refs[4:8]
    stream_out, gains_out, rows, ordered = refs[8:]
    stream = packed[:, :32, :].astype(F32).reshape(256, 128).T
    stream_out[...] = stream.astype(BF16)
    gains = jnp.sum(packed[:, 32:40, :].astype(F32), axis=0)
    gains_out[...] = gains
    mixer = jnp.concatenate([gains[0:1], gains[1:2]], axis=1)
    rows[...] = stream.reshape(16, 8, 256)
    send_order(where, kv_at, rows, ordered)
    stream = ordered[...].reshape(128, 256)
    normed = (stream * mixer).astype(BF16)
    squares = squares_lanes(jnp.sum(stream * stream, axis=1, keepdims=True), 128)
    squares = squares.reshape(16, 8, 128)
    for k in range(4):
        outs[k][:, :, 3072:] = squares[k * 4 : k * 4 + 4]
    at = 0
    for weight in weights:
        n = weight.shape[1]
        out = jnp.dot(normed, weight[...], preferred_element_type=F32).astype(BF16)
        out = out.reshape(16, 8, n)
        for k in range(4):
            outs[k][:, :, at : at + n] = out[k * 4 : k * 4 + 4]
        at += n


def retain_body(where, own, a, b, c, state, mixed_out, key_out, value_out, kept):
    sums, scale = total_of(3072, own, a, b, c)
    query = scale * sums[:, :512]
    key = scale * sums[:, 512:1024] * DK ** (-0.5)
    value = scale * sums[:, 1024:2048]
    gate = scale * sums[:, 2048:3072]
    query_t = query.T
    key_out[...] = key.T
    value_out[...] = value
    silu = gate * jax.nn.sigmoid(gate)
    for b in range(8):
        for h in range(2):
            total = jnp.zeros((8, 512), F32)
            for r in range(0, 256, 64):
                qc = query_t[h * 256 + r : h * 256 + r + 64, b : b + 1]
                total = total + jnp.sum((qc * state[b, h, r : r + 64, :]).reshape(8, 8, 512), axis=0)
            kept[b : b + 1, h * 512 : (h + 1) * 512] = jnp.sum(total, axis=0, keepdims=True)
    for h in range(2):
        cols = slice(h * 512, (h + 1) * 512)
        heads = slice(h * 256, (h + 1) * 256)
        match = jnp.sum(query[:, heads] * key[:, heads], axis=1, keepdims=True)
        out = rate_of(where, h) * kept[:, cols] + match * value[:, cols]
        out = out * lax.rsqrt(jnp.mean(out * out, axis=1, keepdims=True) + EPS)
        mixed = (silu[:, cols] * out).astype(BF16)
        for j in range(16):
            mixed_out[j, :, cols] = mixed


def out_body(where, mixed, weight, mine_out, theirs_out):
    out = jnp.dot(mixed[...].reshape(128, 1024), weight[...], preferred_element_type=F32)
    out = out.astype(BF16)
    even = where[0] % 2 == 0
    mine_out[...] = jnp.where(even, out[:, :128], out[:, 128:])
    theirs_out[...] = jnp.where(even, out[:, 128:], out[:, :128])


def add_body(a, b, out):
    out[...] = (a[...].astype(F32) + b[...].astype(F32)).astype(BF16)


def middle_body(where, stream, a, b, out):
    attention = a[...].astype(F32) + b[...].astype(F32)
    own = jnp.where(where[0] % 2 == 0, stream[:, :128], stream[:, 128:])
    out[...] = (own.astype(F32) + attention).astype(BF16)


def up_body(where, mine, other, gains, weight, out, middle_t):
    even = where[0] % 2 == 0
    mine, other = mine[...].astype(F32), other[...].astype(F32)
    middle = jnp.concatenate(
        [jnp.where(even, mine, other), jnp.where(even, other, mine)], axis=1
    )
    middle_t[...] = middle.T.astype(BF16)
    channel = jnp.concatenate([gains[2:3, :], gains[3:4, :]], axis=1)
    normed = (middle * channel).astype(BF16)
    out[:, 2048:] = squares_lanes(jnp.sum(middle * middle, axis=1, keepdims=True), 128)
    out[:, :2048] = jnp.dot(normed, weight[...], preferred_element_type=F32).astype(BF16)


def lift_body(parts, out):
    sums = jnp.sum(parts[...].astype(F32), axis=0)
    scale = lax.rsqrt((sums[:, 2048:2049] + sums[:, 2049:2050]) / D + EPS)
    lifted = jnp.maximum(scale * sums[:, :2048], 0.0)
    hidden = (lifted * lifted).astype(BF16)
    for j in range(16):
        out[j] = hidden


def finish_body(where, parts, middle_t, out):
    lowered = jnp.sum(parts[...].astype(F32), axis=0)
    own = middle_t[pl.ds(pl.multiple_of(where[0] * 32, 32), 32), :]
    out[...] = (own.astype(F32) + lowered).astype(BF16)


def advance_body(half, where, key_t, value, state, *refs):
    new_hbm, new, sems = refs[-3:]
    writes = []
    for i in range(4):
        b = half * 4 + i
        for h in range(2):
            rate = rate_of(where, h)
            row = value[b : b + 1, h * 512 : (h + 1) * 512]
            for r in range(0, 256, 64):
                kc = key_t[h * 256 + r : h * 256 + r + 64, b : b + 1]
                new[i, h, r : r + 64, :] = rate * state[b, h, r : r + 64, :] + kc * row
        copy = pltpu.make_async_copy(new.at[i], new_hbm.at[b], sems.at[i])
        copy.start()
        writes.append(copy)
    for copy in writes:
        copy.wait()


def advance(half, where, key_t, value, state, new_state=None):
    before = [] if new_state is None else [new_state]
    return pl.pallas_call(
        partial(advance_body, half),
        out_shape=shape(state.shape, F32),
        in_specs=[SMEM, VMEM, VMEM, VMEM] + [HBM] * len(before),
        out_specs=HBM,
        scratch_shapes=[pltpu.VMEM((4,) + state.shape[1:], F32), pltpu.SemaphoreType.DMA((4,))],
        input_output_aliases={4: 0} if before else {},
        compiler_params=pltpu.CompilerParams(vmem_limit_bytes=8 << 20),
        cost_estimate=pl.CostEstimate(flops=20_000_000, transcendentals=0, bytes_accessed=8 << 20),
        name="advance_" + str(half),
    )(where, key_t, value, in_vmem(state), *before)


def per_device(
    activations,
    mixer_gain,
    channel_gain,
    query_weight,
    key_weight,
    value_weight,
    gate_weight,
    output_weight,
    up_weight,
    down_weight,
    state_in,
):
    where = lax.axis_index("tp").astype(jnp.int32)[None]
    kv_at = lax.axis_index("kv").astype(jnp.int32)[None]
    where, kv_at = lax.optimization_barrier((where, kv_at))
    sources = (activations.T, mixer_gain[None], channel_gain[None])
    weights = (query_weight, key_weight, value_weight, gate_weight)
    rows, *weights = kernel(
        pack_body,
        (shape((8, 40, 128), BF16),) + tuple(pltpu.VMEM(w.shape, BF16) for w in weights),
        [SMEM] + [HBM] * 7,
        "pack",
        [pltpu.VMEM(v.shape, BF16) for v in sources] + [pltpu.SemaphoreType.DMA((7,))],
        limit_mib=1,
    )(where, *map(in_hbm, sources + weights))
    packed = lax.all_to_all(rows, "tp", 0, 0, tiled=True)
    *terms, stream, gains = kernel(
        project_body,
        (shape((4, 8, 3200), BF16),) * 4 + (shape((128, 256), BF16), shape((8, 128), F32)),
        [SMEM, SMEM] + [VMEM] * 5,
        "project",
        [pltpu.VMEM((16, 8, 256), F32)] * 2,
        limit_mib=8,
    )(where, kv_at, packed, *map(in_vmem, weights))
    state, out_w = load((state_in, output_weight), "load_early")
    own, state, out_w = lax.optimization_barrier((terms[0], state, out_w))
    own, *parts = kernel(
        partial(fold_body, 3072),
        (shape((8, 3200), F32),) + (shape((8, 3200), BF16),) * 3,
        [SMEM, SMEM] + [VMEM] * 4,
        "fold",
        limit_mib=8,
    )(where, kv_at, own, *exchange(terms[1:], True))
    mixed, key_t, value = kernel(
        retain_body,
        (shape((16, 8, 1024), BF16), shape((512, 8), F32), shape((8, 1024), F32)),
        [SMEM] + [VMEM] * 5,
        "retain",
        [pltpu.VMEM((8, 1024), F32)],
        limit_mib=8,
    )(where, own, *exchange(parts, False), in_vmem(state))
    mixed_all = lax.all_to_all(mixed, "kv", 0, 0, tiled=True)

    half = shape((128, 128), BF16)
    mine, theirs = kernel(out_body, (half, half), [SMEM, VMEM, VMEM], "out", limit_mib=4)(
        where, mixed_all, in_vmem(out_w)
    )
    pair = kernel(add_body, half, [VMEM] * 2, "add_pair", limit_mib=1)(mine, swap_cores(theirs))
    received = swap_chips(pair, 1)
    new_state = advance(0, where, key_t, value, state)
    received, new_state = lax.optimization_barrier((received, new_state))
    quad = kernel(add_body, half, [VMEM] * 2, "add_quad", limit_mib=1)(pair, received)
    received = swap_chips(quad, 3)
    new_state = advance(1, where, key_t, value, state, new_state)
    received, new_state = lax.optimization_barrier((received, new_state))
    middle_half = kernel(middle_body, half, [SMEM] + [VMEM] * 3, "middle", limit_mib=1)(
        where, stream, quad, received
    )
    up_w = load((up_weight,), "load_up")[0]
    up_terms, middle_t = kernel(
        up_body,
        (shape((128, 2176), BF16), shape((256, 128), BF16)),
        [SMEM] + [VMEM] * 4,
        "up",
        limit_mib=4,
    )(where, middle_half, swap_cores(middle_half), gains, in_vmem(up_w))
    up_parts = lax.all_to_all(up_terms.reshape(16, 8, 2176), "kv", 0, 0, tiled=True)
    hidden = kernel(lift_body, shape((16, 8, 2048), BF16), [VMEM], "lift", limit_mib=4)(up_parts)
    hidden_all = lax.all_to_all(hidden, "kv", 0, 0, tiled=True).reshape(128, 2048)
    down_terms = jnp.dot(hidden_all, down_weight, preferred_element_type=F32).astype(BF16)
    down_parts = lax.all_to_all(down_terms.T.reshape(8, 32, 128), "tp", 0, 0, tiled=True)
    out_t = kernel(finish_body, shape((32, 128), BF16), [SMEM, VMEM, VMEM], "finish")(
        where, down_parts, middle_t
    )
    return (out_t.T, new_state)


def solution(mesh):
    return jax.shard_map(
        per_device,
        mesh=mesh,
        in_specs=(
            P(None, ("kv", "tp")),
            P(("kv", "tp")),
            P(("kv", "tp")),
            P("kv", "tp"),
            P("kv", "tp"),
            P("kv", "tp"),
            P("kv", "tp"),
            P("tp", "kv"),
            P("kv", "tp"),
            P("tp", "kv"),
            P("kv", "tp", None, None),
        ),
        out_specs=(P(None, ("kv", "tp")), P("kv", "tp", None, None)),
        check_vma=False,
    )
```

```python
from functools import partial

import jax
import jax.numpy as jnp
from jax import lax
from jax.experimental import pallas as pl
from jax.experimental.pallas import tpu as pltpu
from jax.sharding import PartitionSpec as P

D = 4096
HEADS = 16
DK = 256
DV = 512
EPS = 1e-06
DECAYS = [float(1.0 - 2.0 ** (-1.0 - 6.0 * h / (HEADS - 1))) for h in range(HEADS)]
F32 = jnp.float32
BF16 = jnp.bfloat16
VMEM = pl.BlockSpec(memory_space=pltpu.VMEM)
SMEM = pl.BlockSpec(memory_space=pltpu.SMEM)
HBM = pl.BlockSpec(memory_space=pltpu.HBM)
STEPS = (1, 3, 2)


def in_vmem(value):
    return pltpu.with_memory_space_constraint(value, pltpu.VMEM)


def in_hbm(value):
    return pltpu.with_memory_space_constraint(value, pltpu.HBM)


def kernel(body, outs, in_specs, name, scratch=(), limit_mib=16, out_specs=None, flops=0):
    return pl.pallas_call(
        body,
        out_shape=outs,
        in_specs=in_specs,
        out_specs=jax.tree.map(lambda _: VMEM, outs) if out_specs is None else out_specs,
        scratch_shapes=list(scratch),
        compiler_params=pltpu.CompilerParams(vmem_limit_bytes=limit_mib << 20),
        cost_estimate=pl.CostEstimate(flops=flops, transcendentals=0, bytes_accessed=0)
        if flops
        else None,
        name=name,
    )


def shape(dims, dtype):
    return jax.ShapeDtypeStruct(dims, dtype)


def load_body(*refs):
    count = len(refs) // 2
    sems = refs[-1]
    copies = [
        pltpu.make_async_copy(refs[i], refs[count + i], sems.at[i]) for i in range(count)
    ]
    for copy in copies:
        copy.start()
    for copy in copies:
        copy.wait()


def load(arrays, name):
    return kernel(
        load_body,
        tuple(pltpu.VMEM(a.shape, a.dtype) for a in arrays),
        [HBM] * len(arrays),
        name,
        [pltpu.SemaphoreType.DMA((len(arrays),))],
        limit_mib=1,
        flops=8_000_000,
    )(*map(in_hbm, arrays))


def shift_pairs(step, first):
    pairs = []
    for kv in range(16):
        z, y = kv // 4, kv % 4
        for tp in range(8):
            if (tp % 2 == 0) == first:
                to = (z + step) % 4 * 4 + y
            else:
                to = z * 4 + (y + step) % 4
            pairs.append((kv * 8 + tp, to * 8 + tp))
    return pairs


def exchange(pieces, first):
    return [
        lax.ppermute(piece, ("kv", "tp"), shift_pairs(step, first))
        for step, piece in zip(STEPS, pieces)
    ]


def place(where, kv_at):
    core, kv = where[0] % 2, kv_at[0]
    z, y = kv // 4, kv % 4
    return core, jnp.where(core == 0, z, y), jnp.where(core == 0, y, z)


def send_order(where, kv_at, rows, out):
    core, first, _ = place(where, kv_at)
    for k, step in enumerate((0,) + STEPS):
        to = (first + step) % 4
        for i in range(4):
            out[k * 4 + i] = rows[jnp.where(core == 0, to * 4 + i, i * 4 + to)]


def fold_body(width, where, kv_at, own, a, b, c, kept, *outs):
    _, _, second = place(where, kv_at)
    for k, step in enumerate((0,) + STEPS):
        i = (second + step) % 4
        total = own[i].astype(F32) + a[i].astype(F32) + b[i].astype(F32) + c[i].astype(F32)
        squares = total[:, width : width + 1] + total[:, width + 1 : width + 2]
        if k == 0:
            kept[:, :width] = total[:, :width]
            kept[:, width:] = jnp.broadcast_to(squares, (8, 128))
        else:
            outs[k - 1][:, :width] = total[:, :width].astype(BF16)
            outs[k - 1][:, width:] = squares_lanes(squares, 128)


def total_of(width, kept, a, b, c):
    squares = kept[:, width : width + 1]
    for part in (a, b, c):
        squares = squares + part[:, width : width + 1].astype(F32)
        squares = squares + part[:, width + 1 : width + 2].astype(F32)
    total = kept[:, :width] + a[:, :width].astype(F32)
    total = total + b[:, :width].astype(F32) + c[:, :width].astype(F32)
    return total, lax.rsqrt(squares / D + EPS)


def swap_cores(value):
    return lax.ppermute(value, "tp", [(i, i ^ 1) for i in range(8)])


def swap_chips(value, mask):
    return lax.ppermute(value, "tp", [(i, i ^ (2 * mask)) for i in range(8)])


def squares_lanes(total, width):
    lane = lax.broadcasted_iota(jnp.int32, (total.shape[0], width), 1)
    high = total.astype(BF16).astype(F32)
    return jnp.where(lane == 0, high, jnp.where(lane == 1, total - high, 0.0)).astype(BF16)


def pack_body(where, act_hbm, mixer_hbm, channel_hbm, wq, wk, wv, wg, out, *refs):
    weights, (act_t, mixer, channel, sems) = refs[:4], refs[4:]
    pairs = ((act_hbm, act_t), (mixer_hbm, mixer), (channel_hbm, channel))
    pairs += tuple(zip((wq, wk, wv, wg), weights))
    copies = [pltpu.make_async_copy(a, b, sems.at[i]) for i, (a, b) in enumerate(pairs)]
    for copy in copies:
        copy.start()
    for copy in copies[:3]:
        copy.wait()
    first, slot = where[0] // 4, where[0] % 4
    lane = lax.broadcasted_iota(jnp.int32, (8, 128), 1) // 32
    row = lax.broadcasted_iota(jnp.int32, (8, 128), 0)
    tiled = [jnp.concatenate([g[...].astype(F32)] * 4, axis=1) for g in (mixer, channel)]
    gains = jnp.where(row == first, tiled[0], jnp.where(row == first + 2, tiled[1], 0.0))
    gains = jnp.where(lane == slot, gains, 0.0).astype(BF16)
    rows = act_t[...]
    for j in range(8):
        out[j, :32, :] = rows
        out[j, 32:, :] = gains
    for copy in copies[3:]:
        copy.wait()


def rate_of(where, h):
    rate = jnp.float32(DECAYS[h])
    for t in range(1, 8):
        rate = jnp.where(where[0] == t, jnp.float32(DECAYS[2 * t + h]), rate)
    return rate


def project_body(where, kv_at, packed, *refs):
    weights, outs = refs[:4], refs[4:8]
    stream_out, gains_out, rows, ordered = refs[8:]
    stream = packed[:, :32, :].astype(F32).reshape(256, 128).T
    stream_out[...] = stream.astype(BF16)
    gains = jnp.sum(packed[:, 32:40, :].astype(F32), axis=0)
    gains_out[...] = gains
    mixer = jnp.concatenate([gains[0:1], gains[1:2]], axis=1)
    rows[...] = stream.reshape(16, 8, 256)
    send_order(where, kv_at, rows, ordered)
    stream = ordered[...].reshape(128, 256)
    normed = (stream * mixer).astype(BF16)
    squares = squares_lanes(jnp.sum(stream * stream, axis=1, keepdims=True), 128)
    squares = squares.reshape(16, 8, 128)
    for k in range(4):
        outs[k][:, :, 3072:] = squares[k * 4 : k * 4 + 4]
    at = 0
    for weight in weights:
        n = weight.shape[1]
        out = jnp.dot(normed, weight[...], preferred_element_type=F32).astype(BF16)
        out = out.reshape(16, 8, n)
        for k in range(4):
            outs[k][:, :, at : at + n] = out[k * 4 : k * 4 + 4]
        at += n


def retain_body(where, own, a, b, c, state, mixed_out, key_out, value_out, kept):
    sums, scale = total_of(3072, own, a, b, c)
    query = scale * sums[:, :512]
    key = scale * sums[:, 512:1024] * DK ** (-0.5)
    value = scale * sums[:, 1024:2048]
    gate = scale * sums[:, 2048:3072]
    query_t = query.T
    key_out[...] = key.T
    value_out[...] = value
    silu = gate * jax.nn.sigmoid(gate)
    for b in range(8):
        for h in range(2):
            total = jnp.zeros((8, 512), F32)
            for r in range(0, 256, 64):
                qc = query_t[h * 256 + r : h * 256 + r + 64, b : b + 1]
                total = total + jnp.sum((qc * state[b, h, r : r + 64, :]).reshape(8, 8, 512), axis=0)
            kept[b : b + 1, h * 512 : (h + 1) * 512] = jnp.sum(total, axis=0, keepdims=True)
    for h in range(2):
        cols = slice(h * 512, (h + 1) * 512)
        heads = slice(h * 256, (h + 1) * 256)
        match = jnp.sum(query[:, heads] * key[:, heads], axis=1, keepdims=True)
        out = rate_of(where, h) * kept[:, cols] + match * value[:, cols]
        out = out * lax.rsqrt(jnp.mean(out * out, axis=1, keepdims=True) + EPS)
        mixed = (silu[:, cols] * out).astype(BF16)
        for j in range(16):
            mixed_out[j, :, cols] = mixed


def out_body(where, mixed, weight, mine_out, theirs_out):
    out = jnp.dot(mixed[...].reshape(128, 1024), weight[...], preferred_element_type=F32)
    out = out.astype(BF16)
    even = where[0] % 2 == 0
    mine_out[...] = jnp.where(even, out[:, :128], out[:, 128:])
    theirs_out[...] = jnp.where(even, out[:, 128:], out[:, :128])


def add_body(a, b, out):
    out[...] = (a[...].astype(F32) + b[...].astype(F32)).astype(BF16)


def middle_body(where, stream, a, b, out):
    attention = a[...].astype(F32) + b[...].astype(F32)
    own = jnp.where(where[0] % 2 == 0, stream[:, :128], stream[:, 128:])
    out[...] = (own.astype(F32) + attention).astype(BF16)


def up_body(where, kv_at, mine, other, gains, weight, *refs):
    outs, (middle_t, rows, ordered) = refs[:4], refs[4:]
    even = where[0] % 2 == 0
    mine, other = mine[...].astype(F32), other[...].astype(F32)
    middle = jnp.concatenate(
        [jnp.where(even, mine, other), jnp.where(even, other, mine)], axis=1
    )
    middle_t[...] = middle.T.astype(BF16)
    rows[...] = middle.reshape(16, 8, 256)
    send_order(where, kv_at, rows, ordered)
    middle = ordered[...].reshape(128, 256)
    channel = jnp.concatenate([gains[2:3, :], gains[3:4, :]], axis=1)
    normed = (middle * channel).astype(BF16)
    squares = squares_lanes(jnp.sum(middle * middle, axis=1, keepdims=True), 128)
    squares = squares.reshape(16, 8, 128)
    out = jnp.dot(normed, weight[...], preferred_element_type=F32).astype(BF16)
    out = out.reshape(16, 8, 2048)
    for k in range(4):
        outs[k][:, :, :2048] = out[k * 4 : k * 4 + 4]
        outs[k][:, :, 2048:] = squares[k * 4 : k * 4 + 4]


def sum_of(refs):
    total = sum(ref[...].astype(F32) for ref in refs)
    total = total.reshape(32, total.shape[2])
    return total[:, :2048], total[:, 2048:2049] + total[:, 2049:2050]


def gather_sum_body(*refs):
    out = refs[-1]
    total, squares = sum_of(refs[:-1])
    out[:, :, :2048] = total.astype(BF16).reshape(4, 8, 2048)
    out[:, :, 2048:] = squares_lanes(squares, 128).reshape(4, 8, 128)


def lift_body(*refs):
    out = refs[-1]
    total, squares = sum_of(refs[:-1])
    lifted = jnp.maximum(lax.rsqrt(squares / D + EPS) * total, 0.0)
    out[...] = (lifted * lifted).astype(BF16).reshape(4, 8, 2048)


def down_body(where, kv_at, *refs):
    pieces, (weight, out, rows) = refs[:4], refs[4:]
    core, first, _ = place(where, kv_at)
    for step, piece in zip((0,) + STEPS, pieces):
        at = (first + 4 - step) % 4
        for i in range(4):
            rows[jnp.where(core == 0, at * 4 + i, i * 4 + at)] = piece[i]
    terms = jnp.dot(rows[...].reshape(128, 2048), weight[...], preferred_element_type=F32)
    out[...] = terms.T.astype(BF16).reshape(8, 32, 128)


def finish_body(where, parts, middle_t, out):
    lowered = jnp.sum(parts[...].astype(F32), axis=0)
    own = middle_t[pl.ds(pl.multiple_of(where[0] * 32, 32), 32), :]
    out[...] = (own.astype(F32) + lowered).astype(BF16)


def advance_body(half, where, key_t, value, state, *refs):
    new_hbm, new, sems = refs[-3:]
    writes = []
    for i in range(4):
        b = half * 4 + i
        for h in range(2):
            rate = rate_of(where, h)
            row = value[b : b + 1, h * 512 : (h + 1) * 512]
            for r in range(0, 256, 64):
                kc = key_t[h * 256 + r : h * 256 + r + 64, b : b + 1]
                new[i, h, r : r + 64, :] = rate * state[b, h, r : r + 64, :] + kc * row
        copy = pltpu.make_async_copy(new.at[i], new_hbm.at[b], sems.at[i])
        copy.start()
        writes.append(copy)
    for copy in writes:
        copy.wait()


def advance(half, where, key_t, value, state, new_state=None):
    before = [] if new_state is None else [new_state]
    return pl.pallas_call(
        partial(advance_body, half),
        out_shape=shape(state.shape, F32),
        in_specs=[SMEM, VMEM, VMEM, VMEM] + [HBM] * len(before),
        out_specs=HBM,
        scratch_shapes=[pltpu.VMEM((4,) + state.shape[1:], F32), pltpu.SemaphoreType.DMA((4,))],
        input_output_aliases={4: 0} if before else {},
        compiler_params=pltpu.CompilerParams(vmem_limit_bytes=8 << 20),
        cost_estimate=pl.CostEstimate(flops=20_000_000, transcendentals=0, bytes_accessed=8 << 20),
        name="advance_" + str(half),
    )(where, key_t, value, in_vmem(state), *before)


def per_device(
    activations,
    mixer_gain,
    channel_gain,
    query_weight,
    key_weight,
    value_weight,
    gate_weight,
    output_weight,
    up_weight,
    down_weight,
    state_in,
):
    where = lax.axis_index("tp").astype(jnp.int32)[None]
    kv_at = lax.axis_index("kv").astype(jnp.int32)[None]
    where, kv_at = lax.optimization_barrier((where, kv_at))
    sources = (activations.T, mixer_gain[None], channel_gain[None])
    weights = (query_weight, key_weight, value_weight, gate_weight)
    rows, *weights = kernel(
        pack_body,
        (shape((8, 40, 128), BF16),) + tuple(pltpu.VMEM(w.shape, BF16) for w in weights),
        [SMEM] + [HBM] * 7,
        "pack",
        [pltpu.VMEM(v.shape, BF16) for v in sources] + [pltpu.SemaphoreType.DMA((7,))],
        limit_mib=1,
    )(where, *map(in_hbm, sources + weights))
    packed = lax.all_to_all(rows, "tp", 0, 0, tiled=True)
    *terms, stream, gains = kernel(
        project_body,
        (shape((4, 8, 3200), BF16),) * 4 + (shape((128, 256), BF16), shape((8, 128), F32)),
        [SMEM, SMEM] + [VMEM] * 5,
        "project",
        [pltpu.VMEM((16, 8, 256), F32)] * 2,
        limit_mib=8,
    )(where, kv_at, packed, *map(in_vmem, weights))
    state, out_w = load((state_in, output_weight), "load_early")
    own, state, out_w = lax.optimization_barrier((terms[0], state, out_w))
    own, *parts = kernel(
        partial(fold_body, 3072),
        (shape((8, 3200), F32),) + (shape((8, 3200), BF16),) * 3,
        [SMEM, SMEM] + [VMEM] * 4,
        "fold",
        limit_mib=8,
    )(where, kv_at, own, *exchange(terms[1:], True))
    mixed, key_t, value = kernel(
        retain_body,
        (shape((16, 8, 1024), BF16), shape((512, 8), F32), shape((8, 1024), F32)),
        [SMEM] + [VMEM] * 5,
        "retain",
        [pltpu.VMEM((8, 1024), F32)],
        limit_mib=8,
    )(where, own, *exchange(parts, False), in_vmem(state))
    mixed_all = lax.all_to_all(mixed, "kv", 0, 0, tiled=True)

    half = shape((128, 128), BF16)
    mine, theirs = kernel(out_body, (half, half), [SMEM, VMEM, VMEM], "out", limit_mib=4)(
        where, mixed_all, in_vmem(out_w)
    )
    pair = kernel(add_body, half, [VMEM] * 2, "add_pair", limit_mib=1)(mine, swap_cores(theirs))
    received = swap_chips(pair, 1)
    new_state = advance(0, where, key_t, value, state)
    received, new_state = lax.optimization_barrier((received, new_state))
    quad = kernel(add_body, half, [VMEM] * 2, "add_quad", limit_mib=1)(pair, received)
    received = swap_chips(quad, 3)
    new_state = advance(1, where, key_t, value, state, new_state)
    received, new_state = lax.optimization_barrier((received, new_state))
    middle_half = kernel(middle_body, half, [SMEM] + [VMEM] * 3, "middle", limit_mib=1)(
        where, stream, quad, received
    )
    up_w = load((up_weight,), "load_up")[0]
    *up_terms, middle_t = kernel(
        up_body,
        (shape((4, 8, 2176), BF16),) * 4 + (shape((256, 128), BF16),),
        [SMEM, SMEM] + [VMEM] * 4,
        "up",
        [pltpu.VMEM((16, 8, 256), F32)] * 2,
        limit_mib=8,
    )(where, kv_at, middle_half, swap_cores(middle_half), gains, in_vmem(up_w))
    down_w = load((down_weight,), "load_down")[0]
    own, down_w = lax.optimization_barrier((up_terms[0], down_w))
    sums = kernel(
        gather_sum_body, shape((4, 8, 2176), BF16), [VMEM] * 4, "gather_sum", limit_mib=4
    )(own, *exchange(up_terms[1:], True))
    hidden = kernel(lift_body, shape((4, 8, 2048), BF16), [VMEM] * 4, "lift", limit_mib=4)(
        sums, *exchange([sums] * 3, False)
    )
    down_terms = kernel(
        down_body,
        shape((8, 32, 128), BF16),
        [SMEM, SMEM] + [VMEM] * 5,
        "down",
        [pltpu.VMEM((16, 8, 2048), BF16)],
        limit_mib=8,
    )(where, kv_at, hidden, *exchange([hidden] * 3, True), in_vmem(down_w))
    down_parts = lax.all_to_all(down_terms, "tp", 0, 0, tiled=True)
    out_t = kernel(finish_body, shape((32, 128), BF16), [SMEM, VMEM, VMEM], "finish")(
        where, down_parts, middle_t
    )
    return (out_t.T, new_state)


def solution(mesh):
    return jax.shard_map(
        per_device,
        mesh=mesh,
        in_specs=(
            P(None, ("kv", "tp")),
            P(("kv", "tp")),
            P(("kv", "tp")),
            P("kv", "tp"),
            P("kv", "tp"),
            P("kv", "tp"),
            P("kv", "tp"),
            P("tp", "kv"),
            P("kv", "tp"),
            P("tp", "kv"),
            P("kv", "tp", None, None),
        ),
        out_specs=(P(None, ("kv", "tp")), P("kv", "tp", None, None)),
        check_vma=False,
    )
```

```python
from functools import partial

import jax
import jax.numpy as jnp
from jax import lax
from jax.experimental import pallas as pl
from jax.experimental.pallas import tpu as pltpu
from jax.sharding import PartitionSpec as P

D = 4096
HEADS = 16
DK = 256
DV = 512
EPS = 1e-06
DECAYS = [float(1.0 - 2.0 ** (-1.0 - 6.0 * h / (HEADS - 1))) for h in range(HEADS)]
F32 = jnp.float32
BF16 = jnp.bfloat16
VMEM = pl.BlockSpec(memory_space=pltpu.VMEM)
SMEM = pl.BlockSpec(memory_space=pltpu.SMEM)
HBM = pl.BlockSpec(memory_space=pltpu.HBM)
STEPS = (3, 1, 2)


def in_vmem(value):
    return pltpu.with_memory_space_constraint(value, pltpu.VMEM)


def in_hbm(value):
    return pltpu.with_memory_space_constraint(value, pltpu.HBM)


def kernel(body, outs, in_specs, name, scratch=(), limit_mib=16, out_specs=None, flops=0):
    return pl.pallas_call(
        body,
        out_shape=outs,
        in_specs=in_specs,
        out_specs=jax.tree.map(lambda _: VMEM, outs) if out_specs is None else out_specs,
        scratch_shapes=list(scratch),
        compiler_params=pltpu.CompilerParams(vmem_limit_bytes=limit_mib << 20),
        cost_estimate=pl.CostEstimate(flops=flops, transcendentals=0, bytes_accessed=0)
        if flops
        else None,
        name=name,
    )


def shape(dims, dtype):
    return jax.ShapeDtypeStruct(dims, dtype)


def load_body(*refs):
    count = len(refs) // 2
    sems = refs[-1]
    copies = [
        pltpu.make_async_copy(refs[i], refs[count + i], sems.at[i]) for i in range(count)
    ]
    for copy in copies:
        copy.start()
    for copy in copies:
        copy.wait()


def load(arrays, name):
    return kernel(
        load_body,
        tuple(pltpu.VMEM(a.shape, a.dtype) for a in arrays),
        [HBM] * len(arrays),
        name,
        [pltpu.SemaphoreType.DMA((len(arrays),))],
        limit_mib=1,
        flops=8_000_000,
    )(*map(in_hbm, arrays))


def shift_pairs(step, first):
    pairs = []
    for kv in range(16):
        z, y = kv // 4, kv % 4
        for tp in range(8):
            if (tp % 2 == 0) == first:
                to = (z + step) % 4 * 4 + y
            else:
                to = z * 4 + (y + step) % 4
            pairs.append((kv * 8 + tp, to * 8 + tp))
    return pairs


def exchange(pieces, first):
    return [
        lax.ppermute(piece, ("kv", "tp"), shift_pairs(step, first))
        for step, piece in zip(STEPS, pieces)
    ]


def place(where, kv_at):
    core, kv = where[0] % 2, kv_at[0]
    z, y = kv // 4, kv % 4
    return core, jnp.where(core == 0, z, y), jnp.where(core == 0, y, z)


def send_order(where, kv_at, rows, out):
    core, first, _ = place(where, kv_at)
    for k, step in enumerate((0,) + STEPS):
        to = (first + step) % 4
        for i in range(4):
            out[k * 4 + i] = rows[jnp.where(core == 0, to * 4 + i, i * 4 + to)]


def fold_body(width, where, kv_at, own, a, b, c, kept, *outs):
    _, _, second = place(where, kv_at)
    for k, step in enumerate((0,) + STEPS):
        i = (second + step) % 4
        total = own[i].astype(F32) + a[i].astype(F32) + b[i].astype(F32) + c[i].astype(F32)
        squares = total[:, width : width + 1] + total[:, width + 1 : width + 2]
        if k == 0:
            kept[:, :width] = total[:, :width]
            kept[:, width:] = jnp.broadcast_to(squares, (8, 128))
        else:
            outs[k - 1][:, :width] = total[:, :width].astype(BF16)
            outs[k - 1][:, width:] = squares_lanes(squares, 128)


def total_of(width, kept, a, b, c):
    squares = kept[:, width : width + 1]
    for part in (a, b, c):
        squares = squares + part[:, width : width + 1].astype(F32)
        squares = squares + part[:, width + 1 : width + 2].astype(F32)
    total = kept[:, :width] + a[:, :width].astype(F32)
    total = total + b[:, :width].astype(F32) + c[:, :width].astype(F32)
    return total, lax.rsqrt(squares / D + EPS)


def swap_cores(value):
    return lax.ppermute(value, "tp", [(i, i ^ 1) for i in range(8)])


def swap_chips(value, mask):
    return lax.ppermute(value, "tp", [(i, i ^ (2 * mask)) for i in range(8)])


def squares_lanes(total, width):
    lane = lax.broadcasted_iota(jnp.int32, (total.shape[0], width), 1)
    high = total.astype(BF16).astype(F32)
    return jnp.where(lane == 0, high, jnp.where(lane == 1, total - high, 0.0)).astype(BF16)


def pack_body(where, act_hbm, mixer_hbm, channel_hbm, wq, wk, wv, wg, out, *refs):
    weights, (act_t, mixer, channel, sems) = refs[:4], refs[4:]
    pairs = ((act_hbm, act_t), (mixer_hbm, mixer), (channel_hbm, channel))
    pairs += tuple(zip((wq, wk, wv, wg), weights))
    copies = [pltpu.make_async_copy(a, b, sems.at[i]) for i, (a, b) in enumerate(pairs)]
    for copy in copies:
        copy.start()
    for copy in copies[:3]:
        copy.wait()
    first, slot = where[0] // 4, where[0] % 4
    lane = lax.broadcasted_iota(jnp.int32, (8, 128), 1) // 32
    row = lax.broadcasted_iota(jnp.int32, (8, 128), 0)
    tiled = [jnp.concatenate([g[...].astype(F32)] * 4, axis=1) for g in (mixer, channel)]
    gains = jnp.where(row == first, tiled[0], jnp.where(row == first + 2, tiled[1], 0.0))
    gains = jnp.where(lane == slot, gains, 0.0).astype(BF16)
    rows = act_t[...]
    for j in range(8):
        out[j, :32, :] = rows
        out[j, 32:, :] = gains
    for copy in copies[3:]:
        copy.wait()


def rate_of(where, h):
    rate = jnp.float32(DECAYS[h])
    for t in range(1, 8):
        rate = jnp.where(where[0] == t, jnp.float32(DECAYS[2 * t + h]), rate)
    return rate


def project_body(where, kv_at, packed, *refs):
    weights, outs = refs[:4], refs[4:8]
    stream_out, gains_out, rows, ordered = refs[8:]
    stream = packed[:, :32, :].astype(F32).reshape(256, 128).T
    stream_out[...] = stream.astype(BF16)
    gains = jnp.sum(packed[:, 32:40, :].astype(F32), axis=0)
    gains_out[...] = gains
    mixer = jnp.concatenate([gains[0:1], gains[1:2]], axis=1)
    rows[...] = stream.reshape(16, 8, 256)
    send_order(where, kv_at, rows, ordered)
    stream = ordered[...].reshape(128, 256)
    normed = (stream * mixer).astype(BF16)
    squares = squares_lanes(jnp.sum(stream * stream, axis=1, keepdims=True), 128)
    squares = squares.reshape(16, 8, 128)
    for k in range(4):
        outs[k][:, :, 3072:] = squares[k * 4 : k * 4 + 4]
    at = 0
    for weight in weights:
        n = weight.shape[1]
        out = jnp.dot(normed, weight[...], preferred_element_type=F32).astype(BF16)
        out = out.reshape(16, 8, n)
        for k in range(4):
            outs[k][:, :, at : at + n] = out[k * 4 : k * 4 + 4]
        at += n


def retain_body(where, own, a, b, c, state, mixed_out, key_out, value_out, kept):
    sums, scale = total_of(3072, own, a, b, c)
    query = scale * sums[:, :512]
    key = scale * sums[:, 512:1024] * DK ** (-0.5)
    value = scale * sums[:, 1024:2048]
    gate = scale * sums[:, 2048:3072]
    query_t = query.T
    key_out[...] = key.T
    value_out[...] = value
    silu = gate * jax.nn.sigmoid(gate)
    for b in range(8):
        for h in range(2):
            total = jnp.zeros((8, 512), F32)
            for r in range(0, 256, 64):
                qc = query_t[h * 256 + r : h * 256 + r + 64, b : b + 1]
                total = total + jnp.sum((qc * state[b, h, r : r + 64, :]).reshape(8, 8, 512), axis=0)
            kept[b : b + 1, h * 512 : (h + 1) * 512] = jnp.sum(total, axis=0, keepdims=True)
    for h in range(2):
        cols = slice(h * 512, (h + 1) * 512)
        heads = slice(h * 256, (h + 1) * 256)
        match = jnp.sum(query[:, heads] * key[:, heads], axis=1, keepdims=True)
        out = rate_of(where, h) * kept[:, cols] + match * value[:, cols]
        out = out * lax.rsqrt(jnp.mean(out * out, axis=1, keepdims=True) + EPS)
        mixed = (silu[:, cols] * out).astype(BF16)
        for j in range(16):
            mixed_out[j, :, cols] = mixed


def out_body(where, mixed, weight, mine_out, theirs_out):
    out = jnp.dot(mixed[...].reshape(128, 1024), weight[...], preferred_element_type=F32)
    out = out.astype(BF16)
    even = where[0] % 2 == 0
    mine_out[...] = jnp.where(even, out[:, :128], out[:, 128:])
    theirs_out[...] = jnp.where(even, out[:, 128:], out[:, :128])


def add_body(a, b, out):
    out[...] = (a[...].astype(F32) + b[...].astype(F32)).astype(BF16)


def middle_body(where, stream, a, b, out):
    attention = a[...].astype(F32) + b[...].astype(F32)
    own = jnp.where(where[0] % 2 == 0, stream[:, :128], stream[:, 128:])
    out[...] = (own.astype(F32) + attention).astype(BF16)


def up_body(where, kv_at, mine, other, gains, weight, *refs):
    outs, (middle_t, rows, ordered) = refs[:4], refs[4:]
    even = where[0] % 2 == 0
    mine, other = mine[...].astype(F32), other[...].astype(F32)
    middle = jnp.concatenate(
        [jnp.where(even, mine, other), jnp.where(even, other, mine)], axis=1
    )
    middle_t[...] = middle.T.astype(BF16)
    rows[...] = middle.reshape(16, 8, 256)
    send_order(where, kv_at, rows, ordered)
    middle = ordered[...].reshape(128, 256)
    channel = jnp.concatenate([gains[2:3, :], gains[3:4, :]], axis=1)
    normed = (middle * channel).astype(BF16)
    squares = squares_lanes(jnp.sum(middle * middle, axis=1, keepdims=True), 128)
    squares = squares.reshape(16, 8, 128)
    out = jnp.dot(normed, weight[...], preferred_element_type=F32).astype(BF16)
    out = out.reshape(16, 8, 2048)
    for k in range(4):
        outs[k][:, :, :2048] = out[k * 4 : k * 4 + 4]
        outs[k][:, :, 2048:] = squares[k * 4 : k * 4 + 4]


def sum_of(refs):
    total = sum(ref[...].astype(F32) for ref in refs)
    total = total.reshape(32, total.shape[2])
    return total[:, :2048], total[:, 2048:2049] + total[:, 2049:2050]


def gather_sum_body(*refs):
    out = refs[-1]
    total, squares = sum_of(refs[:-1])
    out[:, :, :2048] = total.astype(BF16).reshape(4, 8, 2048)
    out[:, :, 2048:] = squares_lanes(squares, 128).reshape(4, 8, 128)


def lift_body(*refs):
    out = refs[-1]
    total, squares = sum_of(refs[:-1])
    lifted = jnp.maximum(lax.rsqrt(squares / D + EPS) * total, 0.0)
    out[...] = (lifted * lifted).astype(BF16).reshape(4, 8, 2048)


def down_body(where, kv_at, *refs):
    pieces, (weight, out, rows) = refs[:4], refs[4:]
    core, first, _ = place(where, kv_at)
    for step, piece in zip((0,) + STEPS, pieces):
        at = (first + 4 - step) % 4
        for i in range(4):
            rows[jnp.where(core == 0, at * 4 + i, i * 4 + at)] = piece[i]
    terms = jnp.dot(rows[...].reshape(128, 2048), weight[...], preferred_element_type=F32)
    out[...] = terms.T.astype(BF16).reshape(8, 32, 128)


def finish_body(where, parts, middle_t, out):
    lowered = jnp.sum(parts[...].astype(F32), axis=0)
    own = middle_t[pl.ds(pl.multiple_of(where[0] * 32, 32), 32), :]
    out[...] = (own.astype(F32) + lowered).astype(BF16)


def advance_body(half, where, key_t, value, state, *refs):
    new_hbm, new, sems = refs[-3:]
    writes = []
    for i in range(4):
        b = half * 4 + i
        for h in range(2):
            rate = rate_of(where, h)
            row = value[b : b + 1, h * 512 : (h + 1) * 512]
            for r in range(0, 256, 64):
                kc = key_t[h * 256 + r : h * 256 + r + 64, b : b + 1]
                new[i, h, r : r + 64, :] = rate * state[b, h, r : r + 64, :] + kc * row
        copy = pltpu.make_async_copy(new.at[i], new_hbm.at[b], sems.at[i])
        copy.start()
        writes.append(copy)
    for copy in writes:
        copy.wait()


def advance(half, where, key_t, value, state, new_state=None):
    before = [] if new_state is None else [new_state]
    return pl.pallas_call(
        partial(advance_body, half),
        out_shape=shape(state.shape, F32),
        in_specs=[SMEM, VMEM, VMEM, VMEM] + [HBM] * len(before),
        out_specs=HBM,
        scratch_shapes=[pltpu.VMEM((4,) + state.shape[1:], F32), pltpu.SemaphoreType.DMA((4,))],
        input_output_aliases={4: 0} if before else {},
        compiler_params=pltpu.CompilerParams(vmem_limit_bytes=8 << 20),
        cost_estimate=pl.CostEstimate(flops=20_000_000, transcendentals=0, bytes_accessed=8 << 20),
        name="advance_" + str(half),
    )(where, key_t, value, in_vmem(state), *before)


def per_device(
    activations,
    mixer_gain,
    channel_gain,
    query_weight,
    key_weight,
    value_weight,
    gate_weight,
    output_weight,
    up_weight,
    down_weight,
    state_in,
):
    where = lax.axis_index("tp").astype(jnp.int32)[None]
    kv_at = lax.axis_index("kv").astype(jnp.int32)[None]
    where, kv_at = lax.optimization_barrier((where, kv_at))
    sources = (activations.T, mixer_gain[None], channel_gain[None])
    weights = (query_weight, key_weight, value_weight, gate_weight)
    rows, *weights = kernel(
        pack_body,
        (shape((8, 40, 128), BF16),) + tuple(pltpu.VMEM(w.shape, BF16) for w in weights),
        [SMEM] + [HBM] * 7,
        "pack",
        [pltpu.VMEM(v.shape, BF16) for v in sources] + [pltpu.SemaphoreType.DMA((7,))],
        limit_mib=1,
    )(where, *map(in_hbm, sources + weights))
    packed = lax.all_to_all(rows, "tp", 0, 0, tiled=True)
    *terms, stream, gains = kernel(
        project_body,
        (shape((4, 8, 3200), BF16),) * 4 + (shape((128, 256), BF16), shape((8, 128), F32)),
        [SMEM, SMEM] + [VMEM] * 5,
        "project",
        [pltpu.VMEM((16, 8, 256), F32)] * 2,
        limit_mib=8,
    )(where, kv_at, packed, *map(in_vmem, weights))
    state, out_w = load((state_in, output_weight), "load_early")
    own, state, out_w = lax.optimization_barrier((terms[0], state, out_w))
    own, *parts = kernel(
        partial(fold_body, 3072),
        (shape((8, 3200), F32),) + (shape((8, 3200), BF16),) * 3,
        [SMEM, SMEM] + [VMEM] * 4,
        "fold",
        limit_mib=8,
    )(where, kv_at, own, *exchange(terms[1:], True))
    mixed, key_t, value = kernel(
        retain_body,
        (shape((16, 8, 1024), BF16), shape((512, 8), F32), shape((8, 1024), F32)),
        [SMEM] + [VMEM] * 5,
        "retain",
        [pltpu.VMEM((8, 1024), F32)],
        limit_mib=8,
    )(where, own, *exchange(parts, False), in_vmem(state))
    mixed_all = lax.all_to_all(mixed, "kv", 0, 0, tiled=True)

    half = shape((128, 128), BF16)
    mine, theirs = kernel(out_body, (half, half), [SMEM, VMEM, VMEM], "out", limit_mib=4)(
        where, mixed_all, in_vmem(out_w)
    )
    pair = kernel(add_body, half, [VMEM] * 2, "add_pair", limit_mib=1)(mine, swap_cores(theirs))
    received = swap_chips(pair, 1)
    new_state = advance(0, where, key_t, value, state)
    received, new_state = lax.optimization_barrier((received, new_state))
    quad = kernel(add_body, half, [VMEM] * 2, "add_quad", limit_mib=1)(pair, received)
    received = swap_chips(quad, 3)
    new_state = advance(1, where, key_t, value, state, new_state)
    received, new_state = lax.optimization_barrier((received, new_state))
    middle_half = kernel(middle_body, half, [SMEM] + [VMEM] * 3, "middle", limit_mib=1)(
        where, stream, quad, received
    )
    up_w = load((up_weight,), "load_up")[0]
    *up_terms, middle_t = kernel(
        up_body,
        (shape((4, 8, 2176), BF16),) * 4 + (shape((256, 128), BF16),),
        [SMEM, SMEM] + [VMEM] * 4,
        "up",
        [pltpu.VMEM((16, 8, 256), F32)] * 2,
        limit_mib=8,
    )(where, kv_at, middle_half, swap_cores(middle_half), gains, in_vmem(up_w))
    down_w = load((down_weight,), "load_down")[0]
    own, down_w = lax.optimization_barrier((up_terms[0], down_w))
    sums = kernel(
        gather_sum_body, shape((4, 8, 2176), BF16), [VMEM] * 4, "gather_sum", limit_mib=4
    )(own, *exchange(up_terms[1:], True))
    hidden = kernel(lift_body, shape((4, 8, 2048), BF16), [VMEM] * 4, "lift", limit_mib=4)(
        sums, *exchange([sums] * 3, False)
    )
    down_terms = kernel(
        down_body,
        shape((8, 32, 128), BF16),
        [SMEM, SMEM] + [VMEM] * 5,
        "down",
        [pltpu.VMEM((16, 8, 2048), BF16)],
        limit_mib=8,
    )(where, kv_at, hidden, *exchange([hidden] * 3, True), in_vmem(down_w))
    down_parts = lax.all_to_all(down_terms, "tp", 0, 0, tiled=True)
    out_t = kernel(finish_body, shape((32, 128), BF16), [SMEM, VMEM, VMEM], "finish")(
        where, down_parts, middle_t
    )
    return (out_t.T, new_state)


def solution(mesh):
    return jax.shard_map(
        per_device,
        mesh=mesh,
        in_specs=(
            P(None, ("kv", "tp")),
            P(("kv", "tp")),
            P(("kv", "tp")),
            P("kv", "tp"),
            P("kv", "tp"),
            P("kv", "tp"),
            P("kv", "tp"),
            P("tp", "kv"),
            P("kv", "tp"),
            P("tp", "kv"),
            P("kv", "tp", None, None),
        ),
        out_specs=(P(None, ("kv", "tp")), P("kv", "tp", None, None)),
        check_vma=False,
    )
```

```python
from functools import partial

import jax
import jax.numpy as jnp
from jax import lax
from jax.experimental import pallas as pl
from jax.experimental.pallas import tpu as pltpu
from jax.sharding import PartitionSpec as P

D = 4096
HEADS = 16
DK = 256
DV = 512
EPS = 1e-06
DECAYS = [float(1.0 - 2.0 ** (-1.0 - 6.0 * h / (HEADS - 1))) for h in range(HEADS)]
F32 = jnp.float32
BF16 = jnp.bfloat16
VMEM = pl.BlockSpec(memory_space=pltpu.VMEM)
SMEM = pl.BlockSpec(memory_space=pltpu.SMEM)
HBM = pl.BlockSpec(memory_space=pltpu.HBM)
HEAD_STEPS = (1, 3, 2)
STEPS = (3, 1, 2)


def in_vmem(value):
    return pltpu.with_memory_space_constraint(value, pltpu.VMEM)


def in_hbm(value):
    return pltpu.with_memory_space_constraint(value, pltpu.HBM)


def kernel(body, outs, in_specs, name, scratch=(), limit_mib=16, out_specs=None, flops=0):
    return pl.pallas_call(
        body,
        out_shape=outs,
        in_specs=in_specs,
        out_specs=jax.tree.map(lambda _: VMEM, outs) if out_specs is None else out_specs,
        scratch_shapes=list(scratch),
        compiler_params=pltpu.CompilerParams(vmem_limit_bytes=limit_mib << 20),
        cost_estimate=pl.CostEstimate(flops=flops, transcendentals=0, bytes_accessed=0)
        if flops
        else None,
        name=name,
    )


def shape(dims, dtype):
    return jax.ShapeDtypeStruct(dims, dtype)


def load_body(*refs):
    count = len(refs) // 2
    sems = refs[-1]
    copies = [
        pltpu.make_async_copy(refs[i], refs[count + i], sems.at[i]) for i in range(count)
    ]
    for copy in copies:
        copy.start()
    for copy in copies:
        copy.wait()


def load(arrays, name):
    return kernel(
        load_body,
        tuple(pltpu.VMEM(a.shape, a.dtype) for a in arrays),
        [HBM] * len(arrays),
        name,
        [pltpu.SemaphoreType.DMA((len(arrays),))],
        limit_mib=1,
        flops=8_000_000,
    )(*map(in_hbm, arrays))


def shift_pairs(step, first):
    pairs = []
    for kv in range(16):
        z, y = kv // 4, kv % 4
        for tp in range(8):
            if (tp % 2 == 0) == first:
                to = (z + step) % 4 * 4 + y
            else:
                to = z * 4 + (y + step) % 4
            pairs.append((kv * 8 + tp, to * 8 + tp))
    return pairs


def exchange(pieces, first, steps):
    return [
        lax.ppermute(piece, ("kv", "tp"), shift_pairs(step, first))
        for step, piece in zip(steps, pieces)
    ]


def place(where, kv_at):
    core, kv = where[0] % 2, kv_at[0]
    z, y = kv // 4, kv % 4
    return core, jnp.where(core == 0, z, y), jnp.where(core == 0, y, z)


def send_order(where, kv_at, steps, rows, out):
    core, first, _ = place(where, kv_at)
    for k, step in enumerate((0,) + steps):
        to = (first + step) % 4
        for i in range(4):
            out[k * 4 + i] = rows[jnp.where(core == 0, to * 4 + i, i * 4 + to)]


def fold_body(width, where, kv_at, own, a, b, c, kept, *outs):
    _, _, second = place(where, kv_at)
    for k, step in enumerate((0,) + HEAD_STEPS):
        i = (second + step) % 4
        total = own[i].astype(F32) + a[i].astype(F32) + b[i].astype(F32) + c[i].astype(F32)
        squares = total[:, width : width + 1] + total[:, width + 1 : width + 2]
        if k == 0:
            kept[:, :width] = total[:, :width]
            kept[:, width:] = jnp.broadcast_to(squares, (8, 128))
        else:
            outs[k - 1][:, :width] = total[:, :width].astype(BF16)
            outs[k - 1][:, width:] = squares_lanes(squares, 128)


def total_of(width, kept, a, b, c):
    squares = kept[:, width : width + 1]
    for part in (a, b, c):
        squares = squares + part[:, width : width + 1].astype(F32)
        squares = squares + part[:, width + 1 : width + 2].astype(F32)
    total = kept[:, :width] + a[:, :width].astype(F32)
    total = total + b[:, :width].astype(F32) + c[:, :width].astype(F32)
    return total, lax.rsqrt(squares / D + EPS)


def swap_cores(value):
    return lax.ppermute(value, "tp", [(i, i ^ 1) for i in range(8)])


def from_chips(value):
    return [
        lax.ppermute(value, "tp", [(i, (i + 2 * step) % 8) for i in range(8)]) for step in STEPS
    ]


def squares_lanes(total, width):
    lane = lax.broadcasted_iota(jnp.int32, (total.shape[0], width), 1)
    high = total.astype(BF16).astype(F32)
    return jnp.where(lane == 0, high, jnp.where(lane == 1, total - high, 0.0)).astype(BF16)


def pack_body(where, act_hbm, mixer_hbm, channel_hbm, wq, wk, wv, wg, out, *refs):
    weights, (act_t, mixer, channel, sems) = refs[:4], refs[4:]
    pairs = ((act_hbm, act_t), (mixer_hbm, mixer), (channel_hbm, channel))
    pairs += tuple(zip((wq, wk, wv, wg), weights))
    copies = [pltpu.make_async_copy(a, b, sems.at[i]) for i, (a, b) in enumerate(pairs)]
    for copy in copies:
        copy.start()
    for copy in copies[:3]:
        copy.wait()
    first, slot = where[0] // 4, where[0] % 4
    lane = lax.broadcasted_iota(jnp.int32, (8, 128), 1) // 32
    row = lax.broadcasted_iota(jnp.int32, (8, 128), 0)
    tiled = [jnp.concatenate([g[...].astype(F32)] * 4, axis=1) for g in (mixer, channel)]
    gains = jnp.where(row == first, tiled[0], jnp.where(row == first + 2, tiled[1], 0.0))
    gains = jnp.where(lane == slot, gains, 0.0).astype(BF16)
    rows = act_t[...]
    for j in range(8):
        out[j, :32, :] = rows
        out[j, 32:, :] = gains
    for copy in copies[3:]:
        copy.wait()


def rate_of(where, h):
    rate = jnp.float32(DECAYS[h])
    for t in range(1, 8):
        rate = jnp.where(where[0] == t, jnp.float32(DECAYS[2 * t + h]), rate)
    return rate


def project_body(where, kv_at, packed, *refs):
    weights, outs = refs[:4], refs[4:8]
    stream_out, gains_out, rows, ordered = refs[8:]
    stream = packed[:, :32, :].astype(F32).reshape(256, 128).T
    stream_out[...] = stream.astype(BF16)
    gains = jnp.sum(packed[:, 32:40, :].astype(F32), axis=0)
    gains_out[...] = gains
    mixer = jnp.concatenate([gains[0:1], gains[1:2]], axis=1)
    rows[...] = stream.reshape(16, 8, 256)
    send_order(where, kv_at, HEAD_STEPS, rows, ordered)
    stream = ordered[...].reshape(128, 256)
    normed = (stream * mixer).astype(BF16)
    squares = squares_lanes(jnp.sum(stream * stream, axis=1, keepdims=True), 128)
    squares = squares.reshape(16, 8, 128)
    for k in range(4):
        outs[k][:, :, 3072:] = squares[k * 4 : k * 4 + 4]
    at = 0
    for weight in weights:
        n = weight.shape[1]
        out = jnp.dot(normed, weight[...], preferred_element_type=F32).astype(BF16)
        out = out.reshape(16, 8, n)
        for k in range(4):
            outs[k][:, :, at : at + n] = out[k * 4 : k * 4 + 4]
        at += n


def retain_body(where, own, a, b, c, state, mixed_out, key_out, value_out, kept):
    sums, scale = total_of(3072, own, a, b, c)
    query = scale * sums[:, :512]
    key = scale * sums[:, 512:1024] * DK ** (-0.5)
    value = scale * sums[:, 1024:2048]
    gate = scale * sums[:, 2048:3072]
    query_t = query.T
    key_out[...] = key.T
    value_out[...] = value
    silu = gate * jax.nn.sigmoid(gate)
    for b in range(8):
        for h in range(2):
            total = jnp.zeros((8, 512), F32)
            for r in range(0, 256, 64):
                qc = query_t[h * 256 + r : h * 256 + r + 64, b : b + 1]
                total = total + jnp.sum((qc * state[b, h, r : r + 64, :]).reshape(8, 8, 512), axis=0)
            kept[b : b + 1, h * 512 : (h + 1) * 512] = jnp.sum(total, axis=0, keepdims=True)
    for h in range(2):
        cols = slice(h * 512, (h + 1) * 512)
        heads = slice(h * 256, (h + 1) * 256)
        match = jnp.sum(query[:, heads] * key[:, heads], axis=1, keepdims=True)
        out = rate_of(where, h) * kept[:, cols] + match * value[:, cols]
        out = out * lax.rsqrt(jnp.mean(out * out, axis=1, keepdims=True) + EPS)
        mixed = (silu[:, cols] * out).astype(BF16)
        for j in range(16):
            mixed_out[j, :, cols] = mixed


def out_body(where, mixed, weight, mine_out, theirs_out):
    out = jnp.dot(mixed[...].reshape(128, 1024), weight[...], preferred_element_type=F32)
    out = out.astype(BF16)
    even = where[0] % 2 == 0
    mine_out[...] = jnp.where(even, out[:, :128], out[:, 128:])
    theirs_out[...] = jnp.where(even, out[:, 128:], out[:, :128])


def add_body(a, b, out):
    out[...] = (a[...].astype(F32) + b[...].astype(F32)).astype(BF16)


def middle_body(where, stream, *refs):
    out = refs[-1]
    attention = sum(ref[...].astype(F32) for ref in refs[:-1])
    own = jnp.where(where[0] % 2 == 0, stream[:, :128], stream[:, 128:])
    out[...] = (own.astype(F32) + attention).astype(BF16)


def up_body(where, kv_at, mine, other, gains, weight, *refs):
    outs, (middle_t, rows, ordered) = refs[:4], refs[4:]
    even = where[0] % 2 == 0
    mine, other = mine[...].astype(F32), other[...].astype(F32)
    middle = jnp.concatenate(
        [jnp.where(even, mine, other), jnp.where(even, other, mine)], axis=1
    )
    middle_t[...] = middle.T.astype(BF16)
    rows[...] = middle.reshape(16, 8, 256)
    send_order(where, kv_at, STEPS, rows, ordered)
    middle = ordered[...].reshape(128, 256)
    channel = jnp.concatenate([gains[2:3, :], gains[3:4, :]], axis=1)
    normed = (middle * channel).astype(BF16)
    squares = squares_lanes(jnp.sum(middle * middle, axis=1, keepdims=True), 128)
    squares = squares.reshape(16, 8, 128)
    out = jnp.dot(normed, weight[...], preferred_element_type=F32).astype(BF16)
    out = out.reshape(16, 8, 2048)
    for k in range(4):
        outs[k][:, :, :2048] = out[k * 4 : k * 4 + 4]
        outs[k][:, :, 2048:] = squares[k * 4 : k * 4 + 4]


def sum_of(refs):
    total = sum(ref[...].astype(F32) for ref in refs)
    total = total.reshape(32, total.shape[2])
    return total[:, :2048], total[:, 2048:2049] + total[:, 2049:2050]


def gather_sum_body(*refs):
    out = refs[-1]
    total, squares = sum_of(refs[:-1])
    out[:, :, :2048] = total.astype(BF16).reshape(4, 8, 2048)
    out[:, :, 2048:] = squares_lanes(squares, 128).reshape(4, 8, 128)


def lift_body(*refs):
    out = refs[-1]
    total, squares = sum_of(refs[:-1])
    lifted = jnp.maximum(lax.rsqrt(squares / D + EPS) * total, 0.0)
    out[...] = (lifted * lifted).astype(BF16).reshape(4, 8, 2048)


def down_body(where, kv_at, *refs):
    pieces, (weight, out, rows) = refs[:4], refs[4:]
    core, first, _ = place(where, kv_at)
    for step, piece in zip((0,) + STEPS, pieces):
        at = (first + 4 - step) % 4
        for i in range(4):
            rows[jnp.where(core == 0, at * 4 + i, i * 4 + at)] = piece[i]
    terms = jnp.dot(rows[...].reshape(128, 2048), weight[...], preferred_element_type=F32)
    out[...] = terms.T.astype(BF16).reshape(8, 32, 128)


def finish_body(where, parts, middle_t, out):
    lowered = jnp.sum(parts[...].astype(F32), axis=0)
    own = middle_t[pl.ds(pl.multiple_of(where[0] * 32, 32), 32), :]
    out[...] = (own.astype(F32) + lowered).astype(BF16)


def advance_body(half, where, key_t, value, state, *refs):
    new_hbm, new, sems = refs[-3:]
    writes = []
    for i in range(4):
        b = half * 4 + i
        for h in range(2):
            rate = rate_of(where, h)
            row = value[b : b + 1, h * 512 : (h + 1) * 512]
            for r in range(0, 256, 64):
                kc = key_t[h * 256 + r : h * 256 + r + 64, b : b + 1]
                new[i, h, r : r + 64, :] = rate * state[b, h, r : r + 64, :] + kc * row
        copy = pltpu.make_async_copy(new.at[i], new_hbm.at[b], sems.at[i])
        copy.start()
        writes.append(copy)
    for copy in writes:
        copy.wait()


def advance(half, where, key_t, value, state, new_state=None):
    before = [] if new_state is None else [new_state]
    return pl.pallas_call(
        partial(advance_body, half),
        out_shape=shape(state.shape, F32),
        in_specs=[SMEM, VMEM, VMEM, VMEM] + [HBM] * len(before),
        out_specs=HBM,
        scratch_shapes=[pltpu.VMEM((4,) + state.shape[1:], F32), pltpu.SemaphoreType.DMA((4,))],
        input_output_aliases={4: 0} if before else {},
        compiler_params=pltpu.CompilerParams(vmem_limit_bytes=8 << 20),
        cost_estimate=pl.CostEstimate(flops=20_000_000, transcendentals=0, bytes_accessed=8 << 20),
        name="advance_" + str(half),
    )(where, key_t, value, in_vmem(state), *before)


def per_device(
    activations,
    mixer_gain,
    channel_gain,
    query_weight,
    key_weight,
    value_weight,
    gate_weight,
    output_weight,
    up_weight,
    down_weight,
    state_in,
):
    where = lax.axis_index("tp").astype(jnp.int32)[None]
    kv_at = lax.axis_index("kv").astype(jnp.int32)[None]
    where, kv_at = lax.optimization_barrier((where, kv_at))
    sources = (activations.T, mixer_gain[None], channel_gain[None])
    weights = (query_weight, key_weight, value_weight, gate_weight)
    rows, *weights = kernel(
        pack_body,
        (shape((8, 40, 128), BF16),) + tuple(pltpu.VMEM(w.shape, BF16) for w in weights),
        [SMEM] + [HBM] * 7,
        "pack",
        [pltpu.VMEM(v.shape, BF16) for v in sources] + [pltpu.SemaphoreType.DMA((7,))],
        limit_mib=1,
    )(where, *map(in_hbm, sources + weights))
    packed = lax.all_to_all(rows, "tp", 0, 0, tiled=True)
    *terms, stream, gains = kernel(
        project_body,
        (shape((4, 8, 3200), BF16),) * 4 + (shape((128, 256), BF16), shape((8, 128), F32)),
        [SMEM, SMEM] + [VMEM] * 5,
        "project",
        [pltpu.VMEM((16, 8, 256), F32)] * 2,
        limit_mib=8,
    )(where, kv_at, packed, *map(in_vmem, weights))
    state, out_w = load((state_in, output_weight), "load_early")
    own, state, out_w = lax.optimization_barrier((terms[0], state, out_w))
    own, *parts = kernel(
        partial(fold_body, 3072),
        (shape((8, 3200), F32),) + (shape((8, 3200), BF16),) * 3,
        [SMEM, SMEM] + [VMEM] * 4,
        "fold",
        limit_mib=8,
    )(where, kv_at, own, *exchange(terms[1:], True, HEAD_STEPS))
    mixed, key_t, value = kernel(
        retain_body,
        (shape((16, 8, 1024), BF16), shape((512, 8), F32), shape((8, 1024), F32)),
        [SMEM] + [VMEM] * 5,
        "retain",
        [pltpu.VMEM((8, 1024), F32)],
        limit_mib=8,
    )(where, own, *exchange(parts, False, HEAD_STEPS), in_vmem(state))
    mixed_all = lax.all_to_all(mixed, "kv", 0, 0, tiled=True)

    half = shape((128, 128), BF16)
    mine, theirs = kernel(out_body, (half, half), [SMEM, VMEM, VMEM], "out", limit_mib=4)(
        where, mixed_all, in_vmem(out_w)
    )
    pair = kernel(add_body, half, [VMEM] * 2, "add_pair", limit_mib=1)(mine, swap_cores(theirs))
    received = from_chips(pair)
    new_state = advance(0, where, key_t, value, state)
    own_pair, new_state = lax.optimization_barrier((pair, new_state))
    middle_half = kernel(middle_body, half, [SMEM] + [VMEM] * 5, "middle", limit_mib=1)(
        where, stream, own_pair, *received
    )
    up_w = load((up_weight,), "load_up")[0]
    *up_terms, middle_t = kernel(
        up_body,
        (shape((4, 8, 2176), BF16),) * 4 + (shape((256, 128), BF16),),
        [SMEM, SMEM] + [VMEM] * 4,
        "up",
        [pltpu.VMEM((16, 8, 256), F32)] * 2,
        limit_mib=8,
    )(where, kv_at, middle_half, swap_cores(middle_half), gains, in_vmem(up_w))
    down_w = load((down_weight,), "load_down")[0]
    new_state = advance(1, where, key_t, value, state, new_state)
    own, down_w, new_state = lax.optimization_barrier((up_terms[0], down_w, new_state))
    sums = kernel(
        gather_sum_body, shape((4, 8, 2176), BF16), [VMEM] * 4, "gather_sum", limit_mib=4
    )(own, *exchange(up_terms[1:], True, STEPS))
    hidden = kernel(lift_body, shape((4, 8, 2048), BF16), [VMEM] * 4, "lift", limit_mib=4)(
        sums, *exchange([sums] * 3, False, STEPS)
    )
    down_terms = kernel(
        down_body,
        shape((8, 32, 128), BF16),
        [SMEM, SMEM] + [VMEM] * 5,
        "down",
        [pltpu.VMEM((16, 8, 2048), BF16)],
        limit_mib=8,
    )(where, kv_at, hidden, *exchange([hidden] * 3, True, STEPS), in_vmem(down_w))
    down_parts = lax.all_to_all(down_terms, "tp", 0, 0, tiled=True)
    out_t = kernel(finish_body, shape((32, 128), BF16), [SMEM, VMEM, VMEM], "finish")(
        where, down_parts, middle_t
    )
    return (out_t.T, new_state)


def solution(mesh):
    return jax.shard_map(
        per_device,
        mesh=mesh,
        in_specs=(
            P(None, ("kv", "tp")),
            P(("kv", "tp")),
            P(("kv", "tp")),
            P("kv", "tp"),
            P("kv", "tp"),
            P("kv", "tp"),
            P("kv", "tp"),
            P("tp", "kv"),
            P("kv", "tp"),
            P("tp", "kv"),
            P("kv", "tp", None, None),
        ),
        out_specs=(P(None, ("kv", "tp")), P("kv", "tp", None, None)),
        check_vma=False,
    )
```

```python
from functools import partial

import jax
import jax.numpy as jnp
from jax import lax
from jax.experimental import pallas as pl
from jax.experimental.pallas import tpu as pltpu
from jax.sharding import PartitionSpec as P

D = 4096
HEADS = 16
DK = 256
DV = 512
EPS = 1e-06
DECAYS = [float(1.0 - 2.0 ** (-1.0 - 6.0 * h / (HEADS - 1))) for h in range(HEADS)]
F32 = jnp.float32
BF16 = jnp.bfloat16
VMEM = pl.BlockSpec(memory_space=pltpu.VMEM)
SMEM = pl.BlockSpec(memory_space=pltpu.SMEM)
HBM = pl.BlockSpec(memory_space=pltpu.HBM)
HEAD_STEPS = (1, 3, 2)
STEPS = (3, 1, 2)


def in_vmem(value):
    return pltpu.with_memory_space_constraint(value, pltpu.VMEM)


def in_hbm(value):
    return pltpu.with_memory_space_constraint(value, pltpu.HBM)


def kernel(body, outs, in_specs, name, scratch=(), limit_mib=16, out_specs=None, flops=0):
    return pl.pallas_call(
        body,
        out_shape=outs,
        in_specs=in_specs,
        out_specs=jax.tree.map(lambda _: VMEM, outs) if out_specs is None else out_specs,
        scratch_shapes=list(scratch),
        compiler_params=pltpu.CompilerParams(vmem_limit_bytes=limit_mib << 20),
        cost_estimate=pl.CostEstimate(flops=flops, transcendentals=0, bytes_accessed=0)
        if flops
        else None,
        name=name,
    )


def shape(dims, dtype):
    return jax.ShapeDtypeStruct(dims, dtype)


def load_body(*refs):
    count = len(refs) // 2
    sems = refs[-1]
    copies = [
        pltpu.make_async_copy(refs[i], refs[count + i], sems.at[i]) for i in range(count)
    ]
    for copy in copies:
        copy.start()
    for copy in copies:
        copy.wait()


def load(arrays, name):
    return kernel(
        load_body,
        tuple(pltpu.VMEM(a.shape, a.dtype) for a in arrays),
        [HBM] * len(arrays),
        name,
        [pltpu.SemaphoreType.DMA((len(arrays),))],
        limit_mib=1,
        flops=8_000_000,
    )(*map(in_hbm, arrays))


def shift_pairs(step, first):
    pairs = []
    for kv in range(16):
        z, y = kv // 4, kv % 4
        for tp in range(8):
            if (tp % 2 == 0) == first:
                to = (z + step) % 4 * 4 + y
            else:
                to = z * 4 + (y + step) % 4
            pairs.append((kv * 8 + tp, to * 8 + tp))
    return pairs


def exchange(pieces, first, steps):
    return [
        lax.ppermute(piece, ("kv", "tp"), shift_pairs(step, first))
        for step, piece in zip(steps, pieces)
    ]


def place(where, kv_at):
    core, kv = where[0] % 2, kv_at[0]
    z, y = kv // 4, kv % 4
    return core, jnp.where(core == 0, z, y), jnp.where(core == 0, y, z)


def send_order(where, kv_at, steps, rows, out):
    core, first, _ = place(where, kv_at)
    for k, step in enumerate((0,) + steps):
        to = (first + step) % 4
        for i in range(4):
            out[k * 4 + i] = rows[jnp.where(core == 0, to * 4 + i, i * 4 + to)]


def fold_body(width, where, kv_at, own, a, b, c, kept, *outs):
    _, _, second = place(where, kv_at)
    for k, step in enumerate((0,) + HEAD_STEPS):
        i = (second + step) % 4
        total = own[i].astype(F32) + a[i].astype(F32) + b[i].astype(F32) + c[i].astype(F32)
        squares = total[:, width : width + 1] + total[:, width + 1 : width + 2]
        if k == 0:
            kept[:, :width] = total[:, :width]
            kept[:, width:] = jnp.broadcast_to(squares, (8, 128))
        else:
            outs[k - 1][:, :width] = total[:, :width].astype(BF16)
            outs[k - 1][:, width:] = squares_lanes(squares, 128)


def total_of(width, kept, a, b, c):
    squares = kept[:, width : width + 1]
    for part in (a, b, c):
        squares = squares + part[:, width : width + 1].astype(F32)
        squares = squares + part[:, width + 1 : width + 2].astype(F32)
    total = kept[:, :width] + a[:, :width].astype(F32)
    total = total + b[:, :width].astype(F32) + c[:, :width].astype(F32)
    return total, lax.rsqrt(squares / D + EPS)


def swap_cores(value):
    return lax.ppermute(value, "tp", [(i, i ^ 1) for i in range(8)])


def from_chips(value):
    return [
        lax.ppermute(value, "tp", [(i, (i + 2 * step) % 8) for i in range(8)]) for step in STEPS
    ]


def squares_lanes(total, width):
    lane = lax.broadcasted_iota(jnp.int32, (total.shape[0], width), 1)
    high = total.astype(BF16).astype(F32)
    return jnp.where(lane == 0, high, jnp.where(lane == 1, total - high, 0.0)).astype(BF16)


def pack_body(where, act_hbm, mixer_hbm, channel_hbm, wq, wk, wv, wg, out, *refs):
    weights, (act_t, mixer, channel, sems) = refs[:4], refs[4:]
    pairs = ((act_hbm, act_t), (mixer_hbm, mixer), (channel_hbm, channel))
    pairs += tuple(zip((wq, wk, wv, wg), weights))
    copies = [pltpu.make_async_copy(a, b, sems.at[i]) for i, (a, b) in enumerate(pairs)]
    for copy in copies:
        copy.start()
    for copy in copies[:3]:
        copy.wait()
    first, slot = where[0] // 4, where[0] % 4
    lane = lax.broadcasted_iota(jnp.int32, (8, 128), 1) // 32
    row = lax.broadcasted_iota(jnp.int32, (8, 128), 0)
    tiled = [jnp.concatenate([g[...].astype(F32)] * 4, axis=1) for g in (mixer, channel)]
    gains = jnp.where(row == first, tiled[0], jnp.where(row == first + 2, tiled[1], 0.0))
    gains = jnp.where(lane == slot, gains, 0.0).astype(BF16)
    rows = act_t[...]
    for j in range(8):
        out[j, :32, :] = rows
        out[j, 32:, :] = gains
    for copy in copies[3:]:
        copy.wait()


def rate_of(where, h):
    rate = jnp.float32(DECAYS[h])
    for t in range(1, 8):
        rate = jnp.where(where[0] == t, jnp.float32(DECAYS[2 * t + h]), rate)
    return rate


def project_body(where, kv_at, packed, *refs):
    weights, outs = refs[:4], refs[4:8]
    stream_out, gains_out, rows, ordered = refs[8:]
    stream = packed[:, :32, :].astype(F32).reshape(256, 128).T
    stream_out[...] = stream.astype(BF16)
    gains = jnp.sum(packed[:, 32:40, :].astype(F32), axis=0)
    gains_out[...] = gains
    mixer = jnp.concatenate([gains[0:1], gains[1:2]], axis=1)
    rows[...] = stream.reshape(16, 8, 256)
    send_order(where, kv_at, HEAD_STEPS, rows, ordered)
    stream = ordered[...].reshape(128, 256)
    normed = (stream * mixer).astype(BF16)
    squares = squares_lanes(jnp.sum(stream * stream, axis=1, keepdims=True), 128)
    squares = squares.reshape(16, 8, 128)
    for k in range(4):
        outs[k][:, :, 3072:] = squares[k * 4 : k * 4 + 4]
    at = 0
    for weight in weights:
        n = weight.shape[1]
        out = jnp.dot(normed, weight[...], preferred_element_type=F32).astype(BF16)
        out = out.reshape(16, 8, n)
        for k in range(4):
            outs[k][:, :, at : at + n] = out[k * 4 : k * 4 + 4]
        at += n


def retain_body(where, own, a, b, c, state, mixed_out, key_out, value_out, kept):
    sums, scale = total_of(3072, own, a, b, c)
    query = scale * sums[:, :512]
    key = scale * sums[:, 512:1024] * DK ** (-0.5)
    value = scale * sums[:, 1024:2048]
    gate = scale * sums[:, 2048:3072]
    query_t = query.T
    key_out[...] = key.T
    value_out[...] = value
    silu = gate * jax.nn.sigmoid(gate)
    for b in range(8):
        for h in range(2):
            total = jnp.zeros((8, 512), F32)
            for r in range(0, 256, 64):
                qc = query_t[h * 256 + r : h * 256 + r + 64, b : b + 1]
                total = total + jnp.sum((qc * state[b, h, r : r + 64, :]).reshape(8, 8, 512), axis=0)
            kept[b : b + 1, h * 512 : (h + 1) * 512] = jnp.sum(total, axis=0, keepdims=True)
    for h in range(2):
        cols = slice(h * 512, (h + 1) * 512)
        heads = slice(h * 256, (h + 1) * 256)
        match = jnp.sum(query[:, heads] * key[:, heads], axis=1, keepdims=True)
        out = rate_of(where, h) * kept[:, cols] + match * value[:, cols]
        out = out * lax.rsqrt(jnp.mean(out * out, axis=1, keepdims=True) + EPS)
        mixed = (silu[:, cols] * out).astype(BF16)
        for j in range(16):
            mixed_out[j, :, cols] = mixed


def out_body(mixed, weight, out):
    terms = jnp.dot(mixed[...].reshape(128, 1024), weight[...], preferred_element_type=F32)
    out[...] = terms.astype(BF16)


def add_body(*refs):
    out = refs[-1]
    out[...] = sum(ref[...].astype(F32) for ref in refs[:-1]).astype(BF16)


def up_body(where, kv_at, stream, mine, other, gains, weight, *refs):
    outs, (middle_t, rows, ordered) = refs[:4], refs[4:]
    attention = mine[...].astype(F32) + other[...].astype(F32)
    middle = (stream[...].astype(F32) + attention).astype(BF16).astype(F32)
    middle_t[...] = middle.T.astype(BF16)
    rows[...] = middle.reshape(16, 8, 256)
    send_order(where, kv_at, STEPS, rows, ordered)
    middle = ordered[...].reshape(128, 256)
    channel = jnp.concatenate([gains[2:3, :], gains[3:4, :]], axis=1)
    normed = (middle * channel).astype(BF16)
    squares = squares_lanes(jnp.sum(middle * middle, axis=1, keepdims=True), 128)
    squares = squares.reshape(16, 8, 128)
    out = jnp.dot(normed, weight[...], preferred_element_type=F32).astype(BF16)
    out = out.reshape(16, 8, 2048)
    for k in range(4):
        outs[k][:, :, :2048] = out[k * 4 : k * 4 + 4]
        outs[k][:, :, 2048:] = squares[k * 4 : k * 4 + 4]


def sum_of(refs):
    total = sum(ref[...].astype(F32) for ref in refs)
    total = total.reshape(32, total.shape[2])
    return total[:, :2048], total[:, 2048:2049] + total[:, 2049:2050]


def gather_sum_body(*refs):
    out = refs[-1]
    total, squares = sum_of(refs[:-1])
    out[:, :, :2048] = total.astype(BF16).reshape(4, 8, 2048)
    out[:, :, 2048:] = squares_lanes(squares, 128).reshape(4, 8, 128)


def lift_body(*refs):
    out = refs[-1]
    total, squares = sum_of(refs[:-1])
    lifted = jnp.maximum(lax.rsqrt(squares / D + EPS) * total, 0.0)
    out[...] = (lifted * lifted).astype(BF16).reshape(4, 8, 2048)


def down_body(where, kv_at, *refs):
    pieces, (weight, out, rows) = refs[:4], refs[4:]
    core, first, _ = place(where, kv_at)
    for step, piece in zip((0,) + STEPS, pieces):
        at = (first + 4 - step) % 4
        for i in range(4):
            rows[jnp.where(core == 0, at * 4 + i, i * 4 + at)] = piece[i]
    terms = jnp.dot(rows[...].reshape(128, 2048), weight[...], preferred_element_type=F32)
    out[...] = terms.T.astype(BF16).reshape(8, 32, 128)


def finish_body(where, parts, middle_t, out):
    lowered = jnp.sum(parts[...].astype(F32), axis=0)
    own = middle_t[pl.ds(pl.multiple_of(where[0] * 32, 32), 32), :]
    out[...] = (own.astype(F32) + lowered).astype(BF16)


def advance_body(half, where, key_t, value, state, *refs):
    new_hbm, new, sems = refs[-3:]
    writes = []
    for i in range(4):
        b = half * 4 + i
        for h in range(2):
            rate = rate_of(where, h)
            row = value[b : b + 1, h * 512 : (h + 1) * 512]
            for r in range(0, 256, 64):
                kc = key_t[h * 256 + r : h * 256 + r + 64, b : b + 1]
                new[i, h, r : r + 64, :] = rate * state[b, h, r : r + 64, :] + kc * row
        copy = pltpu.make_async_copy(new.at[i], new_hbm.at[b], sems.at[i])
        copy.start()
        writes.append(copy)
    for copy in writes:
        copy.wait()


def advance(half, where, key_t, value, state, new_state=None):
    before = [] if new_state is None else [new_state]
    return pl.pallas_call(
        partial(advance_body, half),
        out_shape=shape(state.shape, F32),
        in_specs=[SMEM, VMEM, VMEM, VMEM] + [HBM] * len(before),
        out_specs=HBM,
        scratch_shapes=[pltpu.VMEM((4,) + state.shape[1:], F32), pltpu.SemaphoreType.DMA((4,))],
        input_output_aliases={4: 0} if before else {},
        compiler_params=pltpu.CompilerParams(vmem_limit_bytes=8 << 20),
        cost_estimate=pl.CostEstimate(flops=20_000_000, transcendentals=0, bytes_accessed=8 << 20),
        name="advance_" + str(half),
    )(where, key_t, value, in_vmem(state), *before)


def per_device(
    activations,
    mixer_gain,
    channel_gain,
    query_weight,
    key_weight,
    value_weight,
    gate_weight,
    output_weight,
    up_weight,
    down_weight,
    state_in,
):
    where = lax.axis_index("tp").astype(jnp.int32)[None]
    kv_at = lax.axis_index("kv").astype(jnp.int32)[None]
    where, kv_at = lax.optimization_barrier((where, kv_at))
    sources = (activations.T, mixer_gain[None], channel_gain[None])
    weights = (query_weight, key_weight, value_weight, gate_weight)
    rows, *weights = kernel(
        pack_body,
        (shape((8, 40, 128), BF16),) + tuple(pltpu.VMEM(w.shape, BF16) for w in weights),
        [SMEM] + [HBM] * 7,
        "pack",
        [pltpu.VMEM(v.shape, BF16) for v in sources] + [pltpu.SemaphoreType.DMA((7,))],
        limit_mib=1,
    )(where, *map(in_hbm, sources + weights))
    packed = lax.all_to_all(rows, "tp", 0, 0, tiled=True)
    *terms, stream, gains = kernel(
        project_body,
        (shape((4, 8, 3200), BF16),) * 4 + (shape((128, 256), BF16), shape((8, 128), F32)),
        [SMEM, SMEM] + [VMEM] * 5,
        "project",
        [pltpu.VMEM((16, 8, 256), F32)] * 2,
        limit_mib=8,
    )(where, kv_at, packed, *map(in_vmem, weights))
    state, out_w = load((state_in, output_weight), "load_early")
    own, state, out_w = lax.optimization_barrier((terms[0], state, out_w))
    own, *parts = kernel(
        partial(fold_body, 3072),
        (shape((8, 3200), F32),) + (shape((8, 3200), BF16),) * 3,
        [SMEM, SMEM] + [VMEM] * 4,
        "fold",
        limit_mib=8,
    )(where, kv_at, own, *exchange(terms[1:], True, HEAD_STEPS))
    mixed, key_t, value = kernel(
        retain_body,
        (shape((16, 8, 1024), BF16), shape((512, 8), F32), shape((8, 1024), F32)),
        [SMEM] + [VMEM] * 5,
        "retain",
        [pltpu.VMEM((8, 1024), F32)],
        limit_mib=8,
    )(where, own, *exchange(parts, False, HEAD_STEPS), in_vmem(state))
    mixed_all = lax.all_to_all(mixed, "kv", 0, 0, tiled=True)

    block = shape((128, 256), BF16)
    terms = kernel(out_body, block, [VMEM] * 2, "out", limit_mib=4)(mixed_all, in_vmem(out_w))
    received = from_chips(terms)
    new_state = advance(0, where, key_t, value, state)
    terms, new_state = lax.optimization_barrier((terms, new_state))
    quad = kernel(add_body, block, [VMEM] * 4, "add_chips", limit_mib=1)(terms, *received)
    up_w = load((up_weight,), "load_up")[0]
    *up_terms, middle_t = kernel(
        up_body,
        (shape((4, 8, 2176), BF16),) * 4 + (shape((256, 128), BF16),),
        [SMEM, SMEM] + [VMEM] * 5,
        "up",
        [pltpu.VMEM((16, 8, 256), F32)] * 2,
        limit_mib=8,
    )(where, kv_at, stream, quad, swap_cores(quad), gains, in_vmem(up_w))
    down_w = load((down_weight,), "load_down")[0]
    new_state = advance(1, where, key_t, value, state, new_state)
    own, down_w, new_state = lax.optimization_barrier((up_terms[0], down_w, new_state))
    sums = kernel(
        gather_sum_body, shape((4, 8, 2176), BF16), [VMEM] * 4, "gather_sum", limit_mib=4
    )(own, *exchange(up_terms[1:], True, STEPS))
    hidden = kernel(lift_body, shape((4, 8, 2048), BF16), [VMEM] * 4, "lift", limit_mib=4)(
        sums, *exchange([sums] * 3, False, STEPS)
    )
    down_terms = kernel(
        down_body,
        shape((8, 32, 128), BF16),
        [SMEM, SMEM] + [VMEM] * 5,
        "down",
        [pltpu.VMEM((16, 8, 2048), BF16)],
        limit_mib=8,
    )(where, kv_at, hidden, *exchange([hidden] * 3, True, STEPS), in_vmem(down_w))
    down_parts = lax.all_to_all(down_terms, "tp", 0, 0, tiled=True)
    out_t = kernel(finish_body, shape((32, 128), BF16), [SMEM, VMEM, VMEM], "finish")(
        where, down_parts, middle_t
    )
    return (out_t.T, new_state)


def solution(mesh):
    return jax.shard_map(
        per_device,
        mesh=mesh,
        in_specs=(
            P(None, ("kv", "tp")),
            P(("kv", "tp")),
            P(("kv", "tp")),
            P("kv", "tp"),
            P("kv", "tp"),
            P("kv", "tp"),
            P("kv", "tp"),
            P("tp", "kv"),
            P("kv", "tp"),
            P("tp", "kv"),
            P("kv", "tp", None, None),
        ),
        out_specs=(P(None, ("kv", "tp")), P("kv", "tp", None, None)),
        check_vma=False,
    )
```

```python
from functools import partial

import jax
import jax.numpy as jnp
from jax import lax
from jax.experimental import pallas as pl
from jax.experimental.pallas import tpu as pltpu
from jax.sharding import PartitionSpec as P

D = 4096
HEADS = 16
DK = 256
DV = 512
EPS = 1e-06
DECAYS = [float(1.0 - 2.0 ** (-1.0 - 6.0 * h / (HEADS - 1))) for h in range(HEADS)]
F32 = jnp.float32
BF16 = jnp.bfloat16
VMEM = pl.BlockSpec(memory_space=pltpu.VMEM)
SMEM = pl.BlockSpec(memory_space=pltpu.SMEM)
HBM = pl.BlockSpec(memory_space=pltpu.HBM)
HEAD_STEPS = (1, 3, 2)
STEPS = (3, 1, 2)


def in_vmem(value):
    return pltpu.with_memory_space_constraint(value, pltpu.VMEM)


def in_hbm(value):
    return pltpu.with_memory_space_constraint(value, pltpu.HBM)


def kernel(body, outs, in_specs, name, scratch=(), limit_mib=16, out_specs=None, flops=0):
    return pl.pallas_call(
        body,
        out_shape=outs,
        in_specs=in_specs,
        out_specs=jax.tree.map(lambda _: VMEM, outs) if out_specs is None else out_specs,
        scratch_shapes=list(scratch),
        compiler_params=pltpu.CompilerParams(vmem_limit_bytes=limit_mib << 20),
        cost_estimate=pl.CostEstimate(flops=flops, transcendentals=0, bytes_accessed=0)
        if flops
        else None,
        name=name,
    )


def shape(dims, dtype):
    return jax.ShapeDtypeStruct(dims, dtype)


def load_body(*refs):
    count = len(refs) // 2
    sems = refs[-1]
    copies = [
        pltpu.make_async_copy(refs[i], refs[count + i], sems.at[i]) for i in range(count)
    ]
    for copy in copies:
        copy.start()
    for copy in copies:
        copy.wait()


def load(arrays, name):
    return kernel(
        load_body,
        tuple(pltpu.VMEM(a.shape, a.dtype) for a in arrays),
        [HBM] * len(arrays),
        name,
        [pltpu.SemaphoreType.DMA((len(arrays),))],
        limit_mib=1,
        flops=8_000_000,
    )(*map(in_hbm, arrays))


def shift_pairs(step, first):
    pairs = []
    for kv in range(16):
        z, y = kv // 4, kv % 4
        for tp in range(8):
            if (tp % 2 == 1) == first:
                to = (z + step) % 4 * 4 + y
            else:
                to = z * 4 + (y + step) % 4
            pairs.append((kv * 8 + tp, to * 8 + tp))
    return pairs


def exchange(pieces, first, steps):
    return [
        lax.ppermute(piece, ("kv", "tp"), shift_pairs(step, first))
        for step, piece in zip(steps, pieces)
    ]


def place(where, kv_at):
    core, kv = 1 - where[0] % 2, kv_at[0]
    z, y = kv // 4, kv % 4
    return core, jnp.where(core == 0, z, y), jnp.where(core == 0, y, z)


def send_order(where, kv_at, steps, rows, out):
    core, first, _ = place(where, kv_at)
    for k, step in enumerate((0,) + steps):
        to = (first + step) % 4
        for i in range(4):
            out[k * 4 + i] = rows[jnp.where(core == 0, to * 4 + i, i * 4 + to)]


def fold_body(width, where, kv_at, own, a, b, c, kept, *outs):
    _, _, second = place(where, kv_at)
    for k, step in enumerate((0,) + HEAD_STEPS):
        i = (second + step) % 4
        total = own[i].astype(F32) + a[i].astype(F32) + b[i].astype(F32) + c[i].astype(F32)
        squares = total[:, width : width + 1] + total[:, width + 1 : width + 2]
        if k == 0:
            kept[:, :width] = total[:, :width]
            kept[:, width:] = jnp.broadcast_to(squares, (8, 128))
        else:
            outs[k - 1][:, :width] = total[:, :width].astype(BF16)
            outs[k - 1][:, width:] = squares_lanes(squares, 128)


def total_of(width, kept, a, b, c):
    squares = kept[:, width : width + 1]
    for part in (a, b, c):
        squares = squares + part[:, width : width + 1].astype(F32)
        squares = squares + part[:, width + 1 : width + 2].astype(F32)
    total = kept[:, :width] + a[:, :width].astype(F32)
    total = total + b[:, :width].astype(F32) + c[:, :width].astype(F32)
    return total, lax.rsqrt(squares / D + EPS)


def swap_cores(value):
    return lax.ppermute(value, "tp", [(i, i ^ 1) for i in range(8)])


def from_chips(value):
    return [
        lax.ppermute(value, "tp", [(i, (i + 2 * step) % 8) for i in range(8)]) for step in STEPS
    ]


def squares_lanes(total, width):
    lane = lax.broadcasted_iota(jnp.int32, (total.shape[0], width), 1)
    high = total.astype(BF16).astype(F32)
    return jnp.where(lane == 0, high, jnp.where(lane == 1, total - high, 0.0)).astype(BF16)


def pack_body(where, act_hbm, mixer_hbm, channel_hbm, wq, wk, wv, wg, out, *refs):
    weights, (act_t, mixer, channel, sems) = refs[:4], refs[4:]
    pairs = ((act_hbm, act_t), (mixer_hbm, mixer), (channel_hbm, channel))
    pairs += tuple(zip((wq, wk, wv, wg), weights))
    copies = [pltpu.make_async_copy(a, b, sems.at[i]) for i, (a, b) in enumerate(pairs)]
    for copy in copies:
        copy.start()
    for copy in copies[:3]:
        copy.wait()
    first, slot = where[0] // 4, where[0] % 4
    lane = lax.broadcasted_iota(jnp.int32, (8, 128), 1) // 32
    row = lax.broadcasted_iota(jnp.int32, (8, 128), 0)
    tiled = [jnp.concatenate([g[...].astype(F32)] * 4, axis=1) for g in (mixer, channel)]
    gains = jnp.where(row == first, tiled[0], jnp.where(row == first + 2, tiled[1], 0.0))
    gains = jnp.where(lane == slot, gains, 0.0).astype(BF16)
    rows = act_t[...]
    for j in range(8):
        out[j, :32, :] = rows
        out[j, 32:, :] = gains
    for copy in copies[3:]:
        copy.wait()


def rate_of(where, h):
    rate = jnp.float32(DECAYS[h])
    for t in range(1, 8):
        rate = jnp.where(where[0] == t, jnp.float32(DECAYS[2 * t + h]), rate)
    return rate


def project_body(where, kv_at, packed, *refs):
    weights, outs = refs[:4], refs[4:8]
    stream_out, gains_out, rows, ordered = refs[8:]
    stream = packed[:, :32, :].astype(F32).reshape(256, 128).T
    stream_out[...] = stream.astype(BF16)
    gains = jnp.sum(packed[:, 32:40, :].astype(F32), axis=0)
    gains_out[...] = gains
    mixer = jnp.concatenate([gains[0:1], gains[1:2]], axis=1)
    rows[...] = stream.reshape(16, 8, 256)
    send_order(where, kv_at, HEAD_STEPS, rows, ordered)
    stream = ordered[...].reshape(128, 256)
    normed = (stream * mixer).astype(BF16)
    squares = squares_lanes(jnp.sum(stream * stream, axis=1, keepdims=True), 128)
    squares = squares.reshape(16, 8, 128)
    for k in range(4):
        outs[k][:, :, 3072:] = squares[k * 4 : k * 4 + 4]
    at = 0
    for weight in weights:
        n = weight.shape[1]
        out = jnp.dot(normed, weight[...], preferred_element_type=F32).astype(BF16)
        out = out.reshape(16, 8, n)
        for k in range(4):
            outs[k][:, :, at : at + n] = out[k * 4 : k * 4 + 4]
        at += n


def retain_body(where, own, a, b, c, state, mixed_out, key_out, value_out, kept):
    sums, scale = total_of(3072, own, a, b, c)
    query = scale * sums[:, :512]
    key = scale * sums[:, 512:1024] * DK ** (-0.5)
    value = scale * sums[:, 1024:2048]
    gate = scale * sums[:, 2048:3072]
    query_t = query.T
    key_out[...] = key.T
    value_out[...] = value
    silu = gate * jax.nn.sigmoid(gate)
    for b in range(8):
        for h in range(2):
            total = jnp.zeros((8, 512), F32)
            for r in range(0, 256, 64):
                qc = query_t[h * 256 + r : h * 256 + r + 64, b : b + 1]
                total = total + jnp.sum((qc * state[b, h, r : r + 64, :]).reshape(8, 8, 512), axis=0)
            kept[b : b + 1, h * 512 : (h + 1) * 512] = jnp.sum(total, axis=0, keepdims=True)
    for h in range(2):
        cols = slice(h * 512, (h + 1) * 512)
        heads = slice(h * 256, (h + 1) * 256)
        match = jnp.sum(query[:, heads] * key[:, heads], axis=1, keepdims=True)
        out = rate_of(where, h) * kept[:, cols] + match * value[:, cols]
        out = out * lax.rsqrt(jnp.mean(out * out, axis=1, keepdims=True) + EPS)
        mixed = (silu[:, cols] * out).astype(BF16)
        for j in range(16):
            mixed_out[j, :, cols] = mixed


def out_body(mixed, weight, out):
    terms = jnp.dot(mixed[...].reshape(128, 1024), weight[...], preferred_element_type=F32)
    out[...] = terms.astype(BF16)


def add_body(*refs):
    out = refs[-1]
    out[...] = sum(ref[...].astype(F32) for ref in refs[:-1]).astype(BF16)


def up_body(where, kv_at, stream, mine, other, gains, weight, *refs):
    outs, (middle_t, rows, ordered) = refs[:4], refs[4:]
    attention = mine[...].astype(F32) + other[...].astype(F32)
    middle = (stream[...].astype(F32) + attention).astype(BF16).astype(F32)
    middle_t[...] = middle.T.astype(BF16)
    rows[...] = middle.reshape(16, 8, 256)
    send_order(where, kv_at, STEPS, rows, ordered)
    middle = ordered[...].reshape(128, 256)
    channel = jnp.concatenate([gains[2:3, :], gains[3:4, :]], axis=1)
    normed = (middle * channel).astype(BF16)
    squares = squares_lanes(jnp.sum(middle * middle, axis=1, keepdims=True), 128)
    squares = squares.reshape(16, 8, 128)
    out = jnp.dot(normed, weight[...], preferred_element_type=F32).astype(BF16)
    out = out.reshape(16, 8, 2048)
    for k in range(4):
        outs[k][:, :, :2048] = out[k * 4 : k * 4 + 4]
        outs[k][:, :, 2048:] = squares[k * 4 : k * 4 + 4]


def sum_of(refs):
    total = sum(ref[...].astype(F32) for ref in refs)
    total = total.reshape(32, total.shape[2])
    return total[:, :2048], total[:, 2048:2049] + total[:, 2049:2050]


def gather_sum_body(*refs):
    out = refs[-1]
    total, squares = sum_of(refs[:-1])
    out[:, :, :2048] = total.astype(BF16).reshape(4, 8, 2048)
    out[:, :, 2048:] = squares_lanes(squares, 128).reshape(4, 8, 128)


def lift_body(*refs):
    out = refs[-1]
    total, squares = sum_of(refs[:-1])
    lifted = jnp.maximum(lax.rsqrt(squares / D + EPS) * total, 0.0)
    out[...] = (lifted * lifted).astype(BF16).reshape(4, 8, 2048)


def down_body(where, kv_at, *refs):
    pieces, (weight, out, rows) = refs[:4], refs[4:]
    core, first, _ = place(where, kv_at)
    for step, piece in zip((0,) + STEPS, pieces):
        at = (first + 4 - step) % 4
        for i in range(4):
            rows[jnp.where(core == 0, at * 4 + i, i * 4 + at)] = piece[i]
    terms = jnp.dot(rows[...].reshape(128, 2048), weight[...], preferred_element_type=F32)
    out[...] = terms.T.astype(BF16).reshape(8, 32, 128)


def finish_body(where, parts, middle_t, out):
    lowered = jnp.sum(parts[...].astype(F32), axis=0)
    own = middle_t[pl.ds(pl.multiple_of(where[0] * 32, 32), 32), :]
    out[...] = (own.astype(F32) + lowered).astype(BF16)


def advance_body(half, where, key_t, value, state, *refs):
    new_hbm, new, sems = refs[-3:]
    writes = []
    for i in range(4):
        b = half * 4 + i
        for h in range(2):
            rate = rate_of(where, h)
            row = value[b : b + 1, h * 512 : (h + 1) * 512]
            for r in range(0, 256, 64):
                kc = key_t[h * 256 + r : h * 256 + r + 64, b : b + 1]
                new[i, h, r : r + 64, :] = rate * state[b, h, r : r + 64, :] + kc * row
        copy = pltpu.make_async_copy(new.at[i], new_hbm.at[b], sems.at[i])
        copy.start()
        writes.append(copy)
    for copy in writes:
        copy.wait()


def advance(half, where, key_t, value, state, new_state=None):
    before = [] if new_state is None else [new_state]
    return pl.pallas_call(
        partial(advance_body, half),
        out_shape=shape(state.shape, F32),
        in_specs=[SMEM, VMEM, VMEM, VMEM] + [HBM] * len(before),
        out_specs=HBM,
        scratch_shapes=[pltpu.VMEM((4,) + state.shape[1:], F32), pltpu.SemaphoreType.DMA((4,))],
        input_output_aliases={4: 0} if before else {},
        compiler_params=pltpu.CompilerParams(vmem_limit_bytes=8 << 20),
        cost_estimate=pl.CostEstimate(flops=20_000_000, transcendentals=0, bytes_accessed=8 << 20),
        name="advance_" + str(half),
    )(where, key_t, value, in_vmem(state), *before)


def per_device(
    activations,
    mixer_gain,
    channel_gain,
    query_weight,
    key_weight,
    value_weight,
    gate_weight,
    output_weight,
    up_weight,
    down_weight,
    state_in,
):
    where = lax.axis_index("tp").astype(jnp.int32)[None]
    kv_at = lax.axis_index("kv").astype(jnp.int32)[None]
    where, kv_at = lax.optimization_barrier((where, kv_at))
    sources = (activations.T, mixer_gain[None], channel_gain[None])
    weights = (query_weight, key_weight, value_weight, gate_weight)
    rows, *weights = kernel(
        pack_body,
        (shape((8, 40, 128), BF16),) + tuple(pltpu.VMEM(w.shape, BF16) for w in weights),
        [SMEM] + [HBM] * 7,
        "pack",
        [pltpu.VMEM(v.shape, BF16) for v in sources] + [pltpu.SemaphoreType.DMA((7,))],
        limit_mib=1,
    )(where, *map(in_hbm, sources + weights))
    packed = lax.all_to_all(rows, "tp", 0, 0, tiled=True)
    *terms, stream, gains = kernel(
        project_body,
        (shape((4, 8, 3200), BF16),) * 4 + (shape((128, 256), BF16), shape((8, 128), F32)),
        [SMEM, SMEM] + [VMEM] * 5,
        "project",
        [pltpu.VMEM((16, 8, 256), F32)] * 2,
        limit_mib=8,
    )(where, kv_at, packed, *map(in_vmem, weights))
    state, out_w = load((state_in, output_weight), "load_early")
    own, state, out_w = lax.optimization_barrier((terms[0], state, out_w))
    own, *parts = kernel(
        partial(fold_body, 3072),
        (shape((8, 3200), F32),) + (shape((8, 3200), BF16),) * 3,
        [SMEM, SMEM] + [VMEM] * 4,
        "fold",
        limit_mib=8,
    )(where, kv_at, own, *exchange(terms[1:], True, HEAD_STEPS))
    mixed, key_t, value = kernel(
        retain_body,
        (shape((16, 8, 1024), BF16), shape((512, 8), F32), shape((8, 1024), F32)),
        [SMEM] + [VMEM] * 5,
        "retain",
        [pltpu.VMEM((8, 1024), F32)],
        limit_mib=8,
    )(where, own, *exchange(parts, False, HEAD_STEPS), in_vmem(state))
    mixed_all = lax.all_to_all(mixed, "kv", 0, 0, tiled=True)

    block = shape((128, 256), BF16)
    terms = kernel(out_body, block, [VMEM] * 2, "out", limit_mib=4)(mixed_all, in_vmem(out_w))
    received = from_chips(terms)
    new_state = advance(0, where, key_t, value, state)
    up_w = load((up_weight,), "load_up")[0]
    terms, new_state, up_w = lax.optimization_barrier((terms, new_state, up_w))
    quad = kernel(add_body, block, [VMEM] * 4, "add_chips", limit_mib=1)(terms, *received)
    *up_terms, middle_t = kernel(
        up_body,
        (shape((4, 8, 2176), BF16),) * 4 + (shape((256, 128), BF16),),
        [SMEM, SMEM] + [VMEM] * 5,
        "up",
        [pltpu.VMEM((16, 8, 256), F32)] * 2,
        limit_mib=8,
    )(where, kv_at, stream, quad, swap_cores(quad), gains, in_vmem(up_w))
    down_w = load((down_weight,), "load_down")[0]
    new_state = advance(1, where, key_t, value, state, new_state)
    own, down_w, new_state = lax.optimization_barrier((up_terms[0], down_w, new_state))
    sums = kernel(
        gather_sum_body, shape((4, 8, 2176), BF16), [VMEM] * 4, "gather_sum", limit_mib=4
    )(own, *exchange(up_terms[1:], True, STEPS))
    hidden = kernel(lift_body, shape((4, 8, 2048), BF16), [VMEM] * 4, "lift", limit_mib=4)(
        sums, *exchange([sums] * 3, False, STEPS)
    )
    down_terms = kernel(
        down_body,
        shape((8, 32, 128), BF16),
        [SMEM, SMEM] + [VMEM] * 5,
        "down",
        [pltpu.VMEM((16, 8, 2048), BF16)],
        limit_mib=8,
    )(where, kv_at, hidden, *exchange([hidden] * 3, True, STEPS), in_vmem(down_w))
    down_parts = lax.all_to_all(down_terms, "tp", 0, 0, tiled=True)
    out_t = kernel(finish_body, shape((32, 128), BF16), [SMEM, VMEM, VMEM], "finish")(
        where, down_parts, middle_t
    )
    return (out_t.T, new_state)


def solution(mesh):
    return jax.shard_map(
        per_device,
        mesh=mesh,
        in_specs=(
            P(None, ("kv", "tp")),
            P(("kv", "tp")),
            P(("kv", "tp")),
            P("kv", "tp"),
            P("kv", "tp"),
            P("kv", "tp"),
            P("kv", "tp"),
            P("tp", "kv"),
            P("kv", "tp"),
            P("tp", "kv"),
            P("kv", "tp", None, None),
        ),
        out_specs=(P(None, ("kv", "tp")), P("kv", "tp", None, None)),
        check_vma=False,
    )
```

```python
from functools import partial

import jax
import jax.numpy as jnp
from jax import lax
from jax.experimental import pallas as pl
from jax.experimental.pallas import tpu as pltpu
from jax.sharding import PartitionSpec as P

D = 4096
HEADS = 16
DK = 256
DV = 512
EPS = 1e-06
DECAYS = [float(1.0 - 2.0 ** (-1.0 - 6.0 * h / (HEADS - 1))) for h in range(HEADS)]
F32 = jnp.float32
BF16 = jnp.bfloat16
VMEM = pl.BlockSpec(memory_space=pltpu.VMEM)
SMEM = pl.BlockSpec(memory_space=pltpu.SMEM)
HBM = pl.BlockSpec(memory_space=pltpu.HBM)
HEAD_STEPS = (1, 3, 2)
STEPS = (3, 1, 2)


def in_vmem(value):
    return pltpu.with_memory_space_constraint(value, pltpu.VMEM)


def in_hbm(value):
    return pltpu.with_memory_space_constraint(value, pltpu.HBM)


def kernel(body, outs, in_specs, name, scratch=(), limit_mib=16, out_specs=None, flops=0):
    return pl.pallas_call(
        body,
        out_shape=outs,
        in_specs=in_specs,
        out_specs=jax.tree.map(lambda _: VMEM, outs) if out_specs is None else out_specs,
        scratch_shapes=list(scratch),
        compiler_params=pltpu.CompilerParams(vmem_limit_bytes=limit_mib << 20),
        cost_estimate=pl.CostEstimate(flops=flops, transcendentals=0, bytes_accessed=0)
        if flops
        else None,
        name=name,
    )


def shape(dims, dtype):
    return jax.ShapeDtypeStruct(dims, dtype)


def load_body(*refs):
    count = len(refs) // 2
    sems = refs[-1]
    copies = [
        pltpu.make_async_copy(refs[i], refs[count + i], sems.at[i]) for i in range(count)
    ]
    for copy in copies:
        copy.start()
    for copy in copies:
        copy.wait()


def load(arrays, name):
    return kernel(
        load_body,
        tuple(pltpu.VMEM(a.shape, a.dtype) for a in arrays),
        [HBM] * len(arrays),
        name,
        [pltpu.SemaphoreType.DMA((len(arrays),))],
        limit_mib=1,
        flops=8_000_000,
    )(*map(in_hbm, arrays))


def shift_pairs(step, first):
    pairs = []
    for kv in range(16):
        z, y = kv // 4, kv % 4
        for tp in range(8):
            if (tp % 2 == 1) == first:
                to = (z + step) % 4 * 4 + y
            else:
                to = z * 4 + (y + step) % 4
            pairs.append((kv * 8 + tp, to * 8 + tp))
    return pairs


def exchange(pieces, first, steps):
    return [
        lax.ppermute(piece, ("kv", "tp"), shift_pairs(step, first))
        for step, piece in zip(steps, pieces)
    ]


def place(where, kv_at):
    core, kv = 1 - where[0] % 2, kv_at[0]
    z, y = kv // 4, kv % 4
    return core, jnp.where(core == 0, z, y), jnp.where(core == 0, y, z)


def send_order(where, kv_at, steps, rows, out):
    core, first, _ = place(where, kv_at)
    for k, step in enumerate((0,) + steps):
        to = (first + step) % 4
        for i in range(4):
            out[k * 4 + i] = rows[jnp.where(core == 0, to * 4 + i, i * 4 + to)]


def fold_body(width, where, kv_at, own, a, b, c, kept, *outs):
    _, _, second = place(where, kv_at)
    for k, step in enumerate((0,) + HEAD_STEPS):
        i = (second + step) % 4
        total = own[i].astype(F32) + a[i].astype(F32) + b[i].astype(F32) + c[i].astype(F32)
        squares = total[:, width : width + 1] + total[:, width + 1 : width + 2]
        if k == 0:
            kept[:, :width] = total[:, :width]
            kept[:, width:] = jnp.broadcast_to(squares, (8, 128))
        else:
            outs[k - 1][:, :width] = total[:, :width].astype(BF16)
            outs[k - 1][:, width:] = squares_lanes(squares, 128)


def total_of(width, kept, a, b, c):
    squares = kept[:, width : width + 1]
    for part in (a, b, c):
        squares = squares + part[:, width : width + 1].astype(F32)
        squares = squares + part[:, width + 1 : width + 2].astype(F32)
    total = kept[:, :width] + a[:, :width].astype(F32)
    total = total + b[:, :width].astype(F32) + c[:, :width].astype(F32)
    return total, lax.rsqrt(squares / D + EPS)


def swap_cores(value):
    return lax.ppermute(value, "tp", [(i, i ^ 1) for i in range(8)])


def from_chips(value):
    return [
        lax.ppermute(value, "tp", [(i, (i + 2 * step) % 8) for i in range(8)]) for step in HEAD_STEPS
    ]


def squares_lanes(total, width):
    lane = lax.broadcasted_iota(jnp.int32, (total.shape[0], width), 1)
    high = total.astype(BF16).astype(F32)
    return jnp.where(lane == 0, high, jnp.where(lane == 1, total - high, 0.0)).astype(BF16)


def pack_body(where, act_hbm, mixer_hbm, channel_hbm, wq, wk, wv, wg, out, *refs):
    weights, (act_t, mixer, channel, sems) = refs[:4], refs[4:]
    pairs = ((act_hbm, act_t), (mixer_hbm, mixer), (channel_hbm, channel))
    pairs += tuple(zip((wq, wk, wv, wg), weights))
    copies = [pltpu.make_async_copy(a, b, sems.at[i]) for i, (a, b) in enumerate(pairs)]
    for copy in copies:
        copy.start()
    for copy in copies[:3]:
        copy.wait()
    first, slot = where[0] // 4, where[0] % 4
    lane = lax.broadcasted_iota(jnp.int32, (8, 128), 1) // 32
    row = lax.broadcasted_iota(jnp.int32, (8, 128), 0)
    tiled = [jnp.concatenate([g[...].astype(F32)] * 4, axis=1) for g in (mixer, channel)]
    gains = jnp.where(row == first, tiled[0], jnp.where(row == first + 2, tiled[1], 0.0))
    gains = jnp.where(lane == slot, gains, 0.0).astype(BF16)
    rows = act_t[...]
    for j in range(8):
        out[j, :32, :] = rows
        out[j, 32:, :] = gains
    for copy in copies[3:]:
        copy.wait()


def rate_of(where, h):
    rate = jnp.float32(DECAYS[h])
    for t in range(1, 8):
        rate = jnp.where(where[0] == t, jnp.float32(DECAYS[2 * t + h]), rate)
    return rate


def project_body(where, kv_at, packed, *refs):
    weights, outs = refs[:4], refs[4:8]
    stream_out, gains_out, rows, ordered = refs[8:]
    stream = packed[:, :32, :].astype(F32).reshape(256, 128).T
    stream_out[...] = stream.astype(BF16)
    gains = jnp.sum(packed[:, 32:40, :].astype(F32), axis=0)
    gains_out[...] = gains
    mixer = jnp.concatenate([gains[0:1], gains[1:2]], axis=1)
    rows[...] = stream.reshape(16, 8, 256)
    send_order(where, kv_at, HEAD_STEPS, rows, ordered)
    stream = ordered[...].reshape(128, 256)
    normed = (stream * mixer).astype(BF16)
    squares = squares_lanes(jnp.sum(stream * stream, axis=1, keepdims=True), 128)
    squares = squares.reshape(16, 8, 128)
    for k in range(4):
        outs[k][:, :, 3072:] = squares[k * 4 : k * 4 + 4]
    at = 0
    for weight in weights:
        n = weight.shape[1]
        out = jnp.dot(normed, weight[...], preferred_element_type=F32).astype(BF16)
        out = out.reshape(16, 8, n)
        for k in range(4):
            outs[k][:, :, at : at + n] = out[k * 4 : k * 4 + 4]
        at += n


def retain_body(where, own, a, b, c, state, mixed_out, key_out, value_out, kept):
    sums, scale = total_of(3072, own, a, b, c)
    query = scale * sums[:, :512]
    key = scale * sums[:, 512:1024] * DK ** (-0.5)
    value = scale * sums[:, 1024:2048]
    gate = scale * sums[:, 2048:3072]
    query_t = query.T
    key_out[...] = key.T
    value_out[...] = value
    silu = gate * jax.nn.sigmoid(gate)
    for b in range(8):
        for h in range(2):
            total = jnp.zeros((8, 512), F32)
            for r in range(0, 256, 64):
                qc = query_t[h * 256 + r : h * 256 + r + 64, b : b + 1]
                total = total + jnp.sum((qc * state[b, h, r : r + 64, :]).reshape(8, 8, 512), axis=0)
            kept[b : b + 1, h * 512 : (h + 1) * 512] = jnp.sum(total, axis=0, keepdims=True)
    for h in range(2):
        cols = slice(h * 512, (h + 1) * 512)
        heads = slice(h * 256, (h + 1) * 256)
        match = jnp.sum(query[:, heads] * key[:, heads], axis=1, keepdims=True)
        out = rate_of(where, h) * kept[:, cols] + match * value[:, cols]
        out = out * lax.rsqrt(jnp.mean(out * out, axis=1, keepdims=True) + EPS)
        mixed = (silu[:, cols] * out).astype(BF16)
        for j in range(16):
            mixed_out[j, :, cols] = mixed


def out_body(mixed, weight, out):
    terms = jnp.dot(mixed[...].reshape(128, 1024), weight[...], preferred_element_type=F32)
    out[...] = terms.astype(BF16)


def add_body(*refs):
    out = refs[-1]
    out[...] = sum(ref[...].astype(F32) for ref in refs[:-1]).astype(BF16)


def up_body(where, kv_at, stream, mine, other, gains, weight, *refs):
    outs, (middle_t, rows, ordered) = refs[:4], refs[4:]
    attention = mine[...].astype(F32) + other[...].astype(F32)
    middle = (stream[...].astype(F32) + attention).astype(BF16).astype(F32)
    middle_t[...] = middle.T.astype(BF16)
    rows[...] = middle.reshape(16, 8, 256)
    send_order(where, kv_at, STEPS, rows, ordered)
    middle = ordered[...].reshape(128, 256)
    channel = jnp.concatenate([gains[2:3, :], gains[3:4, :]], axis=1)
    normed = (middle * channel).astype(BF16)
    squares = squares_lanes(jnp.sum(middle * middle, axis=1, keepdims=True), 128)
    squares = squares.reshape(16, 8, 128)
    out = jnp.dot(normed, weight[...], preferred_element_type=F32).astype(BF16)
    out = out.reshape(16, 8, 2048)
    for k in range(4):
        outs[k][:, :, :2048] = out[k * 4 : k * 4 + 4]
        outs[k][:, :, 2048:] = squares[k * 4 : k * 4 + 4]


def sum_of(refs):
    total = sum(ref[...].astype(F32) for ref in refs)
    total = total.reshape(32, total.shape[2])
    return total[:, :2048], total[:, 2048:2049] + total[:, 2049:2050]


def gather_sum_body(*refs):
    out = refs[-1]
    total, squares = sum_of(refs[:-1])
    out[:, :, :2048] = total.astype(BF16).reshape(4, 8, 2048)
    out[:, :, 2048:] = squares_lanes(squares, 128).reshape(4, 8, 128)


def lift_body(*refs):
    out = refs[-1]
    total, squares = sum_of(refs[:-1])
    lifted = jnp.maximum(lax.rsqrt(squares / D + EPS) * total, 0.0)
    out[...] = (lifted * lifted).astype(BF16).reshape(4, 8, 2048)


def down_body(where, kv_at, *refs):
    pieces, (weight, out, rows) = refs[:4], refs[4:]
    core, first, _ = place(where, kv_at)
    for step, piece in zip((0,) + STEPS, pieces):
        at = (first + 4 - step) % 4
        for i in range(4):
            rows[jnp.where(core == 0, at * 4 + i, i * 4 + at)] = piece[i]
    terms = jnp.dot(rows[...].reshape(128, 2048), weight[...], preferred_element_type=F32)
    out[...] = terms.T.astype(BF16).reshape(8, 32, 128)


def finish_body(where, parts, middle_t, out):
    lowered = jnp.sum(parts[...].astype(F32), axis=0)
    own = middle_t[pl.ds(pl.multiple_of(where[0] * 32, 32), 32), :]
    out[...] = (own.astype(F32) + lowered).astype(BF16)


def advance_body(half, where, key_t, value, state, *refs):
    new_hbm, new, sems = refs[-3:]
    writes = []
    for i in range(4):
        b = half * 4 + i
        for h in range(2):
            rate = rate_of(where, h)
            row = value[b : b + 1, h * 512 : (h + 1) * 512]
            for r in range(0, 256, 64):
                kc = key_t[h * 256 + r : h * 256 + r + 64, b : b + 1]
                new[i, h, r : r + 64, :] = rate * state[b, h, r : r + 64, :] + kc * row
        copy = pltpu.make_async_copy(new.at[i], new_hbm.at[b], sems.at[i])
        copy.start()
        writes.append(copy)
    for copy in writes:
        copy.wait()


def advance(half, where, key_t, value, state, new_state=None):
    before = [] if new_state is None else [new_state]
    return pl.pallas_call(
        partial(advance_body, half),
        out_shape=shape(state.shape, F32),
        in_specs=[SMEM, VMEM, VMEM, VMEM] + [HBM] * len(before),
        out_specs=HBM,
        scratch_shapes=[pltpu.VMEM((4,) + state.shape[1:], F32), pltpu.SemaphoreType.DMA((4,))],
        input_output_aliases={4: 0} if before else {},
        compiler_params=pltpu.CompilerParams(vmem_limit_bytes=8 << 20),
        cost_estimate=pl.CostEstimate(flops=20_000_000, transcendentals=0, bytes_accessed=8 << 20),
        name="advance_" + str(half),
    )(where, key_t, value, in_vmem(state), *before)


def per_device(
    activations,
    mixer_gain,
    channel_gain,
    query_weight,
    key_weight,
    value_weight,
    gate_weight,
    output_weight,
    up_weight,
    down_weight,
    state_in,
):
    where = lax.axis_index("tp").astype(jnp.int32)[None]
    kv_at = lax.axis_index("kv").astype(jnp.int32)[None]
    where, kv_at = lax.optimization_barrier((where, kv_at))
    sources = (activations.T, mixer_gain[None], channel_gain[None])
    weights = (query_weight, key_weight, value_weight, gate_weight)
    rows, *weights = kernel(
        pack_body,
        (shape((8, 40, 128), BF16),) + tuple(pltpu.VMEM(w.shape, BF16) for w in weights),
        [SMEM] + [HBM] * 7,
        "pack",
        [pltpu.VMEM(v.shape, BF16) for v in sources] + [pltpu.SemaphoreType.DMA((7,))],
        limit_mib=1,
    )(where, *map(in_hbm, sources + weights))
    packed = lax.all_to_all(rows, "tp", 0, 0, tiled=True)
    *terms, stream, gains = kernel(
        project_body,
        (shape((4, 8, 3200), BF16),) * 4 + (shape((128, 256), BF16), shape((8, 128), F32)),
        [SMEM, SMEM] + [VMEM] * 5,
        "project",
        [pltpu.VMEM((16, 8, 256), F32)] * 2,
        limit_mib=8,
    )(where, kv_at, packed, *map(in_vmem, weights))
    state, out_w = load((state_in, output_weight), "load_early")
    own, state, out_w = lax.optimization_barrier((terms[0], state, out_w))
    own, *parts = kernel(
        partial(fold_body, 3072),
        (shape((8, 3200), F32),) + (shape((8, 3200), BF16),) * 3,
        [SMEM, SMEM] + [VMEM] * 4,
        "fold",
        limit_mib=8,
    )(where, kv_at, own, *exchange(terms[1:], True, HEAD_STEPS))
    mixed, key_t, value = kernel(
        retain_body,
        (shape((16, 8, 1024), BF16), shape((512, 8), F32), shape((8, 1024), F32)),
        [SMEM] + [VMEM] * 5,
        "retain",
        [pltpu.VMEM((8, 1024), F32)],
        limit_mib=8,
    )(where, own, *exchange(parts, False, HEAD_STEPS), in_vmem(state))
    mixed_all = lax.all_to_all(mixed, "kv", 0, 0, tiled=True)

    block = shape((128, 256), BF16)
    terms = kernel(out_body, block, [VMEM] * 2, "out", limit_mib=4)(mixed_all, in_vmem(out_w))
    received = from_chips(terms)
    new_state = advance(0, where, key_t, value, state)
    up_w = load((up_weight,), "load_up")[0]
    terms, new_state, up_w = lax.optimization_barrier((terms, new_state, up_w))
    quad = kernel(add_body, block, [VMEM] * 4, "add_chips", limit_mib=1)(terms, *received)
    *up_terms, middle_t = kernel(
        up_body,
        (shape((4, 8, 2176), BF16),) * 4 + (shape((256, 128), BF16),),
        [SMEM, SMEM] + [VMEM] * 5,
        "up",
        [pltpu.VMEM((16, 8, 256), F32)] * 2,
        limit_mib=8,
    )(where, kv_at, stream, quad, swap_cores(quad), gains, in_vmem(up_w))
    down_w = load((down_weight,), "load_down")[0]
    new_state = advance(1, where, key_t, value, state, new_state)
    own, down_w, new_state = lax.optimization_barrier((up_terms[0], down_w, new_state))
    sums = kernel(
        gather_sum_body, shape((4, 8, 2176), BF16), [VMEM] * 4, "gather_sum", limit_mib=4
    )(own, *exchange(up_terms[1:], True, STEPS))
    hidden = kernel(lift_body, shape((4, 8, 2048), BF16), [VMEM] * 4, "lift", limit_mib=4)(
        sums, *exchange([sums] * 3, False, STEPS)
    )
    down_terms = kernel(
        down_body,
        shape((8, 32, 128), BF16),
        [SMEM, SMEM] + [VMEM] * 5,
        "down",
        [pltpu.VMEM((16, 8, 2048), BF16)],
        limit_mib=8,
    )(where, kv_at, hidden, *exchange([hidden] * 3, True, STEPS), in_vmem(down_w))
    down_parts = lax.all_to_all(down_terms, "tp", 0, 0, tiled=True)
    out_t = kernel(finish_body, shape((32, 128), BF16), [SMEM, VMEM, VMEM], "finish")(
        where, down_parts, middle_t
    )
    return (out_t.T, new_state)


def solution(mesh):
    return jax.shard_map(
        per_device,
        mesh=mesh,
        in_specs=(
            P(None, ("kv", "tp")),
            P(("kv", "tp")),
            P(("kv", "tp")),
            P("kv", "tp"),
            P("kv", "tp"),
            P("kv", "tp"),
            P("kv", "tp"),
            P("tp", "kv"),
            P("kv", "tp"),
            P("tp", "kv"),
            P("kv", "tp", None, None),
        ),
        out_specs=(P(None, ("kv", "tp")), P("kv", "tp", None, None)),
        check_vma=False,
    )
```
